32 devices in a mesh: ep: 8 (over z, x), tp: 4 (over y, core).
Axes of the slice: x: 2, y: 2, z: 4, core: 2. Of those that a mesh axis runs over, the one named last changes fastest.
Arguments:
- tokens: bfloat16 [192, 4096], P('ep'), may hold values from -6 to 6
- delta_state: float32 [192, 16, 128, 128], P('ep', 'tp'), may hold values from -0.625 to 0.625
- attn_gain: float32 [4096], replicated, may hold values from 0.1 to 1.9
- query_weight: bfloat16 [4096, 2048], P('ep', 'tp'), may hold values from -0.09375 to 0.09375
- key_weight: bfloat16 [4096, 2048], P('ep', 'tp'), may hold values from -0.09375 to 0.09375
- value_weight: bfloat16 [4096, 2048], P('ep', 'tp'), may hold values from -0.09375 to 0.09375
- decay_weight: bfloat16 [4096, 16], replicated, may hold values from -0.09375 to 0.09375
- beta_weight: bfloat16 [4096, 16], replicated, may hold values from -0.09375 to 0.09375
- decay_rate: float32 [16], P('tp'), may hold values from 0.05 to 3
- head_gain: float32 [128], replicated, may hold values from 0.1 to 1.9
- output_weight: bfloat16 [2048, 4096], P('tp'), may hold values from -0.125 to 0.125
- ffn_gain: float32 [4096], replicated, may hold values from 0.1 to 1.9
- expert_ids: int32 [192, 2], P('ep'), may hold values from 0 to 7, all different within a row; in each aligned block of 24 rows (0 to 23, 24 to 47, ...) at most 12 rows name the same one
- group_prob: float32 [192], P('ep'), may hold values from 0.3 to 1
- expert_logit: float32 [192, 2], P('ep'), may hold values from -8 to 8
- expert_gate: bfloat16 [8, 4096, 1024], P('ep', None, 'tp'), may hold values from -0.09375 to 0.09375
- expert_up: bfloat16 [8, 4096, 1024], P('ep', None, 'tp'), may hold values from -0.09375 to 0.09375
- expert_down: bfloat16 [8, 1024, 4096], P('ep', 'tp'), may hold values from -0.1875 to 0.1875
- dense_gate: bfloat16 [4096, 4096], P('tp', 'ep'), may hold values from -0.09375 to 0.09375
- dense_up: bfloat16 [4096, 4096], P('tp', 'ep'), may hold values from -0.09375 to 0.09375
- dense_down: bfloat16 [4096, 4096], P('ep', 'tp'), may hold values from -0.09375 to 0.09375
- dense_mix: float32 [4096], P('tp'), may hold values from -3 to 3
Outputs:
- mixed_out: bfloat16 [192, 4096], P('ep', 'tp')
- new_state: float32 [192, 16, 128, 128], P('ep', 'tp')
The draws below stay inside these ranges and needn't reach their ends.
Inputs may be any that keep to these rules, and one draw needn't show every extreme that they name: `expert_ids`: each row names 2 different experts. Among the rows of one device (aligned blocks of 24 rows) no expert is named by more than 12 rows, and in every draw some expert reaches 12 in some block.
All inputs are finite; a program needn't handle non-finite values.
Results may differ from the reference program's by a relative error of at most 0.02.
Values may be sent and summed in bfloat16 or wider, within the bound.
A program may use at most 64 MiB of HBM per device.

```python
import math
import jax
import jax.numpy as jnp
import numpy as np
from jax import lax

D = 4096
HEADS = 16
HEAD = 128
FE = 1024
FD = 4096
TOPK = 2
SEQ_DEV = 24
BATCH = 192
EXPERTS = 8
CAP = 12
N_EP = 8
N_TP = 4


def block_scale(stream_key, extent, pieces, low, top_value):
    factor_of = 1.0
    for dim, blocks in pieces:
        heights = jax.random.uniform(jax.random.fold_in(jax.random.fold_in(stream_key, 6), dim), (blocks,), jnp.float32, low / len(pieces), top_value / len(pieces))
        factor_of = factor_of * jnp.repeat(jnp.exp(heights), extent[dim] // blocks).reshape((-1,) + (1,) * (len(extent) - 1 - dim))
    return factor_of


def routed_block(own_key, own, number, rows, count, top, reach, slope):
    sequence = jax.random.permutation(own_key, count)
    crowded, usual = portions_of(count, rows * top, reach, slope, True), portions_of(count, rows * top, reach, slope, False)
    places = jnp.arange(count)

    def named(lengths, offset_by):
        used = int((lengths > 0).sum())
        fixed = max(1, used // 4)
        shifted = fixed + (places - fixed + offset_by * (used - fixed)) % max(1, count - fixed)
        return jnp.zeros((count,), jnp.int32).at[sequence[jnp.where(places < fixed, places, shifted)]].set(jnp.asarray(lengths, jnp.int32))

    lengths = jnp.where(number % 4 == 0, named(crowded, number // 4), named(usual, number - number // 4 - 1))
    mixed = jax.random.permutation(jax.random.fold_in(own, 3), count)
    giver, receiver = mixed[0:count // 2 * 2:2], mixed[1:count // 2 * 2:2]
    slack = jnp.minimum(lengths[giver] - 1, reach - lengths[receiver]) // 2
    slack = jnp.where((giver == sequence[0]) | (receiver == sequence[0]) | (lengths[receiver] == 0), 0, jnp.maximum(slack, 0))
    shifted = jax.random.randint(jax.random.fold_in(own, 4), (count // 2,), 0, 1 << 20) % (slack + 1)
    lengths = lengths.at[giver].add(-shifted).at[receiver].add(shifted)
    items = jnp.searchsorted(jnp.cumsum(lengths), jnp.arange(rows * top), side="right").astype(jnp.int32)
    table = items.reshape(top, rows).T
    table = table[jax.random.permutation(jax.random.fold_in(own, 1), rows)]
    offset_by = jax.random.randint(jax.random.fold_in(own, 2), (rows, 1), 0, top)
    return jnp.take_along_axis(table, (jnp.arange(top)[None, :] + offset_by) % top, axis=1)


def portions_of(count, total, most, lean, full):
    portions = [(1 << 20) // math.isqrt(grade ** lean) + 1 for grade in range(1, count + 1)]
    largest = most if full else min(most, max(-(-total // count), total * portions[0] // sum(portions)))
    least = 1 if total - largest >= count - 1 else 0
    holding, rest = [largest] + [least] * (count - 1), total - largest - least * (count - 1)
    while rest > 0:
        free = [i for i in range(1, count) if holding[i] < largest] or [i for i in range(1, count) if holding[i] < most]
        whole, budget = sum([portions[i] for i in free]), rest
        for i in free:
            more = min(most - holding[i], max(1, budget * portions[i] // whole), rest)
            holding[i] = holding[i] + more
            rest = rest - more
    return np.array(holding)


def bell_draw(stream_key, extent, width, most, pieces=(), held_as=jnp.bfloat16):
    drawn = width * jax.random.normal(stream_key, extent, jnp.float32)
    if pieces:
        drawn = drawn * block_scale(stream_key, extent, pieces, -0.22, 0.18)
    return jnp.clip(drawn, -most, most).astype(held_as)


def setup_inputs(seed: int = 0) -> dict:
    keys = jax.random.split(jax.random.key(seed), 23)
    tokens = bell_draw(keys[0], (BATCH, D), 1.0, 6.0, ((0, 8),))
    delta_state = bell_draw(keys[1], (BATCH, HEADS, HEAD, HEAD), 0.1, 0.625, ((0, 8), (1, 4)), jnp.float32)
    attn_gain = jnp.clip(1.0 + 0.18 * jax.random.normal(keys[2], (D,), jnp.float32), 0.1, 1.9)
    query_weight = bell_draw(keys[3], (D, HEADS * HEAD), D ** -0.5, 0.09375, ((0, 8), (1, 4)))
    key_weight = bell_draw(keys[4], (D, HEADS * HEAD), D ** -0.5, 0.09375, ((0, 8), (1, 4)))
    value_weight = bell_draw(keys[5], (D, HEADS * HEAD), D ** -0.5, 0.09375, ((0, 8), (1, 4)))
    decay_weight = bell_draw(keys[6], (D, HEADS), D ** -0.5, 0.09375)
    beta_weight = bell_draw(keys[7], (D, HEADS), D ** -0.5, 0.09375)
    decay_rate = jnp.clip(jnp.exp(math.log(3.0) - 4.0943445 * jax.random.uniform(keys[8], (HEADS,), jnp.float32) ** block_scale(keys[8], (HEADS,), ((0, 4),), -0.2, 0.2)), 0.05, 3.0)
    head_gain = jnp.clip(1.0 + 0.18 * jax.random.normal(keys[9], (HEAD,), jnp.float32), 0.1, 1.9)
    output_weight = bell_draw(keys[10], (HEADS * HEAD, D), (HEADS * HEAD) ** -0.5, 0.125, ((0, 4),))
    ffn_gain = jnp.clip(1.0 + 0.18 * jax.random.normal(keys[11], (D,), jnp.float32), 0.1, 1.9)
    expert_ids_keys = jax.random.split(jax.random.fold_in(keys[12], 1), BATCH // SEQ_DEV)
    expert_ids_turns = jax.random.permutation(jax.random.fold_in(keys[12], 3), BATCH // SEQ_DEV)
    expert_ids = jax.vmap(lambda own, number: routed_block(jax.random.fold_in(keys[12], 2), own, number, SEQ_DEV, EXPERTS, TOPK, CAP, 2))(expert_ids_keys, expert_ids_turns).reshape((BATCH, TOPK))
    group_prob = jnp.clip(0.3 + 0.7 * jax.random.uniform(keys[13], (BATCH,), jnp.float32) ** block_scale(keys[13], (BATCH,), ((0, 8),), -0.2, 0.2), 0.3, 1.0)
    expert_logit = bell_draw(keys[14], (BATCH, TOPK), 1.5, 8.0, ((0, 8),), jnp.float32)
    expert_gate = bell_draw(keys[15], (EXPERTS, D, FE), D ** -0.5, 0.09375, ((0, 8), (2, 4)))
    expert_up = bell_draw(keys[16], (EXPERTS, D, FE), D ** -0.5, 0.09375, ((0, 8), (2, 4)))
    expert_down = bell_draw(keys[17], (EXPERTS, FE, D), FE ** -0.5, 0.1875, ((0, 8), (1, 4)))
    dense_gate = bell_draw(keys[18], (D, FD), D ** -0.5, 0.09375, ((0, 4), (1, 8)))
    dense_up = bell_draw(keys[19], (D, FD), D ** -0.5, 0.09375, ((0, 4), (1, 8)))
    dense_down = bell_draw(keys[20], (FD, D), FD ** -0.5, 0.09375, ((0, 8), (1, 4)))
    dense_mix = jnp.clip(jax.random.uniform(keys[21], (D,), jnp.float32, -3.0, 3.0) * block_scale(keys[21], (D,), ((0, 4),), -0.4, 0.0), -3.0, 3.0)
    return {"tokens": tokens, "delta_state": delta_state, "attn_gain": attn_gain, "query_weight": query_weight, "key_weight": key_weight, "value_weight": value_weight, "decay_weight": decay_weight, "beta_weight": beta_weight, "decay_rate": decay_rate, "head_gain": head_gain, "output_weight": output_weight, "ffn_gain": ffn_gain, "expert_ids": expert_ids, "group_prob": group_prob, "expert_logit": expert_logit, "expert_gate": expert_gate, "expert_up": expert_up, "expert_down": expert_down, "dense_gate": dense_gate, "dense_up": dense_up, "dense_down": dense_down, "dense_mix": dense_mix}


EPS = 1e-06

def rms_scale(values, gain):
    mean_sq = lax.optimization_barrier(jnp.mean(values * values, axis=-1, keepdims=True))
    return values * lax.rsqrt(mean_sq + EPS) * gain

def unit_rows(values):
    return values * lax.rsqrt(lax.optimization_barrier(jnp.sum(values * values, axis=-1, keepdims=True)) + EPS)

def rounded_back(values):
    return lax.optimization_barrier(values.astype(jnp.bfloat16)).astype(jnp.float32)

def block_sum(left, right, blocks):
    size = left.shape[1] // blocks
    total = jnp.zeros((left.shape[0], right.shape[1]), jnp.float32)
    for index in range(blocks):
        part = jnp.dot(left[:, index * size:(index + 1) * size], right[index * size:(index + 1) * size], preferred_element_type=jnp.float32)
        total = total + rounded_back(part)
    return total

def reference(tokens, delta_state, attn_gain, query_weight, key_weight, value_weight, decay_weight, beta_weight, decay_rate, head_gain, output_weight, ffn_gain, expert_ids, group_prob, expert_logit, expert_gate, expert_up, expert_down, dense_gate, dense_up, dense_down, dense_mix):
    residual = tokens.astype(jnp.float32)
    normed = rms_scale(residual, attn_gain).astype(jnp.bfloat16)

    def heads_of(weight):
        product = jnp.dot(normed, weight, preferred_element_type=jnp.float32)
        return rounded_back(product).reshape(BATCH, HEADS, HEAD)
    query_unit = unit_rows(heads_of(query_weight)) * HEAD ** (-0.5)
    key_unit = unit_rows(heads_of(key_weight))
    value_heads = heads_of(value_weight)
    decay = jnp.exp(-decay_rate * jax.nn.softplus(jnp.dot(normed, decay_weight, preferred_element_type=jnp.float32)))
    beta_gate = jax.nn.sigmoid(jnp.dot(normed, beta_weight, preferred_element_type=jnp.float32))
    recalled = jnp.einsum('bhk,bhkv->bhv', key_unit, delta_state, precision=lax.Precision.HIGHEST)
    correction = beta_gate[..., None] * (value_heads - decay[..., None] * recalled)
    new_state = decay[..., None, None] * delta_state + key_unit[..., :, None] * correction[..., None, :]
    read_out = jnp.einsum('bhk,bhkv->bhv', query_unit, new_state, precision=lax.Precision.HIGHEST)
    head_out = rms_scale(read_out, head_gain).astype(jnp.bfloat16).reshape(BATCH, HEADS * HEAD)
    attn_sum = block_sum(head_out, output_weight, N_TP)
    middle = residual + attn_sum
    ffn_in = rms_scale(middle, ffn_gain).astype(jnp.bfloat16)
    dense_pre_gate = block_sum(ffn_in, dense_gate, N_TP)
    dense_pre_up = block_sum(ffn_in, dense_up, N_TP)
    dense_hidden = (jax.nn.silu(dense_pre_gate) * dense_pre_up).astype(jnp.bfloat16)
    dense_out = jnp.dot(dense_hidden, dense_down, preferred_element_type=jnp.float32)
    pairs = SEQ_DEV * TOPK
    block_ids = expert_ids.reshape(N_EP, pairs)
    onehot = (block_ids[:, :, None] == jnp.arange(EXPERTS, dtype=jnp.int32)[None, None, :]).astype(jnp.int32)
    ranks = lax.optimization_barrier(jnp.sum(onehot * (jnp.cumsum(onehot, axis=1) - 1), axis=2))
    sources = jnp.arange(N_EP, dtype=jnp.int32)[:, None]
    places = (block_ids * (N_EP * CAP) + sources * CAP + ranks).reshape(-1).astype(jnp.int32)
    repeated = jnp.repeat(ffn_in, TOPK, axis=0)
    slots = jnp.zeros((EXPERTS * N_EP * CAP, D), jnp.bfloat16).at[places].set(repeated)
    slots = slots.reshape(EXPERTS, N_EP * CAP, D)

    def one_expert(inputs):
        arrived, gate_w, up_w, down_w = inputs
        gate_vals = jnp.dot(arrived, gate_w, preferred_element_type=jnp.float32)
        up_vals = jnp.dot(arrived, up_w, preferred_element_type=jnp.float32)
        expert_hidden = (jax.nn.silu(gate_vals) * up_vals).astype(jnp.bfloat16)
        return block_sum(expert_hidden, down_w, N_TP).astype(jnp.bfloat16)
    expert_result = lax.map(one_expert, (slots, expert_gate, expert_up, expert_down))
    picked = jnp.take(expert_result.reshape(EXPERTS * N_EP * CAP, D), places, axis=0)
    picked = picked.astype(jnp.float32).reshape(BATCH, TOPK, D)
    logit_exp = jnp.exp(expert_logit)
    route_weight = group_prob[:, None] * logit_exp / lax.optimization_barrier(jnp.sum(logit_exp, axis=1, keepdims=True))
    expert_mix = lax.optimization_barrier(jnp.sum(route_weight[..., None] * picked, axis=1))
    mixed_out = (middle + jax.nn.sigmoid(dense_mix) * dense_out + expert_mix).astype(jnp.bfloat16)
    return (mixed_out, new_state)
```

```python
import functools
import math

import jax
import jax.numpy as jnp
from jax import lax
from jax.experimental import pallas as pl
from jax.experimental.pallas import tpu as pltpu
from jax.sharding import PartitionSpec as P

EPS = 1e-06
BF = jnp.bfloat16
F32 = jnp.float32
MESH = pl.DeviceIdType.MESH


def dot(left, right):
    return jnp.dot(left, right, preferred_element_type=F32)


def dot_t(left, right):
    return lax.dot_general(left, right, (((1,), (1,)), ((), ())), preferred_element_type=F32)


def silu(values):
    return values / (1.0 + jnp.exp(-values))


class BlockOf:
    def __init__(self, ref, block):
        self.ref, self.block = ref, block

    @property
    def at(self):
        return self

    def __getitem__(self, index):
        return self.ref.at[index, self.block]


def kernel(dims, *refs):
    n_ep, n_tp, rows, width, heads, members, cap, n_in, n_weights = dims
    inputs, refs = refs[:n_in], refs[n_in:]
    (tokens, attn_gain, decay_rate, head_gain, ffn_gain, ids, group_prob, logit, mix) = inputs[:9]
    hbm = inputs[9:]
    out, state = refs[:2]
    held = (state,) + refs[2 : 1 + n_weights]
    refs = refs[1 + n_weights :]
    state, w_decay, w_beta, w_q, w_k, w_v, w_o, w_dg, w_du, w_eg, w_eu, w_ed, w_dd = held
    (
        n_send, n_recv, q_send, q_recv, c_send, c_rows, c_recv, kq, recall, corr_ref, decay_ref,
        head_out, a_send, a_recv, s_recv, scale_rows, scale_ref, middle_ref, x_all, g_all, d_send, d_recv, h_all,
        e_send, e_recv, f_send, f_recv, place_ref, dense_ref, load_sem, ep_send, ep_recv, tp_send, tp_recv,
    ) = refs
    me = lax.axis_index("ep")
    my = lax.axis_index("tp")
    chunk = width // n_tp
    depth = width // n_ep
    batch = n_ep * rows
    local = heads * 128
    groups = n_ep // members
    group_slots = members * cap
    group_tokens = members * rows
    slots = groups * group_slots
    my_group = lax.div(me, members)
    my_member = lax.rem(me, members)

    def members_of(offset):
        first = lax.rem(my_group + offset + groups, groups) * members
        start = 1 if offset == 0 else 0
        return [first + lax.rem(my_member + m, members) for m in range(start, members)]

    loads = [
        pltpu.make_async_copy(src, dst, load_sem.at[i])
        for i, (src, dst) in enumerate(zip(hbm, held))
    ]
    state_i, decay_i, beta_i, q_i, k_i, v_i, o_i, dg_i, du_i, eg_i, eu_i, ed_i, dd_i = range(13)
    order = (decay_i, beta_i, q_i, k_i, v_i, state_i, o_i, dg_i, du_i, eg_i, eu_i, ed_i, dd_i)

    ep_peers = [p for offset in range(groups) for p in members_of(offset)]
    tp_peers = [lax.rem(my + d, n_tp) for d in range(1, n_tp)]
    barrier = pltpu.get_barrier_semaphore()
    for p in ep_peers:
        pl.semaphore_signal(barrier, inc=1, device_id=(p, my), device_id_type=MESH)
    for p in tp_peers:
        pl.semaphore_signal(barrier, inc=1, device_id=(me, p), device_id_type=MESH)
    for i in order:
        loads[i].start()

    def ep_copy(phase, src, dst, peer, source):
        return pltpu.make_async_remote_copy(
            src_ref=src, dst_ref=dst,
            send_sem=ep_send.at[phase, peer], recv_sem=ep_recv.at[phase, source],
            device_id=(peer, my), device_id_type=MESH,
        )

    def tp_copy(phase, src, dst, peer, source):
        return pltpu.make_async_remote_copy(
            src_ref=src, dst_ref=dst,
            send_sem=tp_send.at[phase, peer], recv_sem=tp_recv.at[phase, source],
            device_id=(me, peer), device_id_type=MESH,
        )

    def exchange(copy, phase, peers, mine, src_of, dst):
        for p in peers:
            copy(phase, src_of(p), dst.at[mine], p, mine).start()

        def arrived():
            for p in peers:
                done = copy(phase, src_of(p), dst.at[p], p, p)
                done.wait_recv()
                done.wait_send()

        return arrived

    x = tokens[...].astype(F32)
    mean_sq = jnp.mean(x * x, axis=-1, keepdims=True)
    normed = (x * lax.rsqrt(mean_sq + EPS) * attn_gain[...]).astype(BF)
    for p in range(n_ep):
        n_send[p] = normed[:, p * depth : (p + 1) * depth]
    pl.semaphore_wait(barrier, n_ep + n_tp - 2)
    wait_n = exchange(ep_copy, 0, ep_peers, me, lambda p: n_send.at[p], n_recv)
    n_recv[me] = n_send[me]

    logit_exp = jnp.exp(logit[...])
    route = group_prob[...] * logit_exp / jnp.sum(logit_exp, axis=0, keepdims=True)
    names = ids[...]
    eye = lax.broadcasted_iota(jnp.int32, (rows, rows), 0) == lax.broadcasted_iota(
        jnp.int32, (rows, rows), 1
    )
    c_send[...] = jnp.zeros_like(c_send)
    for p in range(n_ep):
        flat = jnp.sum(jnp.where(names == p, route, 0.0), axis=0, keepdims=True)
        c_send[p, :, :rows] = jnp.broadcast_to(flat, (8, rows))
    wait_c = exchange(ep_copy, 4, ep_peers, me, lambda p: c_send.at[p], c_rows)
    c_rows[me] = c_send[me]

    def column(row):
        return jnp.sum(jnp.where(eye, row[:, :rows], 0.0), axis=1, keepdims=True)

    loads[decay_i].wait()
    loads[beta_i].wait()
    decay_pre = dot_t(normed, w_decay[...])
    beta_pre = dot_t(normed, w_beta[...])
    lane = lax.broadcasted_iota(jnp.int32, decay_pre.shape, 1)
    decays, betas = [], []
    for h in range(heads):
        mine = lane == my * heads + h
        d = jnp.sum(jnp.where(mine, decay_pre, 0.0), axis=1, keepdims=True)
        b = jnp.sum(jnp.where(mine, beta_pre, 0.0), axis=1, keepdims=True)
        soft = jnp.maximum(d, 0.0) + jnp.log1p(jnp.exp(-jnp.abs(d)))
        decays.append(jnp.exp(-decay_rate[:, h : h + 1] * soft))
        betas.append(1.0 / (1.0 + jnp.exp(-b)))
    for i in (q_i, k_i, v_i):
        loads[i].wait()

    wait_n()
    spread = n_recv[...].astype(F32).reshape(batch, depth).astype(BF)
    wait_heads = []
    for j, w in enumerate((w_k, w_q, w_v)):
        part = dot(spread, w[...]).reshape(n_ep, rows, local)
        q_send[j] = part.astype(BF)
        wait_heads.append(
            exchange(ep_copy, 1 + j, ep_peers, me, lambda p, j=j: q_send.at[j, p], q_recv.at[j])
        )
        q_recv[j, me] = q_send[j, me]

    def summed(j):
        wait_heads[j]()
        total = q_recv[j, 0].astype(F32)
        for p in range(1, n_ep):
            total = total + q_recv[j, p].astype(F32)
        return total.astype(BF).astype(F32)

    k_rows = summed(0)
    q_rows = summed(1)
    loads[state_i].wait()

    def head_of(values, h):
        return values[:, h * 128 : (h + 1) * 128]

    def unit(values):
        return values * lax.rsqrt(jnp.sum(values * values, axis=-1, keepdims=True) + EPS)

    units = []
    for h in range(heads):
        q_unit = unit(head_of(q_rows, h)) * 128 ** (-0.5)
        k_unit = unit(head_of(k_rows, h))
        units.append((q_unit, k_unit))
        kq[:, h, :] = k_unit
        kq[:, heads + h, :] = q_unit

    def one_row(b, _):
        pair = kq[b].astype(BF)
        for h in range(heads):
            both = dot(pair, state[b, h].astype(BF))
            recall[h, pl.ds(b, 1), :] = both[h : h + 1]
            recall[heads + h, pl.ds(b, 1), :] = both[heads + h : heads + h + 1]
        return 0

    lax.fori_loop(0, rows, one_row, 0, unroll=4)
    v_rows = summed(2)
    for h in range(heads):
        q_unit, k_unit = units[h]
        decay, beta = decays[h], betas[h]
        corr = beta * (head_of(v_rows, h) - decay * recall[h])
        read = decay * recall[heads + h] + jnp.sum(q_unit * k_unit, axis=-1, keepdims=True) * corr
        read = read * lax.rsqrt(jnp.mean(read * read, axis=-1, keepdims=True) + EPS) * head_gain[...]
        head_out[:, h * 128 : (h + 1) * 128] = read.astype(BF)
        corr_ref[h] = corr
        decay_ref[h] = jnp.broadcast_to(decay, (rows, 128))

    loads[o_i].wait()
    ho = head_out[...]
    for c in range(n_tp):
        a_send[c] = dot(ho, w_o[:, c * chunk : (c + 1) * chunk]).astype(BF)
    wait_a = exchange(tp_copy, 0, tp_peers, my, lambda p: a_send.at[p], a_recv)
    a_recv[my] = a_send[my]
    own = pl.ds(pl.multiple_of(my * chunk, 128), chunk)

    def update_row(b, _):
        columns = kq[b].T
        for h in range(heads):
            corr = corr_ref[h, pl.ds(b, 1), :]
            decay = decay_ref[h, pl.ds(b, 1), :]
            state[b, h] = decay * state[b, h] + columns[:, h : h + 1] * corr
        return 0

    lax.fori_loop(0, rows, update_row, 0, unroll=2)
    middle = tokens[:, own].astype(F32)
    wait_a()
    for p in range(n_tp):
        middle = middle + a_recv[p].astype(F32)
    x_all[me] = (middle * ffn_gain[:, own]).astype(BF)
    for p in ep_peers:
        ep_copy(5, x_all.at[me], x_all.at[me], p, me).start()
    middle_ref[...] = middle
    s_recv[my] = jnp.broadcast_to(jnp.sum(middle * middle, axis=-1, keepdims=True), (rows, 128))
    wait_s = exchange(tp_copy, 1, tp_peers, my, lambda p: s_recv.at[my], s_recv)
    wait_c()
    for p in range(n_ep):
        c_recv[p] = jnp.broadcast_to(column(c_rows[p, :1, :]), (rows, 128))
    tri = (
        lax.broadcasted_iota(jnp.int32, (group_tokens, group_tokens), 0)
        >= lax.broadcasted_iota(jnp.int32, (group_tokens, group_tokens), 1)
    ).astype(F32).astype(BF)
    slot = lax.broadcasted_iota(jnp.int32, (group_tokens, group_slots), 1).astype(F32)
    for g in range(groups):
        coef = c_recv[g * members : (g + 1) * members].reshape(group_tokens, 128)[:, :1]
        named = coef > 0.0
        flags = jnp.broadcast_to(jnp.where(named, 1.0, 0.0), (group_tokens, 128)).astype(BF)
        rank = dot(tri, flags)[:, :1] - 1.0
        place_ref[g] = jnp.where((rank == slot) & named, 1.0, 0.0).astype(BF)
    wait_s()
    total = s_recv[0]
    for p in range(1, n_tp):
        total = total + s_recv[p]
    scale = lax.rsqrt(total / width + EPS)
    diagonal = lax.broadcasted_iota(jnp.int32, (rows, 128), 0) == lax.broadcasted_iota(
        jnp.int32, (rows, 128), 1
    )
    scale_rows[me] = jnp.broadcast_to(
        jnp.sum(jnp.where(diagonal, scale, 0.0), axis=0, keepdims=True), (8, 128)
    )
    wait_scale = exchange(ep_copy, 7, ep_peers, me, lambda p: scale_rows.at[me], scale_rows)
    wait_g = []
    for offset in range(groups):
        g = lax.rem(my_group - offset + groups, groups)
        for p in members_of(-offset):
            ep_copy(5, x_all.at[me], x_all.at[p], p, p).wait_recv()
        block = x_all[pl.ds(g * members, members)].astype(F32)
        g_all[my, g] = lax.dot_general(
            place_ref[g], block.reshape(group_tokens, chunk).astype(BF),
            (((0,), (0,)), ((), ())), preferred_element_type=F32,
        ).astype(BF)
        wait_g.append(
            exchange(
                tp_copy, 4 + offset, tp_peers, my, lambda p, g=g: g_all.at[my, g],
                BlockOf(g_all, g),
            )
        )
    for p in ep_peers:
        ep_copy(5, x_all.at[me], x_all.at[me], p, me).wait_send()
    for i in (dg_i, du_i, eg_i, eu_i, ed_i, dd_i):
        loads[i].wait()
    xs = x_all[...].astype(F32).reshape(batch, chunk).astype(BF)
    hidden = w_dg.shape[1]
    part_rows = batch // n_tp
    for j, w in enumerate((w_dg, w_du)):
        part = dot(xs, w[...]).reshape(n_tp, part_rows, hidden)
        d_send[:, :, j * hidden : (j + 1) * hidden] = part.astype(BF)
    wait_d = exchange(tp_copy, 2, tp_peers, my, lambda p: d_send.at[p], d_recv)
    d_recv[my] = d_send[my]

    for wait in wait_g:
        wait()
    wait_scale()
    for p in range(n_ep):
        scale_ref[p] = jnp.broadcast_to(column(scale_rows[p, :1, :]), (rows, 128))
    slot_scale = jnp.concatenate(
        [
            lax.dot_general(
                place_ref[g].astype(F32),
                scale_ref[g * members : (g + 1) * members].reshape(group_tokens, 128),
                (((0,), (0,)), ((), ())), precision=lax.Precision.HIGHEST,
                preferred_element_type=F32,
            )
            for g in range(groups)
        ],
        axis=0,
    )[:, :1]
    gate = jnp.zeros((slots, w_eg.shape[2]), F32)
    up = jnp.zeros((slots, w_eg.shape[2]), F32)
    for c in range(n_tp):
        routed = g_all[c].astype(F32).reshape(slots, chunk).astype(BF)
        gate = gate + dot(routed, w_eg[0, c * chunk : (c + 1) * chunk, :])
        up = up + dot(routed, w_eu[0, c * chunk : (c + 1) * chunk, :])
    expert_hidden = (silu(gate * slot_scale) * (up * slot_scale)).astype(BF)
    for c in range(n_tp):
        part = dot(expert_hidden, w_ed[0, :, c * chunk : (c + 1) * chunk])
        e_send[c] = part.reshape(groups, group_slots, chunk).astype(BF)
    e_recv[my] = e_send[my]
    returns = list(range(1, groups)) + [0]
    group_at = [lax.rem(my_group + offset, groups) for offset in range(groups)]

    def send_e(offset):
        g = group_at[offset]
        return exchange(
            tp_copy, 4 + groups + offset, tp_peers, my, lambda p: e_send.at[p, g],
            BlockOf(e_recv, g),
        )

    wait_e = {returns[0]: send_e(returns[0])}
    wait_d()
    pre = d_recv[0].astype(F32)
    for p in range(1, n_tp):
        pre = pre + d_recv[p].astype(F32)
    per_part = part_rows // rows
    pre = pre * scale_ref[pl.ds(my * per_part, per_part)].reshape(part_rows, 128)[:, :1]
    h_all[my] = (silu(pre[:, :hidden]) * pre[:, hidden:]).astype(BF)
    wait_h = exchange(tp_copy, 3, tp_peers, my, lambda p: h_all.at[my], h_all)
    for offset in returns[1:]:
        wait_e[offset] = send_e(offset)
    wait_h()
    dense_hidden = h_all[...].astype(F32).reshape(batch, hidden).astype(BF)
    dense = dot(dense_hidden, w_dd[...]) * (1.0 / (1.0 + jnp.exp(-mix[...])))
    dense_ref[...] = dense.reshape(n_ep, rows, chunk)
    for offset in returns:
        g = group_at[offset]
        here = pl.ds(g * members, members)
        wait_e[offset]()
        result = e_recv[0, g].astype(F32)
        for p in range(1, n_tp):
            result = result + e_recv[p, g].astype(F32)
        coef = c_recv[here].reshape(group_tokens, 128)[:, :1]
        mixed = coef * dot(place_ref[g], result.astype(BF))
        combined = dense_ref[here] + mixed.reshape(members, rows, chunk)
        f_send[here] = combined.astype(BF)
        for p in members_of(offset):
            ep_copy(6, f_send.at[p], f_recv.at[me], p, me).start()
    final = middle_ref[...] + f_send[me].astype(F32)
    f_recv[me] = jnp.zeros((rows, chunk), BF)
    for p in ep_peers:
        done = ep_copy(6, f_send.at[p], f_recv.at[p], p, p)
        done.wait_recv()
        done.wait_send()
    for p in range(n_ep):
        final = final + f_recv[p].astype(F32)
    out[...] = final.astype(BF)


def per_device(
    tokens, delta_state, attn_gain, query_weight, key_weight, value_weight, decay_weight,
    beta_weight, decay_rate, head_gain, output_weight, ffn_gain, expert_ids, group_prob,
    expert_logit, expert_gate, expert_up, expert_down, dense_gate, dense_up, dense_down, dense_mix,
):
    n_ep = lax.axis_size("ep")
    n_tp = lax.axis_size("tp")
    rows, width = tokens.shape
    heads = delta_state.shape[1]
    local = heads * 128
    topk = expert_ids.shape[1]
    cap = max(2, 2 * rows * topk // n_ep)
    members = 8 // math.gcd(cap, 8)
    if n_ep % members:
        members = n_ep
    groups = n_ep // members
    group_slots = members * cap
    chunk = width // n_tp
    depth = width // n_ep
    batch = n_ep * rows
    hidden = dense_gate.shape[1]
    small = (
        tokens, attn_gain[None, :], decay_rate[None, :], head_gain[None, :], ffn_gain[None, :],
        expert_ids.T, group_prob[None, :], expert_logit.T, dense_mix[None, :],
    )
    weights = (
        delta_state, decay_weight.T, beta_weight.T, query_weight, key_weight, value_weight,
        output_weight, dense_gate, dense_up, expert_gate, expert_up, expert_down, dense_down,
    )
    dims = (n_ep, n_tp, rows, width, heads, members, cap, len(small) + len(weights), len(weights))
    vmem = pl.BlockSpec(memory_space=pltpu.VMEM)
    kq_rows = -(-2 * heads // 8) * 8
    scratch = [pltpu.VMEM(w.shape, w.dtype) for w in weights[1:]]
    scratch += [
        pltpu.VMEM(shape, dtype)
        for shape, dtype in (
            ((n_ep, rows, depth), BF), ((n_ep, rows, depth), BF),
            ((3, n_ep, rows, local), BF), ((3, n_ep, rows, local), BF),
            ((n_ep, 8, 128), F32), ((n_ep, 8, 128), F32), ((n_ep, rows, 128), F32),
            ((rows, kq_rows, 128), F32), ((2 * heads, rows, 128), F32),
            ((heads, rows, 128), F32), ((heads, rows, 128), F32), ((rows, local), BF),
            ((n_tp, rows, chunk), BF), ((n_tp, rows, chunk), BF), ((n_tp, rows, 128), F32),
            ((n_ep, 8, 128), F32), ((n_ep, rows, 128), F32), ((rows, chunk), F32), ((n_ep, rows, chunk), BF), ((n_tp, groups, group_slots, chunk), BF),
            ((n_tp, batch // n_tp, 2 * hidden), BF), ((n_tp, batch // n_tp, 2 * hidden), BF),
            ((n_tp, batch // n_tp, hidden), BF),
            ((n_tp, groups, group_slots, chunk), BF), ((n_tp, groups, group_slots, chunk), BF),
            ((n_ep, rows, chunk), BF), ((n_ep, rows, chunk), BF),
            ((groups, members * rows, group_slots), BF), ((n_ep, rows, chunk), F32),
        )
    ]
    scratch += [
        pltpu.SemaphoreType.DMA((len(weights),)),
        pltpu.SemaphoreType.DMA((8, n_ep)), pltpu.SemaphoreType.DMA((8, n_ep)),
        pltpu.SemaphoreType.DMA((4 + 2 * groups, n_tp)), pltpu.SemaphoreType.DMA((4 + 2 * groups, n_tp)),
    ]
    mixed_out, new_state = pl.pallas_call(
        functools.partial(kernel, dims),
        out_shape=(
            jax.ShapeDtypeStruct((rows, chunk), BF), pltpu.VMEM(delta_state.shape, F32),
        ),
        in_specs=[vmem] * len(small) + [pl.BlockSpec(memory_space=pl.ANY)] * len(weights),
        out_specs=(vmem, vmem),
        scratch_shapes=scratch,
        compiler_params=pltpu.CompilerParams(
            collective_id=0, has_side_effects=True, vmem_limit_bytes=44 * 1024 * 1024
        ),
    )(*small, *weights)
    return mixed_out, new_state


def solution(mesh):
    return jax.shard_map(
        per_device,
        mesh=mesh,
        in_specs=(
            P("ep", None), P("ep", "tp", None, None), P(), P("ep", "tp"), P("ep", "tp"),
            P("ep", "tp"), P(), P(), P("tp"), P(), P("tp", None), P(), P("ep", None), P("ep"),
            P("ep", None), P("ep", None, "tp"), P("ep", None, "tp"), P("ep", "tp", None),
            P("tp", "ep"), P("tp", "ep"), P("ep", "tp"), P("tp"),
        ),
        out_specs=(P("ep", "tp"), P("ep", "tp", None, None)),
        check_vma=False,
    )
```

```python
import functools
import math

import jax
import jax.numpy as jnp
from jax import lax
from jax.experimental import pallas as pl
from jax.experimental.pallas import tpu as pltpu
from jax.sharding import PartitionSpec as P

EPS = 1e-06
BF = jnp.bfloat16
F32 = jnp.float32
MESH = pl.DeviceIdType.MESH


def dot(left, right):
    return jnp.dot(left, right, preferred_element_type=F32)


def dot_t(left, right):
    return lax.dot_general(left, right, (((1,), (1,)), ((), ())), preferred_element_type=F32)


def silu(values):
    return values / (1.0 + jnp.exp(-values))


def kernel(dims, *refs):
    n_ep, n_tp, rows, width, heads, members, cap, n_in = dims
    hbm, refs = refs[:n_in], refs[n_in:]
    out, state = refs[:2]
    held = refs[2 : 11] + (state,) + refs[11 : 1 + n_in]
    refs = refs[1 + n_in :]
    (tokens, attn_gain, decay_rate, head_gain, ffn_gain, ids, group_prob, logit, mix) = held[:9]
    state, w_decay, w_beta, w_q, w_k, w_v, w_o, w_dg, w_du, w_eg, w_eu, w_ed, w_dd = held[9:]
    (
        n_send, n_recv, q_send, q_recv, c_send, c_rows, c_recv, kq, recall, corr_ref, decay_ref,
        head_out, a_send, a_recv, s_recv, scale_rows, scale_ref, middle_ref, x_all, g_all,
        d_half, d_send, d_near, d_far, h_all, e_part, e_near, e_send, e_recv, f_send, f_recv, place_ref, dense_ref, load_sem, ep_send, ep_recv, tp_send, tp_recv,
    ) = refs
    me = lax.axis_index("ep")
    my = lax.axis_index("tp")
    chunk = width // n_tp
    depth = width // n_ep
    batch = n_ep * rows
    local = heads * 128
    groups = n_ep // members
    group_slots = members * cap
    group_tokens = members * rows
    slots = groups * group_slots
    my_group = lax.div(me, members)
    my_member = lax.rem(me, members)

    def members_of(offset):
        first = lax.rem(my_group + offset + groups, groups) * members
        start = 1 if offset == 0 else 0
        return [first + lax.rem(my_member + m, members) for m in range(start, members)]

    loads = [
        pltpu.make_async_copy(src, dst, load_sem.at[i])
        for i, (src, dst) in enumerate(zip(hbm, held))
    ]
    state_i, decay_i, beta_i, q_i, k_i, v_i, o_i, dg_i, du_i, eg_i, eu_i, ed_i, dd_i = range(9, 22)
    order = (decay_i, beta_i, q_i, k_i, v_i, state_i, o_i, dg_i, du_i, eg_i, eu_i, ed_i, dd_i)

    ep_peers = [p for offset in range(groups) for p in members_of(offset)]
    tp_peers = [lax.rem(my + d, n_tp) for d in range(1, n_tp)]
    for i in range(9):
        loads[i].start()
    barrier = pltpu.get_barrier_semaphore()
    for p in ep_peers:
        pl.semaphore_signal(barrier, inc=1, device_id=(p, my), device_id_type=MESH)
    for p in tp_peers:
        pl.semaphore_signal(barrier, inc=1, device_id=(me, p), device_id_type=MESH)
    for i in order:
        loads[i].start()

    def ep_copy(phase, src, dst, peer, source):
        return pltpu.make_async_remote_copy(
            src_ref=src, dst_ref=dst,
            send_sem=ep_send.at[phase, peer], recv_sem=ep_recv.at[phase, source],
            device_id=(peer, my), device_id_type=MESH,
        )

    def tp_copy(phase, src, dst, peer, source):
        return pltpu.make_async_remote_copy(
            src_ref=src, dst_ref=dst,
            send_sem=tp_send.at[phase, peer], recv_sem=tp_recv.at[phase, source],
            device_id=(me, peer), device_id_type=MESH,
        )

    def exchange(copy, phase, peers, mine, src_of, dst):
        for p in peers:
            copy(phase, src_of(p), dst.at[mine], p, mine).start()

        def arrived():
            for p in peers:
                done = copy(phase, src_of(p), dst.at[p], p, p)
                done.wait_recv()
                done.wait_send()

        return arrived

    for i in range(9):
        loads[i].wait()
    x = tokens[...].astype(F32)
    mean_sq = jnp.mean(x * x, axis=-1, keepdims=True)
    normed = (x * lax.rsqrt(mean_sq + EPS) * attn_gain[...]).astype(BF)
    for p in range(n_ep):
        n_send[p] = normed[:, p * depth : (p + 1) * depth]
    pl.semaphore_wait(barrier, n_ep + n_tp - 2)
    wait_n = exchange(ep_copy, 0, ep_peers, me, lambda p: n_send.at[p], n_recv)
    n_recv[me] = n_send[me]

    logit_exp = jnp.exp(logit[...])
    route = group_prob[...] * logit_exp / jnp.sum(logit_exp, axis=0, keepdims=True)
    names = ids[...]
    eye = lax.broadcasted_iota(jnp.int32, (rows, rows), 0) == lax.broadcasted_iota(
        jnp.int32, (rows, rows), 1
    )
    c_send[...] = jnp.zeros_like(c_send)
    for p in range(n_ep):
        flat = jnp.sum(jnp.where(names == p, route, 0.0), axis=0, keepdims=True)
        c_send[p, :, :rows] = jnp.broadcast_to(flat, (8, rows))
    wait_c = exchange(ep_copy, 4, ep_peers, me, lambda p: c_send.at[p], c_rows)
    c_rows[me] = c_send[me]

    def column(row):
        return jnp.sum(jnp.where(eye, row[:, :rows], 0.0), axis=1, keepdims=True)

    loads[decay_i].wait()
    loads[beta_i].wait()
    decay_pre = dot_t(normed, w_decay[...])
    beta_pre = dot_t(normed, w_beta[...])
    lane = lax.broadcasted_iota(jnp.int32, decay_pre.shape, 1)
    decays, betas = [], []
    for h in range(heads):
        mine = lane == my * heads + h
        d = jnp.sum(jnp.where(mine, decay_pre, 0.0), axis=1, keepdims=True)
        b = jnp.sum(jnp.where(mine, beta_pre, 0.0), axis=1, keepdims=True)
        soft = jnp.maximum(d, 0.0) + jnp.log1p(jnp.exp(-jnp.abs(d)))
        decays.append(jnp.exp(-decay_rate[:, h : h + 1] * soft))
        betas.append(1.0 / (1.0 + jnp.exp(-b)))
    for i in (q_i, k_i, v_i):
        loads[i].wait()

    wait_n()
    spread = n_recv[...].astype(F32).reshape(batch, depth).astype(BF)
    wait_heads = []
    for j, w in enumerate((w_k, w_q, w_v)):
        part = dot(spread, w[...]).reshape(n_ep, rows, local)
        q_send[j] = part.astype(BF)
        wait_heads.append(
            exchange(ep_copy, 1 + j, ep_peers, me, lambda p, j=j: q_send.at[j, p], q_recv.at[j])
        )
        q_recv[j, me] = q_send[j, me]

    def summed(j):
        wait_heads[j]()
        total = q_recv[j, 0].astype(F32)
        for p in range(1, n_ep):
            total = total + q_recv[j, p].astype(F32)
        return total.astype(BF).astype(F32)

    k_rows = summed(0)
    q_rows = summed(1)
    loads[state_i].wait()

    def head_of(values, h):
        return values[:, h * 128 : (h + 1) * 128]

    def unit(values):
        return values * lax.rsqrt(jnp.sum(values * values, axis=-1, keepdims=True) + EPS)

    units = []
    for h in range(heads):
        q_unit = unit(head_of(q_rows, h)) * 128 ** (-0.5)
        k_unit = unit(head_of(k_rows, h))
        units.append((q_unit, k_unit))
        kq[:, h, :] = k_unit
        kq[:, heads + h, :] = q_unit

    def one_row(b, _):
        pair = kq[b].astype(BF)
        for h in range(heads):
            both = dot(pair, state[b, h].astype(BF))
            recall[h, pl.ds(b, 1), :] = both[h : h + 1]
            recall[heads + h, pl.ds(b, 1), :] = both[heads + h : heads + h + 1]
        return 0

    lax.fori_loop(0, rows, one_row, 0, unroll=4)
    v_rows = summed(2)
    for h in range(heads):
        q_unit, k_unit = units[h]
        decay, beta = decays[h], betas[h]
        corr = beta * (head_of(v_rows, h) - decay * recall[h])
        read = decay * recall[heads + h] + jnp.sum(q_unit * k_unit, axis=-1, keepdims=True) * corr
        read = read * lax.rsqrt(jnp.mean(read * read, axis=-1, keepdims=True) + EPS) * head_gain[...]
        head_out[:, h * 128 : (h + 1) * 128] = read.astype(BF)
        corr_ref[h] = corr
        decay_ref[h] = jnp.broadcast_to(decay, (rows, 128))

    loads[o_i].wait()
    ho = head_out[...]
    for c in range(n_tp):
        a_send[c] = dot(ho, w_o[:, c * chunk : (c + 1) * chunk]).astype(BF)
    wait_a = exchange(tp_copy, 0, tp_peers, my, lambda p: a_send.at[p], a_recv)
    a_recv[my] = a_send[my]
    own = pl.ds(pl.multiple_of(my * chunk, 128), chunk)

    def update_row(b, _):
        columns = kq[b].T
        for h in range(heads):
            corr = corr_ref[h, pl.ds(b, 1), :]
            decay = decay_ref[h, pl.ds(b, 1), :]
            state[b, h] = decay * state[b, h] + columns[:, h : h + 1] * corr
        return 0

    lax.fori_loop(0, rows, update_row, 0, unroll=2)
    middle = tokens[:, own].astype(F32)
    wait_a()
    for p in range(n_tp):
        middle = middle + a_recv[p].astype(F32)
    x_all[me] = (middle * ffn_gain[:, own]).astype(BF)
    for p in ep_peers:
        ep_copy(5, x_all.at[me], x_all.at[me], p, me).start()
    middle_ref[...] = middle
    s_recv[my] = jnp.broadcast_to(jnp.sum(middle * middle, axis=-1, keepdims=True), (rows, 128))
    wait_s = exchange(tp_copy, 1, tp_peers, my, lambda p: s_recv.at[my], s_recv)
    wait_c()
    for p in range(n_ep):
        c_recv[p] = jnp.broadcast_to(column(c_rows[p, :1, :]), (rows, 128))
    tri = (
        lax.broadcasted_iota(jnp.int32, (group_tokens, group_tokens), 0)
        >= lax.broadcasted_iota(jnp.int32, (group_tokens, group_tokens), 1)
    ).astype(F32).astype(BF)
    slot = lax.broadcasted_iota(jnp.int32, (group_tokens, group_slots), 1).astype(F32)
    for g in range(groups):
        coef = c_recv[g * members : (g + 1) * members].reshape(group_tokens, 128)[:, :1]
        named = coef > 0.0
        flags = jnp.broadcast_to(jnp.where(named, 1.0, 0.0), (group_tokens, 128)).astype(BF)
        rank = dot(tri, flags)[:, :1] - 1.0
        place_ref[g] = jnp.where((rank == slot) & named, 1.0, 0.0).astype(BF)
    wait_s()
    total = s_recv[0]
    for p in range(1, n_tp):
        total = total + s_recv[p]
    scale = lax.rsqrt(total / width + EPS)
    diagonal = lax.broadcasted_iota(jnp.int32, (rows, 128), 0) == lax.broadcasted_iota(
        jnp.int32, (rows, 128), 1
    )
    scale_rows[me] = jnp.broadcast_to(
        jnp.sum(jnp.where(diagonal, scale, 0.0), axis=0, keepdims=True), (8, 128)
    )
    wait_scale = exchange(ep_copy, 7, ep_peers, me, lambda p: scale_rows.at[me], scale_rows)
    core = lax.rem(my, 2)
    line = lax.div(my, 2)
    lines = n_tp // 2
    sibling = my + 1 - 2 * core
    far_lines = [lax.rem(line + d, lines) for d in range(1, lines)]

    def same_core(y):
        return 2 * y + core

    def other_core(y):
        return 2 * y + 1 - core

    def send_g(phase, g):
        block = g_all.at[my, g]
        tp_copy(phase, block, block, sibling, my).start()
        for y in far_lines:
            tp_copy(phase, block, block, same_core(y), my).start()

    def pass_on(phase, g):
        for y in far_lines:
            block = g_all.at[same_core(y), g]
            tp_copy(phase, block, block, same_core(y), same_core(y)).wait_recv()
            pltpu.make_async_remote_copy(
                src_ref=block, dst_ref=block,
                send_sem=tp_send.at[phase, other_core(y)], recv_sem=tp_recv.at[phase, same_core(y)],
                device_id=(me, sibling), device_id_type=MESH,
            ).start()

    def arrived_g(phase, g):
        block = g_all.at[my, g]
        for p in [sibling] + [other_core(y) for y in far_lines]:
            tp_copy(phase, block, g_all.at[p, g], p, p).wait_recv()
        for p in tp_peers:
            tp_copy(phase, block, block, p, my).wait_send()

    group_from = [lax.rem(my_group - offset + groups, groups) for offset in range(groups)]
    for offset in range(groups):
        g = group_from[offset]
        for p in members_of(-offset):
            ep_copy(5, x_all.at[me], x_all.at[p], p, p).wait_recv()
        block = x_all[pl.ds(g * members, members)].astype(F32)
        g_all[my, g] = lax.dot_general(
            place_ref[g], block.reshape(group_tokens, chunk).astype(BF),
            (((0,), (0,)), ((), ())), preferred_element_type=F32,
        ).astype(BF)
        send_g(4 + offset, g)
        if offset > 1:
            pass_on(2 + offset, group_from[offset - 2])
    for i in (dg_i, du_i, eg_i, eu_i, ed_i, dd_i):
        loads[i].wait()
    xs = x_all[...].astype(F32).reshape(batch, chunk).astype(BF)
    hidden = w_dg.shape[1]
    half_rows = batch // 2
    for j, w in enumerate((w_dg, w_du)):
        d_half[:, :, j * hidden : (j + 1) * hidden] = dot(xs, w[...]).reshape(2, half_rows, hidden)
    d_send[1] = d_half[1 - core].astype(BF)
    near_d = tp_copy(2, d_send.at[1], d_near, sibling, sibling)
    tp_copy(2, d_send.at[1], d_near, sibling, my).start()
    if groups > 1:
        pass_on(2 + groups, group_from[groups - 2])
    near_d.wait_recv()
    pre = d_half[core] + d_near[...].astype(F32)
    d_half[0] = pre
    d_send[0] = pre.astype(BF)
    for y in far_lines:
        tp_copy(3, d_send.at[0], d_far.at[line], same_core(y), my).start()
    for p in ep_peers:
        ep_copy(5, x_all.at[me], x_all.at[me], p, me).wait_send()
    wait_scale()
    for p in range(n_ep):
        scale_ref[p] = jnp.broadcast_to(column(scale_rows[p, :1, :]), (rows, 128))
    slot_scale = jnp.concatenate(
        [
            lax.dot_general(
                place_ref[g].astype(F32),
                scale_ref[g * members : (g + 1) * members].reshape(group_tokens, 128),
                (((0,), (0,)), ((), ())), precision=lax.Precision.HIGHEST,
                preferred_element_type=F32,
            )
            for g in range(groups)
        ],
        axis=0,
    )[:, :1]
    pass_on(3 + groups, group_from[groups - 1])
    for offset in range(groups):
        arrived_g(4 + offset, group_from[offset])
    gate = jnp.zeros((slots, w_eg.shape[2]), F32)
    up = jnp.zeros((slots, w_eg.shape[2]), F32)
    for c in range(n_tp):
        routed = g_all[c].astype(F32).reshape(slots, chunk).astype(BF)
        gate = gate + dot(routed, w_eg[0, c * chunk : (c + 1) * chunk, :])
        up = up + dot(routed, w_eu[0, c * chunk : (c + 1) * chunk, :])
    expert_hidden = (silu(gate * slot_scale) * (up * slot_scale)).astype(BF)
    for y in range(lines):
        for c in range(2):
            at = (2 * y + c) * chunk
            part = dot(expert_hidden, w_ed[0, :, at : at + chunk])
            e_part[c, :, y] = part.reshape(groups, group_slots, chunk).astype(BF)
    returns = list(range(1, groups)) + [0]
    group_at = [lax.rem(my_group + offset, groups) for offset in range(groups)]

    def near_e(offset, source):
        g = group_at[offset]
        return tp_copy(
            4 + groups + offset, e_part.at[1 - core, g], e_near.at[g], sibling, source
        )

    def far_e(offset, y, source):
        g = group_at[offset]
        return tp_copy(
            4 + 2 * groups + offset, e_send.at[g, y], e_recv.at[g, lax.div(source, 2)], same_core(y), source
        )

    for offset in returns:
        near_e(offset, my).start()

    for y in far_lines:
        tp_copy(3, d_send.at[0], d_far.at[y], same_core(y), same_core(y)).wait_recv()
    pre = d_half[0]
    for y in far_lines:
        pre = pre + d_far[y].astype(F32)
    half_blocks = n_ep // 2
    pre = pre * scale_ref[pl.ds(core * half_blocks, half_blocks)].reshape(half_rows, 128)[:, :1]
    h_all[core] = (silu(pre[:, :hidden]) * pre[:, hidden:]).astype(BF)
    tp_copy(4 + 3 * groups, h_all.at[core], h_all.at[core], sibling, my).start()
    for offset in returns:
        g = group_at[offset]
        near_e(offset, sibling).wait_recv()
        for y in far_lines:
            e_send[g, y] = (e_part[core, g, y].astype(F32) + e_near[g, y].astype(F32)).astype(BF)
            far_e(offset, y, my).start()
    tp_copy(4 + 3 * groups, h_all.at[core], h_all.at[1 - core], sibling, sibling).wait_recv()
    dense_hidden = h_all[...].astype(F32).reshape(batch, hidden).astype(BF)
    dense = dot(dense_hidden, w_dd[...]) * (1.0 / (1.0 + jnp.exp(-mix[...])))
    dense_ref[...] = dense.reshape(n_ep, rows, chunk)
    for offset in returns:
        g = group_at[offset]
        here = pl.ds(g * members, members)
        result = e_part[core, g, line].astype(F32) + e_near[g, line].astype(F32)
        for y in far_lines:
            far_e(offset, y, same_core(y)).wait_recv()
            result = result + e_recv[g, y].astype(F32)
        coef = c_recv[here].reshape(group_tokens, 128)[:, :1]
        mixed = coef * dot(place_ref[g], result.astype(BF))
        combined = dense_ref[here] + mixed.reshape(members, rows, chunk)
        f_send[here] = combined.astype(BF)
        for p in members_of(offset):
            ep_copy(6, f_send.at[p], f_recv.at[me], p, me).start()
    tp_copy(2, d_send.at[1], d_near, sibling, my).wait_send()
    tp_copy(4 + 3 * groups, h_all.at[core], h_all.at[core], sibling, sibling).wait_send()
    for y in far_lines:
        tp_copy(3, d_send.at[0], d_far.at[line], same_core(y), my).wait_send()
    for offset in range(groups):
        near_e(offset, my).wait_send()
        for y in far_lines:
            far_e(offset, y, my).wait_send()
    final = middle_ref[...] + f_send[me].astype(F32)
    f_recv[me] = jnp.zeros((rows, chunk), BF)
    for p in ep_peers:
        done = ep_copy(6, f_send.at[p], f_recv.at[p], p, p)
        done.wait_recv()
        done.wait_send()
    for p in range(n_ep):
        final = final + f_recv[p].astype(F32)
    out[...] = final.astype(BF)


def per_device(
    tokens, delta_state, attn_gain, query_weight, key_weight, value_weight, decay_weight,
    beta_weight, decay_rate, head_gain, output_weight, ffn_gain, expert_ids, group_prob,
    expert_logit, expert_gate, expert_up, expert_down, dense_gate, dense_up, dense_down, dense_mix,
):
    n_ep = lax.axis_size("ep")
    n_tp = lax.axis_size("tp")
    rows, width = tokens.shape
    heads = delta_state.shape[1]
    local = heads * 128
    topk = expert_ids.shape[1]
    cap = max(2, 2 * rows * topk // n_ep)
    members = 8 // math.gcd(cap, 8)
    if n_ep % members:
        members = n_ep
    groups = n_ep // members
    group_slots = members * cap
    chunk = width // n_tp
    depth = width // n_ep
    batch = n_ep * rows
    hidden = dense_gate.shape[1]
    small = (
        tokens, attn_gain[None, :], decay_rate[None, :], head_gain[None, :], ffn_gain[None, :],
        expert_ids.T, group_prob[None, :], expert_logit.T, dense_mix[None, :],
    )
    weights = (
        delta_state, decay_weight.T, beta_weight.T, query_weight, key_weight, value_weight,
        output_weight, dense_gate, dense_up, expert_gate, expert_up, expert_down, dense_down,
    )
    arrays = tuple(pltpu.with_memory_space_constraint(a, pltpu.HBM) for a in small + weights)
    dims = (n_ep, n_tp, rows, width, heads, members, cap, len(arrays))
    vmem = pl.BlockSpec(memory_space=pltpu.VMEM)
    kq_rows = -(-2 * heads // 8) * 8
    scratch = [pltpu.VMEM(a.shape, a.dtype) for a in small + weights[1:]]
    scratch += [
        pltpu.VMEM(shape, dtype)
        for shape, dtype in (
            ((n_ep, rows, depth), BF), ((n_ep, rows, depth), BF),
            ((3, n_ep, rows, local), BF), ((3, n_ep, rows, local), BF),
            ((n_ep, 8, 128), F32), ((n_ep, 8, 128), F32), ((n_ep, rows, 128), F32),
            ((rows, kq_rows, 128), F32), ((2 * heads, rows, 128), F32),
            ((heads, rows, 128), F32), ((heads, rows, 128), F32), ((rows, local), BF),
            ((n_tp, rows, chunk), BF), ((n_tp, rows, chunk), BF), ((n_tp, rows, 128), F32),
            ((n_ep, 8, 128), F32), ((n_ep, rows, 128), F32), ((rows, chunk), F32), ((n_ep, rows, chunk), BF), ((n_tp, groups, group_slots, chunk), BF),
            ((2, batch // 2, 2 * hidden), F32), ((2, batch // 2, 2 * hidden), BF),
            ((batch // 2, 2 * hidden), BF), ((n_tp // 2, batch // 2, 2 * hidden), BF),
            ((2, batch // 2, hidden), BF),
            ((2, groups, n_tp // 2, group_slots, chunk), BF),
            ((groups, n_tp // 2, group_slots, chunk), BF),
            ((groups, n_tp // 2, group_slots, chunk), BF),
            ((groups, n_tp // 2, group_slots, chunk), BF),
            ((n_ep, rows, chunk), BF), ((n_ep, rows, chunk), BF),
            ((groups, members * rows, group_slots), BF), ((n_ep, rows, chunk), F32),
        )
    ]
    scratch += [
        pltpu.SemaphoreType.DMA((len(arrays),)),
        pltpu.SemaphoreType.DMA((8, n_ep)), pltpu.SemaphoreType.DMA((8, n_ep)),
        pltpu.SemaphoreType.DMA((5 + 3 * groups, n_tp)), pltpu.SemaphoreType.DMA((5 + 3 * groups, n_tp)),
    ]
    mixed_out, new_state = pl.pallas_call(
        functools.partial(kernel, dims),
        out_shape=(
            jax.ShapeDtypeStruct((rows, chunk), BF), pltpu.VMEM(delta_state.shape, F32),
        ),
        in_specs=[pl.BlockSpec(memory_space=pltpu.HBM)] * len(arrays),
        out_specs=(vmem, vmem),
        scratch_shapes=scratch,
        compiler_params=pltpu.CompilerParams(
            collective_id=0, has_side_effects=True, vmem_limit_bytes=44 * 1024 * 1024
        ),
    )(*arrays)
    return mixed_out, new_state


def solution(mesh):
    return jax.shard_map(
        per_device,
        mesh=mesh,
        in_specs=(
            P("ep", None), P("ep", "tp", None, None), P(), P("ep", "tp"), P("ep", "tp"),
            P("ep", "tp"), P(), P(), P("tp"), P(), P("tp", None), P(), P("ep", None), P("ep"),
            P("ep", None), P("ep", None, "tp"), P("ep", None, "tp"), P("ep", "tp", None),
            P("tp", "ep"), P("tp", "ep"), P("ep", "tp"), P("tp"),
        ),
        out_specs=(P("ep", "tp"), P("ep", "tp", None, None)),
        check_vma=False,
    )
```

```python
import functools
import math

import jax
import jax.numpy as jnp
from jax import lax
from jax.experimental import pallas as pl
from jax.experimental.pallas import tpu as pltpu
from jax.sharding import PartitionSpec as P

EPS = 1e-06
BF = jnp.bfloat16
F32 = jnp.float32
MESH = pl.DeviceIdType.MESH


def dot(left, right):
    return jnp.dot(left, right, preferred_element_type=F32)


def dot_t(left, right):
    return lax.dot_general(left, right, (((1,), (1,)), ((), ())), preferred_element_type=F32)


def silu(values):
    return values / (1.0 + jnp.exp(-values))


def far_first(position, count):
    low = 1 - lax.div(2 * position, count)
    order = []
    for k in range(count - 1):
        down = count - 1 - k
        down = down - lax.div(position - down + count, count)
        up = k + lax.div(k - position + count, count)
        order.append(low * down + (1 - low) * up)
    return order


def store_kernel(state, mixed, state_out, mixed_out, sems):
    rows = state.shape[0]
    copies = [pltpu.make_async_copy(mixed, mixed_out, sems.at[rows])]
    copies += [
        pltpu.make_async_copy(state.at[r], state_out.at[r], sems.at[r]) for r in range(rows)
    ]
    for copy in copies:
        copy.start()
    for copy in copies:
        copy.wait()


def semaphores(n_ep, n_tp, groups, n_in):
    pairs, lines = n_ep // 2, n_tp // 2
    sizes = {
        "load": n_in, "ns": 1, "nr": 1, "cs": 1, "cr": 1, "zs": 1, "zr": 1,
        "q1s": 1, "q1r": 3, "q2s": 1, "q2r": 3, "xs": 1, "xr": n_ep,
        "f1s": 1, "f1r": groups, "f2s": 1, "f2r": pairs, "as": 1, "ar": 1, "ss": 1, "sr": 1,
        "d1s": 1, "d1r": 1, "d2s": 1, "d2r": lines, "hs": 1, "hr": 1,
        "gs": 1, "gr": groups * n_tp, "e1s": 1, "e1r": groups, "e2s": 1, "e2r": groups,
    }
    starts, total = {}, 0
    for name, size in sizes.items():
        starts[name] = total
        total += size
    return starts, total


def kernel(dims, *refs):
    n_ep, n_tp, rows, width, heads, members, cap, n_in, starts = dims
    hbm, refs = refs[:n_in], refs[n_in:]
    out, state = refs[:2]
    held = refs[2 : 11] + (state,) + refs[11 : 1 + n_in]
    refs = refs[1 + n_in :]
    (tokens, attn_gain, decay_rate, head_gain, ffn_gain, ids, group_prob, logit, mix) = held[:9]
    state, w_decay, w_beta, w_q, w_k, w_v, w_o, w_dg, w_du, w_eg, w_eu, w_ed, w_dd = held[9:]
    (
        n_send, n_recv, q_away, q_mate, q_own, q_send, q_recv, c_send, c_rows, c_recv, kq, recall,
        corr_ref, decay_ref, head_out, a_send, a_recv, s_recv, scale_rows, scale_ref, middle_ref,
        x_all, g_all, d_half, d_send, d_near, d_far, h_all, e_part, e_near, e_send, e_recv,
        comb, f_away, f_mate, f_send, f_recv, place_ref, dense_ref, sems,
    ) = refs
    me = lax.axis_index("ep")
    my = lax.axis_index("tp")
    chunk = width // n_tp
    depth = width // n_ep
    batch = n_ep * rows
    local = heads * 128
    groups = n_ep // members
    group_slots = members * cap
    group_tokens = members * rows
    slots = groups * group_slots
    pairs = n_ep // 2
    lines = n_tp // 2
    group_pairs = members // 2
    pair = lax.div(me, 2)
    par = lax.rem(me, 2)
    mate = me + 1 - 2 * par
    core = lax.rem(my, 2)
    line = lax.div(my, 2)
    sibling = my + 1 - 2 * core
    my_group = lax.div(pair, group_pairs)
    far_groups = far_first(my_group, groups)
    far_lines = [lax.rem(line + d, lines) for d in range(1, lines)]

    def same_core(y):
        return 2 * y + core

    def other_core(y):
        return 2 * y + 1 - core

    def twin(q):
        return 2 * q + par

    def cross(q):
        return 2 * q + 1 - par

    def pairs_in(g, own=False):
        mine = lax.rem(pair, group_pairs)
        return [
            g * group_pairs + lax.rem(mine + m, group_pairs)
            for m in range(1 if own else 0, group_pairs)
        ]

    others = [q for g in far_groups for q in pairs_in(g)] + pairs_in(my_group, True)
    ep_peers = [p for q in others for p in (cross(q), twin(q))] + [mate]
    far_tp = [p for y in far_lines for p in (same_core(y), other_core(y))]
    tp_peers = far_tp + [sibling]

    def sem(name, index=0):
        return sems.at[starts[name] + index]

    def ep_copy(src, dst, name, peer, index=0):
        return pltpu.make_async_remote_copy(
            src_ref=src, dst_ref=dst, send_sem=sem(name + "s"), recv_sem=sem(name + "r", index),
            device_id=(peer, my), device_id_type=MESH,
        )

    def tp_copy(src, dst, name, peer, index=0):
        return pltpu.make_async_remote_copy(
            src_ref=src, dst_ref=dst, send_sem=sem(name + "s"), recv_sem=sem(name + "r", index),
            device_id=(me, peer), device_id_type=MESH,
        )

    drains = []

    loads = [
        pltpu.make_async_copy(src, dst, sem("load", i))
        for i, (src, dst) in enumerate(zip(hbm, held))
    ]
    state_i, decay_i, beta_i, q_i, k_i, v_i, o_i, dg_i, du_i, eg_i, eu_i, ed_i, dd_i = range(9, 22)
    order = (decay_i, beta_i, k_i, q_i, v_i, state_i, o_i, dg_i, du_i, eg_i, eu_i, ed_i, dd_i)
    for i in range(9):
        loads[i].start()
    barrier = pltpu.get_barrier_semaphore()
    for p in ep_peers:
        pl.semaphore_signal(barrier, inc=1, device_id=(p, my), device_id_type=MESH)
    for p in tp_peers:
        pl.semaphore_signal(barrier, inc=1, device_id=(me, p), device_id_type=MESH)
    for i in order:
        loads[i].start()

    for i in range(9):
        loads[i].wait()
    x = tokens[...].astype(F32)
    mean_sq = jnp.mean(x * x, axis=-1, keepdims=True)
    normed = (x * lax.rsqrt(mean_sq + EPS) * attn_gain[...]).astype(BF)
    for p in range(n_ep):
        n_send[p] = normed[:, p * depth : (p + 1) * depth]
    pl.semaphore_wait(barrier, n_ep + n_tp - 2)
    here = par * pairs + pair
    for p in ep_peers:
        ep_copy(n_send.at[p], n_recv.at[here], "n", p).start()
    n_recv[here] = n_send[me]

    logit_exp = jnp.exp(logit[...])
    route = group_prob[...] * logit_exp / jnp.sum(logit_exp, axis=0, keepdims=True)
    names = ids[...]
    eye = lax.broadcasted_iota(jnp.int32, (rows, rows), 0) == lax.broadcasted_iota(
        jnp.int32, (rows, rows), 1
    )
    c_send[...] = jnp.zeros_like(c_send)
    for p in range(n_ep):
        flat = jnp.sum(jnp.where(names == p, route, 0.0), axis=0, keepdims=True)
        c_send[p, :, :rows] = jnp.broadcast_to(flat, (8, rows))
    for p in ep_peers:
        ep_copy(c_send.at[p], c_rows.at[me], "c", p).start()
    c_rows[me] = c_send[me]

    def column(row):
        return jnp.sum(jnp.where(eye, row[:, :rows], 0.0), axis=1, keepdims=True)

    loads[decay_i].wait()
    loads[beta_i].wait()
    decay_pre = dot_t(normed, w_decay[...])
    beta_pre = dot_t(normed, w_beta[...])
    lane = lax.broadcasted_iota(jnp.int32, decay_pre.shape, 1)
    decays, betas = [], []
    for h in range(heads):
        mine = lane == my * heads + h
        d = jnp.sum(jnp.where(mine, decay_pre, 0.0), axis=1, keepdims=True)
        b = jnp.sum(jnp.where(mine, beta_pre, 0.0), axis=1, keepdims=True)
        soft = jnp.maximum(d, 0.0) + jnp.log1p(jnp.exp(-jnp.abs(d)))
        decays.append(jnp.exp(-decay_rate[:, h : h + 1] * soft))
        betas.append(1.0 / (1.0 + jnp.exp(-b)))
    for i in (q_i, k_i, v_i):
        loads[i].wait()

    most = pl.ds(0, n_ep - 1)
    done_n = ep_copy(n_send.at[most], n_recv.at[most], "n", mate)
    done_n.wait_recv()
    drains.append(done_n)

    def rows_of(parity):
        held_rows = n_recv[pl.ds(parity * pairs, pairs)].astype(F32)
        return held_rows.reshape(pairs * rows, depth).astype(BF)

    away, near = rows_of(1 - par), rows_of(par)
    for j, w in enumerate((w_k, w_q, w_v)):
        q_away[j] = dot(away, w[...]).reshape(pairs, rows, local).astype(BF)
        ep_copy(q_away.at[j], q_mate.at[j], "q1", mate, j).start()
    for j, w in enumerate((w_k, w_q, w_v)):
        q_own[j] = dot(near, w[...]).reshape(pairs, rows, local)
    for j in range(3):
        ep_copy(q_away.at[j], q_mate.at[j], "q1", mate, j).wait_recv()
        both = q_own[j] + q_mate[j].astype(F32)
        q_own[j] = both
        q_send[j] = both.astype(BF)
        for q in others:
            ep_copy(q_send.at[j, q], q_recv.at[j, pair], "q2", twin(q), j).start()
    drains.append(ep_copy(q_away, q_mate, "q1", mate))
    far_blocks = pl.ds(0, pairs - 1)
    sent = q_send.at[pl.ds(0, 3), far_blocks]
    drains.append(ep_copy(sent, q_recv.at[pl.ds(0, 3), far_blocks], "q2", mate))

    def summed(j):
        ep_copy(
            q_send.at[j, far_blocks], q_recv.at[j, far_blocks], "q2", mate, j
        ).wait_recv()
        total = q_own[j, pair]
        for q in others:
            total = total + q_recv[j, q].astype(F32)
        return total.astype(BF).astype(F32)

    k_rows = summed(0)
    q_rows = summed(1)
    loads[state_i].wait()

    def head_of(values, h):
        return values[:, h * 128 : (h + 1) * 128]

    def unit(values):
        return values * lax.rsqrt(jnp.sum(values * values, axis=-1, keepdims=True) + EPS)

    units = []
    for h in range(heads):
        q_unit = unit(head_of(q_rows, h)) * 128 ** (-0.5)
        k_unit = unit(head_of(k_rows, h))
        units.append((q_unit, k_unit))
        kq[:, h, :] = k_unit
        kq[:, heads + h, :] = q_unit

    def one_row(b, _):
        both = kq[b].astype(BF)
        for h in range(heads):
            read = dot(both, state[b, h].astype(BF))
            recall[h, pl.ds(b, 1), :] = read[h : h + 1]
            recall[heads + h, pl.ds(b, 1), :] = read[heads + h : heads + h + 1]
        return 0

    lax.fori_loop(0, rows, one_row, 0, unroll=4)
    v_rows = summed(2)
    for h in range(heads):
        q_unit, k_unit = units[h]
        decay, beta = decays[h], betas[h]
        corr = beta * (head_of(v_rows, h) - decay * recall[h])
        read = decay * recall[heads + h] + jnp.sum(q_unit * k_unit, axis=-1, keepdims=True) * corr
        read = read * lax.rsqrt(jnp.mean(read * read, axis=-1, keepdims=True) + EPS) * head_gain[...]
        head_out[:, h * 128 : (h + 1) * 128] = read.astype(BF)
        corr_ref[h] = corr
        decay_ref[h] = jnp.broadcast_to(decay, (rows, 128))

    loads[o_i].wait()
    ho = head_out[...]

    def columns_of(p):
        return pl.ds(pl.multiple_of(p * chunk, 128), chunk)

    for p in far_tp + [sibling]:
        a_send[p] = dot(ho, w_o[:, columns_of(p)]).astype(BF)
        tp_copy(a_send.at[p], a_recv.at[my], "a", p).start()
    a_recv[my] = dot(ho, w_o[:, columns_of(my)]).astype(BF)
    own = columns_of(my)

    def update_row(b, _):
        columns = kq[b].T
        for h in range(heads):
            corr = corr_ref[h, pl.ds(b, 1), :]
            decay = decay_ref[h, pl.ds(b, 1), :]
            state[b, h] = decay * state[b, h] + columns[:, h : h + 1] * corr
        return 0

    lax.fori_loop(0, rows // 2, update_row, 0, unroll=4)
    middle = tokens[:, own].astype(F32)
    most_tp = pl.ds(0, n_tp - 1)
    done_a = tp_copy(a_send.at[most_tp], a_recv.at[most_tp], "a", sibling)
    done_a.wait_recv()
    drains.append(done_a)
    for p in range(n_tp):
        middle = middle + a_recv[p].astype(F32)
    x_all[me] = (middle * ffn_gain[:, own]).astype(BF)
    for p in [mate] + [twin(q) for q in others]:
        ep_copy(x_all.at[me], x_all.at[me], "x", p, me).start()
    middle_ref[...] = middle
    s_recv[my] = jnp.broadcast_to(jnp.sum(middle * middle, axis=-1, keepdims=True), (rows, 128))
    for p in tp_peers:
        tp_copy(s_recv.at[my], s_recv.at[my], "s", p).start()
    lax.fori_loop(rows // 2, rows, update_row, 0, unroll=4)
    done_c = ep_copy(c_send.at[most], c_rows.at[most], "c", mate)
    done_c.wait_recv()
    drains.append(done_c)
    for p in range(n_ep):
        c_recv[p] = jnp.broadcast_to(column(c_rows[p, :1, :]), (rows, 128))
    tri = (
        lax.broadcasted_iota(jnp.int32, (group_tokens, group_tokens), 0)
        >= lax.broadcasted_iota(jnp.int32, (group_tokens, group_tokens), 1)
    ).astype(F32).astype(BF)
    slot = lax.broadcasted_iota(jnp.int32, (group_tokens, group_slots), 1).astype(F32)
    for g in range(groups):
        coef = c_recv[g * members : (g + 1) * members].reshape(group_tokens, 128)[:, :1]
        named = coef > 0.0
        flags = jnp.broadcast_to(jnp.where(named, 1.0, 0.0), (group_tokens, 128)).astype(BF)
        rank = dot(tri, flags)[:, :1] - 1.0
        place_ref[g] = jnp.where((rank == slot) & named, 1.0, 0.0).astype(BF)
    done_s = tp_copy(s_recv.at[most_tp], s_recv.at[most_tp], "s", sibling)
    done_s.wait_recv()
    drains.append(done_s)
    total = s_recv[0]
    for p in range(1, n_tp):
        total = total + s_recv[p]
    scale = lax.rsqrt(total / width + EPS)
    diagonal = lax.broadcasted_iota(jnp.int32, (rows, 128), 0) == lax.broadcasted_iota(
        jnp.int32, (rows, 128), 1
    )
    scale_rows[me] = jnp.broadcast_to(
        jnp.sum(jnp.where(diagonal, scale, 0.0), axis=0, keepdims=True), (8, 128)
    )
    for p in ep_peers:
        ep_copy(scale_rows.at[me], scale_rows.at[me], "z", p).start()

    def send_g(k, g):
        block = g_all.at[my, g]
        for p in [same_core(y) for y in far_lines] + [sibling]:
            tp_copy(block, block, "g", p, k * n_tp + my).start()

    def pass_on(k, g):
        for y in far_lines:
            p = same_core(y)
            block = g_all.at[p, g]
            tp_copy(block, block, "g", p, k * n_tp + p).wait_recv()
            tp_copy(block, block, "g", sibling, k * n_tp + p).start()

    def arrived_g(k, g, p):
        block = g_all.at[p, g]
        tp_copy(block, block, "g", p, k * n_tp + p).wait_recv()

    def forward_x(g, own_group):
        for q in pairs_in(g, own_group):
            block = x_all.at[twin(q)]
            ep_copy(block, block, "x", twin(q), twin(q)).wait_recv()
            ep_copy(block, block, "x", mate, twin(q)).start()

    group_from = [my_group] + far_groups
    forward_x(my_group, True)
    for k in range(groups):
        g = group_from[k]
        if k + 1 < groups:
            forward_x(group_from[k + 1], False)
        for q in pairs_in(g, k == 0) + ([pair] if k == 0 else []):
            ep_copy(x_all.at[me], x_all.at[cross(q)], "x", mate, cross(q)).wait_recv()
        block = x_all[pl.ds(g * members, members)].astype(F32)
        g_all[my, g] = lax.dot_general(
            place_ref[g], block.reshape(group_tokens, chunk).astype(BF),
            (((0,), (0,)), ((), ())), preferred_element_type=F32,
        ).astype(BF)
        send_g(k, g)
        if k > 1:
            pass_on(k - 2, group_from[k - 2])
    drains.append(ep_copy(x_all.at[most], x_all.at[most], "x", mate))
    drains.append(tp_copy(g_all.at[most_tp], g_all.at[most_tp], "g", sibling))
    for i in (dg_i, du_i, eg_i, eu_i, ed_i, dd_i):
        loads[i].wait()
    xs = x_all[...].astype(F32).reshape(batch, chunk).astype(BF)
    hidden = w_dg.shape[1]
    half_rows = batch // 2
    for j, w in enumerate((w_dg, w_du)):
        d_half[:, :, j * hidden : (j + 1) * hidden] = dot(xs, w[...]).reshape(2, half_rows, hidden)
    d_send[1] = d_half[1 - core].astype(BF)
    near_d = tp_copy(d_send.at[1], d_near, "d1", sibling)
    near_d.start()
    drains.append(near_d)
    if groups > 1:
        pass_on(groups - 2, group_from[groups - 2])

    def expert_in(p, gate, up):
        routed = g_all[p].astype(F32).reshape(slots, chunk).astype(BF)
        return (
            gate + dot(routed, w_eg[0, columns_of(p), :]), up + dot(routed, w_eu[0, columns_of(p), :])
        )

    gate = jnp.zeros((slots, w_eg.shape[2]), F32)
    gate, up = expert_in(my, gate, gate)
    for k in range(groups):
        arrived_g(k, group_from[k], sibling)
    gate, up = expert_in(sibling, gate, up)
    near_d.wait_recv()
    pre = d_half[core] + d_near[...].astype(F32)
    d_half[0] = pre
    d_send[0] = pre.astype(BF)
    for y in far_lines:
        tp_copy(d_send.at[0], d_far.at[line], "d2", same_core(y), line).start()
    for y in far_lines:
        drains.append(tp_copy(d_send.at[0], d_far.at[line], "d2", same_core(y), line))
    pass_on(groups - 1, group_from[groups - 1])
    done_z = ep_copy(scale_rows.at[most], scale_rows.at[most], "z", mate)
    done_z.wait_recv()
    drains.append(done_z)
    for p in range(n_ep):
        scale_ref[p] = jnp.broadcast_to(column(scale_rows[p, :1, :]), (rows, 128))
    slot_scale = jnp.concatenate(
        [
            lax.dot_general(
                place_ref[g].astype(F32),
                scale_ref[g * members : (g + 1) * members].reshape(group_tokens, 128),
                (((0,), (0,)), ((), ())), precision=lax.Precision.HIGHEST,
                preferred_element_type=F32,
            )
            for g in range(groups)
        ],
        axis=0,
    )[:, :1]
    for y in far_lines:
        gate, up = expert_in(same_core(y), gate, up)
    for y in far_lines:
        for k in range(groups):
            arrived_g(k, group_from[k], other_core(y))
        gate, up = expert_in(other_core(y), gate, up)
    expert_hidden = (silu(gate * slot_scale) * (up * slot_scale)).astype(BF)
    returns = far_groups + [my_group]

    def near_e(k):
        g = returns[k]
        return tp_copy(e_part.at[1 - core, g], e_near.at[g], "e1", sibling, k)

    def far_e(k, y):
        g = returns[k]
        return tp_copy(e_send.at[g, y], e_recv.at[g, line], "e2", same_core(y), k)

    def expert_out(which, y):
        part = dot(expert_hidden, w_ed[0, :, columns_of(2 * y + which)])
        e_part[which, :, y] = part.reshape(groups, group_slots, chunk).astype(BF)

    for y in range(lines):
        expert_out(1 - core, y)
    for k in range(groups):
        near_e(k).start()
    for y in range(lines):
        expert_out(core, y)
    for k in range(groups):
        g = returns[k]
        near_e(k).wait_recv()
        for y in far_lines:
            e_send[g, y] = (e_part[core, g, y].astype(F32) + e_near[g, y].astype(F32)).astype(BF)
            far_e(k, y).start()
    drains.append(tp_copy(e_part.at[0], e_near, "e1", sibling))
    other_lines = pl.ds(0, lines - 1)
    sent = e_send.at[pl.ds(0, groups), other_lines]
    drains.append(tp_copy(sent, e_recv.at[pl.ds(0, groups), other_lines], "e2", sibling))
    pre = d_half[0]
    for y in far_lines:
        tp_copy(d_send.at[0], d_far.at[y], "d2", same_core(y), y).wait_recv()
        pre = pre + d_far[y].astype(F32)
    half_blocks = n_ep // 2
    pre = pre * scale_ref[pl.ds(core * half_blocks, half_blocks)].reshape(half_rows, 128)[:, :1]
    h_all[core] = (silu(pre[:, :hidden]) * pre[:, hidden:]).astype(BF)
    sent_h = tp_copy(h_all.at[core], h_all.at[core], "h", sibling)
    sent_h.start()
    drains.append(sent_h)
    tp_copy(h_all.at[core], h_all.at[1 - core], "h", sibling).wait_recv()
    dense_hidden = h_all[...].astype(F32).reshape(batch, hidden).astype(BF)
    dense = dot(dense_hidden, w_dd[...]) * (1.0 / (1.0 + jnp.exp(-mix[...])))
    dense_ref[...] = dense.reshape(n_ep, rows, chunk)

    def near_f(k):
        g = returns[k]
        return ep_copy(f_away.at[g], f_mate.at[g], "f1", mate, k)

    def far_f(k):
        g = returns[k]
        near_f(k).wait_recv()
        both = comb[g, par] + f_mate[g].astype(F32)
        comb[g, par] = both
        f_send[pl.ds(g * group_pairs, group_pairs)] = both.astype(BF)
        for q in pairs_in(g, k == groups - 1):
            ep_copy(f_send.at[q], f_recv.at[pair], "f2", twin(q), pair).start()

    for k in range(groups):
        g = returns[k]
        block = pl.ds(g * members, members)
        result = e_part[core, g, line].astype(F32) + e_near[g, line].astype(F32)
        tp_copy(e_send.at[g, other_lines], e_recv.at[g, other_lines], "e2", sibling, k).wait_recv()
        for y in far_lines:
            result = result + e_recv[g, y].astype(F32)
        coef = c_recv[block].reshape(group_tokens, 128)[:, :1]
        mixed = coef * dot(place_ref[g], result.astype(BF))
        combined = dense_ref[block] + mixed.reshape(members, rows, chunk)
        for m in range(members):
            comb[g, m % 2, m // 2] = combined[m]
        f_away[g] = comb[g, 1 - par].astype(BF)
        near_f(k).start()
        if k > 0:
            far_f(k - 1)
    far_f(groups - 1)
    drains.append(ep_copy(f_away, f_mate, "f1", mate))
    drains.append(ep_copy(f_send.at[far_blocks], f_recv.at[far_blocks], "f2", mate))
    final = middle_ref[...] + comb[my_group, par, lax.rem(pair, group_pairs)]
    for q in others:
        ep_copy(f_send.at[q], f_recv.at[q], "f2", twin(q), q).wait_recv()
        final = final + f_recv[q].astype(F32)
    out[...] = final.astype(BF)
    for copy in drains:
        copy.wait_send()


def per_device(
    tokens, delta_state, attn_gain, query_weight, key_weight, value_weight, decay_weight,
    beta_weight, decay_rate, head_gain, output_weight, ffn_gain, expert_ids, group_prob,
    expert_logit, expert_gate, expert_up, expert_down, dense_gate, dense_up, dense_down, dense_mix,
):
    n_ep = lax.axis_size("ep")
    n_tp = lax.axis_size("tp")
    rows, width = tokens.shape
    heads = delta_state.shape[1]
    local = heads * 128
    topk = expert_ids.shape[1]
    cap = max(2, 2 * rows * topk // n_ep)
    members = max(2, 8 // math.gcd(cap, 8))
    if n_ep % members:
        members = n_ep
    groups = n_ep // members
    group_slots = members * cap
    chunk = width // n_tp
    depth = width // n_ep
    batch = n_ep * rows
    pairs = n_ep // 2
    lines = n_tp // 2
    hidden = dense_gate.shape[1]
    small = (
        tokens, attn_gain[None, :], decay_rate[None, :], head_gain[None, :], ffn_gain[None, :],
        expert_ids.T, group_prob[None, :], expert_logit.T, dense_mix[None, :],
    )
    weights = (
        delta_state, decay_weight.T, beta_weight.T, query_weight, key_weight, value_weight,
        output_weight, dense_gate, dense_up, expert_gate, expert_up, expert_down, dense_down,
    )
    arrays = tuple(pltpu.with_memory_space_constraint(a, pltpu.HBM) for a in small + weights)
    starts, n_sems = semaphores(n_ep, n_tp, groups, len(arrays))
    dims = (n_ep, n_tp, rows, width, heads, members, cap, len(arrays), starts)
    vmem = pl.BlockSpec(memory_space=pltpu.VMEM)
    kq_rows = -(-2 * heads // 8) * 8
    scratch = [pltpu.VMEM(a.shape, a.dtype) for a in small + weights[1:]]
    scratch += [
        pltpu.VMEM(shape, dtype)
        for shape, dtype in (
            ((n_ep, rows, depth), BF), ((n_ep, rows, depth), BF),
            ((3, pairs, rows, local), BF), ((3, pairs, rows, local), BF),
            ((3, pairs, rows, local), F32),
            ((3, pairs, rows, local), BF), ((3, pairs, rows, local), BF),
            ((n_ep, 8, 128), F32), ((n_ep, 8, 128), F32), ((n_ep, rows, 128), F32),
            ((rows, kq_rows, 128), F32), ((2 * heads, rows, 128), F32),
            ((heads, rows, 128), F32), ((heads, rows, 128), F32), ((rows, local), BF),
            ((n_tp, rows, chunk), BF), ((n_tp, rows, chunk), BF), ((n_tp, rows, 128), F32),
            ((n_ep, 8, 128), F32), ((n_ep, rows, 128), F32), ((rows, chunk), F32),
            ((n_ep, rows, chunk), BF), ((n_tp, groups, group_slots, chunk), BF),
            ((2, batch // 2, 2 * hidden), F32), ((2, batch // 2, 2 * hidden), BF),
            ((batch // 2, 2 * hidden), BF), ((lines, batch // 2, 2 * hidden), BF),
            ((2, batch // 2, hidden), BF),
            ((2, groups, lines, group_slots, chunk), BF), ((groups, lines, group_slots, chunk), BF),
            ((groups, lines, group_slots, chunk), BF), ((groups, lines, group_slots, chunk), BF),
            ((groups, 2, members // 2, rows, chunk), F32),
            ((groups, members // 2, rows, chunk), BF), ((groups, members // 2, rows, chunk), BF),
            ((pairs, rows, chunk), BF), ((pairs, rows, chunk), BF),
            ((groups, members * rows, group_slots), BF), ((n_ep, rows, chunk), F32),
        )
    ]
    scratch += [pltpu.SemaphoreType.DMA((n_sems,))]
    mixed_out, new_state = pl.pallas_call(
        functools.partial(kernel, dims),
        out_shape=(pltpu.VMEM((rows, chunk), BF), pltpu.VMEM(delta_state.shape, F32)),
        in_specs=[pl.BlockSpec(memory_space=pltpu.HBM)] * len(arrays),
        out_specs=(vmem, vmem),
        scratch_shapes=scratch,
        compiler_params=pltpu.CompilerParams(
            collective_id=0, has_side_effects=True, vmem_limit_bytes=44 * 1024 * 1024
        ),
    )(*arrays)
    new_state, mixed_out = pl.pallas_call(
        store_kernel,
        out_shape=(pltpu.HBM(delta_state.shape, F32), pltpu.HBM((rows, chunk), BF)),
        in_specs=[vmem] * 2,
        out_specs=(pl.BlockSpec(memory_space=pltpu.HBM),) * 2,
        scratch_shapes=[pltpu.SemaphoreType.DMA((rows + 1,))],
        compiler_params=pltpu.CompilerParams(vmem_limit_bytes=8 * 1024 * 1024),
    )(*(pltpu.with_memory_space_constraint(a, pltpu.VMEM) for a in (new_state, mixed_out)))
    return mixed_out, new_state


def solution(mesh):
    return jax.shard_map(
        per_device,
        mesh=mesh,
        in_specs=(
            P("ep", None), P("ep", "tp", None, None), P(), P("ep", "tp"), P("ep", "tp"),
            P("ep", "tp"), P(), P(), P("tp"), P(), P("tp", None), P(), P("ep", None), P("ep"),
            P("ep", None), P("ep", None, "tp"), P("ep", None, "tp"), P("ep", "tp", None),
            P("tp", "ep"), P("tp", "ep"), P("ep", "tp"), P("tp"),
        ),
        out_specs=(P("ep", "tp"), P("ep", "tp", None, None)),
        check_vma=False,
    )
```

```python
import functools
import math

import jax
import jax.numpy as jnp
from jax import lax
from jax.experimental import pallas as pl
from jax.experimental.pallas import tpu as pltpu
from jax.sharding import PartitionSpec as P

EPS = 1e-06
CROSS_AT = 2
RECALL = 4
UPDATE = 4
X_STRAIGHT = (2,)
F_STRAIGHT = (0, 2)
X_SENDS = (0, 1, 2)
X_ORDER = (2, 0, 1)
BF = jnp.bfloat16
F32 = jnp.float32
MESH = pl.DeviceIdType.MESH


def dot(left, right):
    return jnp.dot(left, right, preferred_element_type=F32)


def dot_t(left, right):
    return lax.dot_general(left, right, (((1,), (1,)), ((), ())), preferred_element_type=F32)


def silu(values):
    return values / (1.0 + jnp.exp(-values))


def far_first(position, count):
    low = 1 - lax.div(2 * position, count)
    order = []
    for k in range(count - 1):
        down = count - 1 - k
        down = down - lax.div(position - down + count, count)
        up = k + lax.div(k - position + count, count)
        order.append(low * down + (1 - low) * up)
    return order


def partners(position, count):
    if count == 4:
        low, high = lax.rem(position, 2), lax.div(position, 2)
        return [3 - position, position + 2 - 4 * high, position + 1 - 2 * low]
    return far_first(position, count)


def store_kernel(state, mixed, state_out, mixed_out, sems):
    rows = state.shape[0]
    small = pltpu.make_async_copy(mixed, mixed_out, sems.at[1])
    small.start()
    for r in range(rows):
        pltpu.make_async_copy(state.at[r], state_out.at[r], sems.at[0]).start()
    pltpu.make_async_copy(state, state_out, sems.at[0]).wait()
    small.wait()


def dense_steps(groups):
    return 1 if groups % 2 else groups // 2


def semaphores(n_ep, n_tp, members, n_in):
    groups = n_ep // members
    pairs, lines = n_ep // 2, n_tp // 2
    steps = dense_steps(groups)
    sizes = {
        "load": n_in, "ns": 1, "nr": pairs + 1, "ms": 1, "mr": 1, "cs": 1, "cr": 1, "zs": 1, "zr": 1,
        "q1s": 1, "q1r": 2, "q2s": 1, "q2r": 2, "k1s": 1, "k1r": 1, "k2s": 1, "k2r": 1, "xs": 1, "xr": n_ep,
        "f1s": 1, "f1r": groups, "f2s": 1, "f2r": n_ep, "as": 1, "ar": 1, "ss": 1, "sr": 1,
        "d1s": 1, "d1r": steps, "d2s": 1, "d2r": steps * lines, "hs": 1, "hr": steps,
        "gs": 1, "gr": groups * n_tp, "e1s": 1, "e1r": groups, "e2s": 1, "e2r": groups,
    }
    starts, total = {}, 0
    for name, size in sizes.items():
        starts[name] = total
        total += size
    return starts, total


def kernel(dims, *refs):
    n_ep, n_tp, rows, width, heads, members, cap, n_in, starts = dims
    hbm, refs = refs[:n_in], refs[n_in:]
    out, state = refs[:2]
    held = refs[2 : 11] + (state,) + refs[11 : 1 + n_in]
    refs = refs[1 + n_in :]
    (tokens, attn_gain, decay_rate, head_gain, ffn_gain, ids, group_prob, logit, mix) = held[:9]
    state, w_decay, w_beta, w_q, w_k, w_v, w_o, w_dg, w_du, w_eg, w_eu, w_ed, w_dd = held[9:]
    (
        n_send, n_recv, k_own, k_send, k_recv, k_away, k_mate, q_away, q_mate, q_own, q_send, q_recv, c_send, c_rows, c_recv, kq, recall,
        corr_ref, decay_ref, head_out, a_send, a_recv, s_recv, scale_rows, scale_ref, middle_ref,
        x_all, g_all, d_half, d_send, d_near, d_far, h_all, e_part, e_near, e_send, e_recv,
        comb, f_away, f_mate, f_send, f_recv, place_ref, dense_ref, sems,
    ) = refs
    me = lax.axis_index("ep")
    my = lax.axis_index("tp")
    chunk = width // n_tp
    depth = width // n_ep
    batch = n_ep * rows
    local = heads * 128
    groups = n_ep // members
    group_slots = members * cap
    group_tokens = members * rows
    slots = groups * group_slots
    pairs = n_ep // 2
    lines = n_tp // 2
    group_pairs = members // 2
    pair = lax.div(me, 2)
    par = lax.rem(me, 2)
    mate = me + 1 - 2 * par
    core = lax.rem(my, 2)
    line = lax.div(my, 2)
    sibling = my + 1 - 2 * core
    my_group = lax.div(pair, group_pairs)
    far_groups = partners(my_group, groups)
    x_straight = {4: X_STRAIGHT, 2: (0,)}.get(groups, ())
    f_straight = {4: F_STRAIGHT, 2: (0,)}.get(groups, ())
    x_sends = X_SENDS if groups == 4 else range(groups - 1)
    x_order = X_ORDER if groups == 4 else range(groups - 1)
    far_lines = [lax.rem(line + d, lines) for d in range(1, lines)]

    def same_core(y):
        return 2 * y + core

    def other_core(y):
        return 2 * y + 1 - core

    def twin(q):
        return 2 * q + par

    def cross(q):
        return 2 * q + 1 - par

    def pairs_in(g, own=False):
        mine = lax.rem(pair, group_pairs)
        return [
            g * group_pairs + lax.rem(mine + m, group_pairs)
            for m in range(1 if own else 0, group_pairs)
        ]

    others = [q for g in far_groups for q in pairs_in(g)] + pairs_in(my_group, True)
    ep_peers = [p for q in others for p in (cross(q), twin(q))] + [mate]
    far_tp = [p for y in far_lines for p in (same_core(y), other_core(y))]
    tp_peers = far_tp + [sibling]

    def sem(name, index=0):
        return sems.at[starts[name] + index]

    def ep_copy(src, dst, name, peer, index=0):
        return pltpu.make_async_remote_copy(
            src_ref=src, dst_ref=dst, send_sem=sem(name + "s"), recv_sem=sem(name + "r", index),
            device_id=(peer, my), device_id_type=MESH,
        )

    def tp_copy(src, dst, name, peer, index=0):
        return pltpu.make_async_remote_copy(
            src_ref=src, dst_ref=dst, send_sem=sem(name + "s"), recv_sem=sem(name + "r", index),
            device_id=(me, peer), device_id_type=MESH,
        )

    drains = []

    loads = [
        pltpu.make_async_copy(src, dst, sem("load", i))
        for i, (src, dst) in enumerate(zip(hbm, held))
    ]
    state_i, decay_i, beta_i, q_i, k_i, v_i, o_i, dg_i, du_i, eg_i, eu_i, ed_i, dd_i = range(9, 22)
    order = (decay_i, beta_i, k_i, q_i, v_i, state_i, o_i, dg_i, du_i, eg_i, eu_i, ed_i, dd_i)
    for i in range(9):
        loads[i].start()
    barrier = pltpu.get_barrier_semaphore()
    for p in ep_peers:
        pl.semaphore_signal(barrier, inc=1, device_id=(p, my), device_id_type=MESH)
    for p in tp_peers:
        pl.semaphore_signal(barrier, inc=1, device_id=(me, p), device_id_type=MESH)
    for i in order:
        loads[i].start()

    for i in range(9):
        loads[i].wait()
    x = tokens[...].astype(F32)
    mean_sq = jnp.mean(x * x, axis=-1, keepdims=True)
    normed = (x * lax.rsqrt(mean_sq + EPS) * attn_gain[...]).astype(BF)
    for p in range(n_ep):
        n_send[p] = normed[:, p * depth : (p + 1) * depth]
    pl.semaphore_wait(barrier, n_ep + n_tp - 2)
    def shelf(p):
        return lax.rem(p, 2) * pairs + lax.div(p, 2)

    def carried(q):
        return 2 * q + lax.rem(par + pair + q + core, 2)

    for q in others:
        ep_copy(n_send.at[carried(q)], n_recv.at[shelf(me)], "n", carried(q), pair).start()
    ep_copy(n_send.at[mate], n_recv.at[shelf(me)], "n", mate, pairs).start()
    n_recv[shelf(me)] = n_send[me]

    logit_exp = jnp.exp(logit[...])
    route = group_prob[...] * logit_exp / jnp.sum(logit_exp, axis=0, keepdims=True)
    names = ids[...]
    eye = lax.broadcasted_iota(jnp.int32, (rows, rows), 0) == lax.broadcasted_iota(
        jnp.int32, (rows, rows), 1
    )
    c_send[...] = jnp.zeros_like(c_send)
    for p in range(n_ep):
        flat = jnp.sum(jnp.where(names == p, route, 0.0), axis=0, keepdims=True)
        c_send[p, :, :rows] = jnp.broadcast_to(flat, (8, rows))
    for p in ep_peers:
        ep_copy(c_send.at[p], c_rows.at[me], "c", p).start()
    c_rows[me] = c_send[me]

    def column(row):
        return jnp.sum(jnp.where(eye, row[:, :rows], 0.0), axis=1, keepdims=True)

    loads[decay_i].wait()
    loads[beta_i].wait()
    decay_pre = dot_t(normed, w_decay[...])
    beta_pre = dot_t(normed, w_beta[...])
    lane = lax.broadcasted_iota(jnp.int32, decay_pre.shape, 1)
    decays, betas = [], []
    for h in range(heads):
        mine = lane == my * heads + h
        d = jnp.sum(jnp.where(mine, decay_pre, 0.0), axis=1, keepdims=True)
        b = jnp.sum(jnp.where(mine, beta_pre, 0.0), axis=1, keepdims=True)
        soft = jnp.maximum(d, 0.0) + jnp.log1p(jnp.exp(-jnp.abs(d)))
        decays.append(jnp.exp(-decay_rate[:, h : h + 1] * soft))
        betas.append(1.0 / (1.0 + jnp.exp(-b)))
    for i in (q_i, k_i, v_i):
        loads[i].wait()

    most = pl.ds(0, n_ep - 1)
    some = pl.ds(0, pairs - 1)
    for q in others:
        block = n_recv.at[shelf(carried(q))]
        ep_copy(block, block, "n", mate, q).wait_recv()
        tp_copy(block, block, "m", sibling).start()
    ep_copy(n_send.at[mate], n_recv.at[shelf(mate)], "n", mate, pairs).wait_recv()
    drains.append(ep_copy(n_send.at[pl.ds(0, pairs)], n_recv.at[pl.ds(0, pairs)], "n", mate))
    passed = tp_copy(n_recv.at[some], n_recv.at[some], "m", sibling)
    passed.wait_recv()
    drains.append(passed)

    def rows_of(parity):
        held_rows = n_recv[pl.ds(parity * pairs, pairs)].astype(F32)
        return held_rows.reshape(pairs * rows, depth).astype(BF)

    away, near = rows_of(1 - par), rows_of(par)
    k_part = dot(jnp.concatenate([away, near], axis=0), w_k[...]).reshape(2, pairs, rows, local)
    k_own[...] = k_part
    for side in range(2):
        k_send[:, side] = k_part[side].astype(BF)
    for q in others:
        ep_copy(k_send.at[q], k_recv.at[pair], "k1", twin(q)).start()
    for j, w in enumerate((w_q, w_v)):
        q_away[j] = dot(away, w[...]).reshape(pairs, rows, local).astype(BF)
        ep_copy(q_away.at[j], q_mate.at[j], "q1", mate, j).start()
    for j, w in enumerate((w_q, w_v)):
        q_own[j] = dot(near, w[...]).reshape(pairs, rows, local)
    for j in range(2):
        ep_copy(q_away.at[j], q_mate.at[j], "q1", mate, j).wait_recv()
        both = q_own[j] + q_mate[j].astype(F32)
        q_own[j] = both
        q_send[j] = both.astype(BF)
        for q in others:
            ep_copy(q_send.at[j, q], q_recv.at[j, pair], "q2", twin(q), j).start()
    drains.append(ep_copy(q_away, q_mate, "q1", mate))
    far_blocks = pl.ds(0, pairs - 1)
    sent = q_send.at[pl.ds(0, 2), far_blocks]
    drains.append(ep_copy(sent, q_recv.at[pl.ds(0, 2), far_blocks], "q2", mate))
    done_k = ep_copy(k_send.at[far_blocks], k_recv.at[far_blocks], "k1", mate)
    done_k.wait_recv()
    drains.append(done_k)
    sums = []
    for side in range(2):
        total = k_own[side, pair]
        for q in others:
            total = total + k_recv[q, side].astype(F32)
        sums.append(total)
        if side == 0:
            k_away[...] = total.astype(BF)
            cross_k = ep_copy(k_away, k_mate, "k2", mate)
            cross_k.start()
            drains.append(cross_k)

    def summed(j):
        ep_copy(
            q_send.at[j, far_blocks], q_recv.at[j, far_blocks], "q2", mate, j
        ).wait_recv()
        total = q_own[j, pair]
        for q in others:
            total = total + q_recv[j, q].astype(F32)
        return total.astype(BF).astype(F32)

    q_rows = summed(0)
    cross_k.wait_recv()
    k_rows = (sums[1] + k_mate[...].astype(F32)).astype(BF).astype(F32)
    loads[state_i].wait()

    def head_of(values, h):
        return values[:, h * 128 : (h + 1) * 128]

    def unit(values):
        return values * lax.rsqrt(jnp.sum(values * values, axis=-1, keepdims=True) + EPS)

    units = []
    for h in range(heads):
        q_unit = unit(head_of(q_rows, h)) * 128 ** (-0.5)
        k_unit = unit(head_of(k_rows, h))
        units.append((q_unit, k_unit))
        kq[:, h, :] = k_unit
        kq[:, heads + h, :] = q_unit

    beside = 2 if heads % 2 == 0 else 1

    def one_row(b, _):
        both = kq[b].astype(BF)
        for first in range(0, heads, beside):
            pieces = [state[b, first + i].astype(BF) for i in range(beside)]
            read = dot(both, jnp.concatenate(pieces, axis=1))
            for i in range(beside):
                h, lanes = first + i, slice(i * 128, (i + 1) * 128)
                recall[h, pl.ds(b, 1), :] = read[h : h + 1, lanes]
                recall[heads + h, pl.ds(b, 1), :] = read[heads + h : heads + h + 1, lanes]
        return 0

    lax.fori_loop(0, rows, one_row, 0, unroll=RECALL)
    v_rows = summed(1)
    for h in range(heads):
        q_unit, k_unit = units[h]
        decay, beta = decays[h], betas[h]
        corr = beta * (head_of(v_rows, h) - decay * recall[h])
        read = decay * recall[heads + h] + jnp.sum(q_unit * k_unit, axis=-1, keepdims=True) * corr
        read = read * lax.rsqrt(jnp.mean(read * read, axis=-1, keepdims=True) + EPS) * head_gain[...]
        head_out[:, h * 128 : (h + 1) * 128] = read.astype(BF)
        corr_ref[h] = corr
        decay_ref[h] = jnp.broadcast_to(decay, (rows, 128))

    loads[o_i].wait()
    ho = head_out[...]

    def columns_of(p):
        return pl.ds(pl.multiple_of(p * chunk, 128), chunk)

    for p in far_tp + [sibling]:
        a_send[p] = dot(ho, w_o[:, columns_of(p)]).astype(BF)
        tp_copy(a_send.at[p], a_recv.at[my], "a", p).start()
    a_recv[my] = dot(ho, w_o[:, columns_of(my)]).astype(BF)
    own = columns_of(my)

    def update_row(b, _):
        columns = kq[b].T
        for h in range(heads):
            corr = corr_ref[h, pl.ds(b, 1), :]
            decay = decay_ref[h, pl.ds(b, 1), :]
            state[b, h] = decay * state[b, h] + columns[:, h : h + 1] * corr
        return 0

    lax.fori_loop(0, rows // 2, update_row, 0, unroll=UPDATE)
    middle = tokens[:, own].astype(F32)
    most_tp = pl.ds(0, n_tp - 1)
    done_a = tp_copy(a_send.at[most_tp], a_recv.at[most_tp], "a", sibling)
    done_a.wait_recv()
    drains.append(done_a)
    for p in range(n_tp):
        middle = middle + a_recv[p].astype(F32)
    x_all[me] = (middle * ffn_gain[:, own]).astype(BF)
    x_peers = [mate] + [twin(q) for q in pairs_in(my_group, True)]
    for i in x_sends:
        x_peers += [twin(q) for q in pairs_in(far_groups[i])]
        if i in x_straight:
            x_peers += [cross(q) for q in pairs_in(far_groups[i])]
    for p in x_peers:
        ep_copy(x_all.at[me], x_all.at[me], "x", p, me).start()
    middle_ref[...] = middle
    s_recv[my] = jnp.broadcast_to(jnp.sum(middle * middle, axis=-1, keepdims=True), (rows, 128))
    for p in tp_peers:
        tp_copy(s_recv.at[my], s_recv.at[my], "s", p).start()
    lax.fori_loop(rows // 2, rows, update_row, 0, unroll=UPDATE)
    done_c = ep_copy(c_send.at[most], c_rows.at[most], "c", mate)
    done_c.wait_recv()
    drains.append(done_c)
    for p in range(n_ep):
        c_recv[p] = jnp.broadcast_to(column(c_rows[p, :1, :]), (rows, 128))
    tri = (
        lax.broadcasted_iota(jnp.int32, (group_tokens, group_tokens), 0)
        >= lax.broadcasted_iota(jnp.int32, (group_tokens, group_tokens), 1)
    ).astype(F32).astype(BF)
    slot = lax.broadcasted_iota(jnp.int32, (group_tokens, group_slots), 1).astype(F32)
    for g in range(groups):
        coef = c_recv[g * members : (g + 1) * members].reshape(group_tokens, 128)[:, :1]
        named = coef > 0.0
        flags = jnp.broadcast_to(jnp.where(named, 1.0, 0.0), (group_tokens, 128)).astype(BF)
        rank = dot(tri, flags)[:, :1] - 1.0
        place_ref[g] = jnp.where((rank == slot) & named, 1.0, 0.0).astype(BF)
    done_s = tp_copy(s_recv.at[most_tp], s_recv.at[most_tp], "s", sibling)
    done_s.wait_recv()
    drains.append(done_s)
    total = s_recv[0]
    for p in range(1, n_tp):
        total = total + s_recv[p]
    scale = lax.rsqrt(total / width + EPS)
    diagonal = lax.broadcasted_iota(jnp.int32, (rows, 128), 0) == lax.broadcasted_iota(
        jnp.int32, (rows, 128), 1
    )
    scale_rows[me] = jnp.broadcast_to(
        jnp.sum(jnp.where(diagonal, scale, 0.0), axis=0, keepdims=True), (8, 128)
    )
    for p in ep_peers:
        ep_copy(scale_rows.at[me], scale_rows.at[me], "z", p).start()

    def send_g(k, g):
        block = g_all.at[my, g]
        for p in [sibling] + [same_core(y) for y in far_lines]:
            tp_copy(block, block, "g", p, k * n_tp + my).start()

    def pass_on(k, g):
        for y in far_lines:
            p = same_core(y)
            block = g_all.at[p, g]
            tp_copy(block, block, "g", p, k * n_tp + p).wait_recv()
            tp_copy(block, block, "g", sibling, k * n_tp + p).start()

    def arrived_g(k, g, p):
        block = g_all.at[p, g]
        tp_copy(block, block, "g", p, k * n_tp + p).wait_recv()

    def forward_x(k):
        for q in pairs_in(group_from[k], k == 0):
            block = x_all.at[twin(q)]
            ep_copy(block, block, "x", twin(q), twin(q)).wait_recv()
            ep_copy(block, block, "x", mate, twin(q)).start()

    group_from = [my_group] + [far_groups[i] for i in x_order]
    hidden = w_dg.shape[1]
    if groups % 2:
        units = [(u * pairs, pairs) for u in range(2)]
    else:
        units = [(g * members, members) for g in group_from]
    steps = len(units) // 2
    unit_rows = units[0][1] * rows
    loads[dg_i].wait()
    loads[du_i].wait()

    def unit_of(ref, u):
        start, count = units[u]
        return ref.at[pl.ds(start, count)]

    def near_d(h):
        return tp_copy(d_send.at[h, 1], d_near.at[h], "d1", sibling, h)

    def far_d(h, y, source):
        return tp_copy(d_send.at[h, 0], d_far.at[h, source], "d2", same_core(y), h * lines + source)

    def dense_dots(h):
        xs = jnp.concatenate(
            [
                unit_of(x_all, 2 * h + u)[...].astype(F32).reshape(unit_rows, chunk)
                for u in range(2)
            ],
            axis=0,
        ).astype(BF)
        for j, w in enumerate((w_dg, w_du)):
            part = dot(xs, w[...]).reshape(2, unit_rows, hidden)
            d_half[h, :, :, j * hidden : (j + 1) * hidden] = part
        d_send[h, 1] = d_half[h, 1 - core].astype(BF)
        near_d(h).start()

    def dense_cross(h):
        near_d(h).wait_recv()
        pre = d_half[h, core] + d_near[h].astype(F32)
        d_half[h, 0] = pre
        d_send[h, 0] = pre.astype(BF)
        for y in far_lines:
            far_d(h, y, line).start()

    def dense_hide(h):
        pre = d_half[h, 0]
        for y in far_lines:
            far_d(h, y, y).wait_recv()
            pre = pre + d_far[h, y].astype(F32)
        first, count = units[2 * h][0] * (1 - core) + units[2 * h + 1][0] * core, units[2 * h][1]
        pre = pre * scale_ref[pl.ds(first, count)].reshape(unit_rows, 128)[:, :1]
        h_all[2 * h + core] = (silu(pre[:, :hidden]) * pre[:, hidden:]).astype(BF)
        sent_h(h).start()

    def sent_h(h):
        return tp_copy(h_all.at[2 * h + core], h_all.at[2 * h + core], "h", sibling, h)

    forward_x(0)
    relayed = [k + 1 for k, i in enumerate(x_order) if i not in x_straight]
    for k in range(groups):
        g = group_from[k]
        if k < len(relayed):
            forward_x(relayed[k])
        if steps == 2 and k == CROSS_AT:
            dense_cross(0)
        if k > 0 and k not in relayed:
            for q in pairs_in(g):
                ep_copy(x_all.at[me], x_all.at[twin(q)], "x", mate, twin(q)).wait_recv()
        for q in pairs_in(g, k == 0) + ([pair] if k == 0 else []):
            ep_copy(x_all.at[me], x_all.at[cross(q)], "x", mate, cross(q)).wait_recv()
        block = x_all[pl.ds(g * members, members)].astype(F32)
        g_all[my, g] = lax.dot_general(
            place_ref[g], block.reshape(group_tokens, chunk).astype(BF),
            (((0,), (0,)), ((), ())), preferred_element_type=F32,
        ).astype(BF)
        send_g(k, g)
        if k > 1:
            pass_on(k - 2, group_from[k - 2])
        if steps == 2 and k == 1:
            dense_dots(0)
    drains.append(ep_copy(x_all.at[most], x_all.at[most], "x", mate))
    drains.append(tp_copy(g_all.at[most_tp], g_all.at[most_tp], "g", sibling))
    for i in (eg_i, eu_i, ed_i, dd_i):
        loads[i].wait()
    for h in range(0 if steps != 2 else 1, steps):
        dense_dots(h)
    if groups > 1:
        pass_on(groups - 2, group_from[groups - 2])
    if steps == 2 and CROSS_AT == 4:
        dense_cross(0)

    def expert_in(p, gate, up):
        routed = g_all[p].astype(F32).reshape(slots, chunk).astype(BF)
        return (
            gate + dot(routed, w_eg[0, columns_of(p), :]), up + dot(routed, w_eu[0, columns_of(p), :])
        )

    gate = jnp.zeros((slots, w_eg.shape[2]), F32)
    gate, up = expert_in(my, gate, gate)
    pass_on(groups - 1, group_from[groups - 1])
    for k in range(groups):
        arrived_g(k, group_from[k], sibling)
    gate, up = expert_in(sibling, gate, up)
    for h in range(0 if steps != 2 else 1, steps):
        dense_cross(h)
    done_z = ep_copy(scale_rows.at[most], scale_rows.at[most], "z", mate)
    done_z.wait_recv()
    drains.append(done_z)
    for p in range(n_ep):
        scale_ref[p] = jnp.broadcast_to(column(scale_rows[p, :1, :]), (rows, 128))
    slot_scale = jnp.concatenate(
        [
            lax.dot_general(
                place_ref[g].astype(F32),
                scale_ref[g * members : (g + 1) * members].reshape(group_tokens, 128),
                (((0,), (0,)), ((), ())), precision=lax.Precision.HIGHEST,
                preferred_element_type=F32,
            )
            for g in range(groups)
        ],
        axis=0,
    )[:, :1]
    for h in range(steps - 1):
        dense_hide(h)
    for y in far_lines:
        gate, up = expert_in(same_core(y), gate, up)
    for y in far_lines:
        for k in range(groups):
            arrived_g(k, group_from[k], other_core(y))
        gate, up = expert_in(other_core(y), gate, up)
    expert_hidden = (silu(gate * slot_scale) * (up * slot_scale)).astype(BF)
    returns = far_groups + [my_group]

    def near_e(k):
        g = returns[k]
        return tp_copy(e_part.at[1 - core, g], e_near.at[g], "e1", sibling, k)

    def far_e(k, y):
        g = returns[k]
        return tp_copy(e_send.at[g, y], e_recv.at[g, line], "e2", same_core(y), k)

    def expert_out(which, y):
        part = dot(expert_hidden, w_ed[0, :, columns_of(2 * y + which)])
        e_part[which, :, y] = part.reshape(groups, group_slots, chunk).astype(BF)

    for y in range(lines):
        expert_out(1 - core, y)
    for k in range(groups):
        near_e(k).start()
    for y in range(lines):
        expert_out(core, y)
    for k in range(groups):
        g = returns[k]
        near_e(k).wait_recv()
        for y in far_lines:
            e_send[g, y] = (e_part[core, g, y].astype(F32) + e_near[g, y].astype(F32)).astype(BF)
            far_e(k, y).start()
    drains.append(tp_copy(e_part.at[0], e_near, "e1", sibling))
    other_lines = pl.ds(0, lines - 1)
    sent = e_send.at[pl.ds(0, groups), other_lines]
    drains.append(tp_copy(sent, e_recv.at[pl.ds(0, groups), other_lines], "e2", sibling))
    dense_hide(steps - 1)
    for h in range(steps):
        tp_copy(h_all.at[core], h_all.at[2 * h + 1 - core], "h", sibling, h).wait_recv()
    drains.append(tp_copy(h_all.at[pl.ds(0, steps)], h_all.at[pl.ds(0, steps)], "h", sibling))
    sent = d_send.at[pl.ds(0, steps), 1]
    drains.append(tp_copy(sent, d_near, "d1", sibling))
    for y in far_lines:
        sent = d_send.at[pl.ds(0, steps), 0]
        drains.append(tp_copy(sent, d_far.at[pl.ds(0, steps), line], "d2", same_core(y)))
    dense_hidden = h_all[...].astype(F32).reshape(batch, hidden).astype(BF)
    dense = dot(dense_hidden, w_dd[...]) * (1.0 / (1.0 + jnp.exp(-mix[...])))
    for u in range(len(units)):
        part = dense[u * unit_rows : (u + 1) * unit_rows]
        unit_of(dense_ref, u)[...] = part.reshape(units[u][1], rows, chunk)

    def near_f(k):
        g = returns[k]
        return ep_copy(f_away.at[g], f_mate.at[g], "f1", mate, k)

    def far_f(k):
        g = returns[k]
        near_f(k).wait_recv()
        both = comb[g, par] + f_mate[g].astype(F32)
        comb[g, par] = both
        send_f(g, both, k == groups - 1)

    def send_f(g, values, own_group):
        f_send[pl.ds(g * group_pairs, group_pairs)] = values.astype(BF)
        for q in pairs_in(g, own_group):
            ep_copy(f_send.at[q], f_recv.at[pair], "f2", twin(q), pair).start()

    def straight_f(k, g):
        send_f(g, comb[g, par], False)
        first = pairs + f_straight.index(k) * group_pairs
        f_send[pl.ds(first, group_pairs)] = comb[g, 1 - par].astype(BF)
        for m in range(group_pairs):
            spare = first + lax.rem(pair, group_pairs)
            q = g * group_pairs + m
            ep_copy(f_send.at[first + m], f_recv.at[spare], "f2", cross(q), spare).start()

    for k in range(groups):
        g = returns[k]
        block = pl.ds(g * members, members)
        result = e_part[core, g, line].astype(F32) + e_near[g, line].astype(F32)
        tp_copy(e_send.at[g, other_lines], e_recv.at[g, other_lines], "e2", sibling, k).wait_recv()
        for y in far_lines:
            result = result + e_recv[g, y].astype(F32)
        coef = c_recv[block].reshape(group_tokens, 128)[:, :1]
        mixed = coef * dot(place_ref[g], result.astype(BF))
        combined = dense_ref[block] + mixed.reshape(members, rows, chunk)
        for m in range(members):
            comb[g, m % 2, m // 2] = combined[m]
        if k in f_straight:
            straight_f(k, g)
        else:
            f_away[g] = comb[g, 1 - par].astype(BF)
            near_f(k).start()
        if k > 1 and k - 2 not in f_straight:
            far_f(k - 2)
    for k in range(max(0, groups - 2), groups):
        if k not in f_straight:
            far_f(k)
    met = pl.ds(0, groups - len(f_straight))
    drains.append(ep_copy(f_away.at[met], f_mate.at[met], "f1", mate))
    spares = list(range(pairs, pairs + len(f_straight) * group_pairs))
    sent = pl.ds(0, pairs - 1 + len(spares))
    drains.append(ep_copy(f_send.at[sent], f_recv.at[sent], "f2", mate))
    final = middle_ref[...] + comb[my_group, par, lax.rem(pair, group_pairs)]
    for q in others + spares:
        ep_copy(f_send.at[q], f_recv.at[q], "f2", mate, q).wait_recv()
        final = final + f_recv[q].astype(F32)
    out[...] = final.astype(BF)
    for copy in drains:
        copy.wait_send()


def per_device(
    tokens, delta_state, attn_gain, query_weight, key_weight, value_weight, decay_weight,
    beta_weight, decay_rate, head_gain, output_weight, ffn_gain, expert_ids, group_prob,
    expert_logit, expert_gate, expert_up, expert_down, dense_gate, dense_up, dense_down, dense_mix,
):
    n_ep = lax.axis_size("ep")
    n_tp = lax.axis_size("tp")
    rows, width = tokens.shape
    heads = delta_state.shape[1]
    local = heads * 128
    topk = expert_ids.shape[1]
    cap = max(2, 2 * rows * topk // n_ep)
    members = max(2, 8 // math.gcd(cap, 8))
    if n_ep % members:
        members = n_ep
    groups = n_ep // members
    group_slots = members * cap
    chunk = width // n_tp
    depth = width // n_ep
    batch = n_ep * rows
    pairs = n_ep // 2
    lines = n_tp // 2
    hidden = dense_gate.shape[1]
    small = (
        tokens, attn_gain[None, :], decay_rate[None, :], head_gain[None, :], ffn_gain[None, :],
        expert_ids.T, group_prob[None, :], expert_logit.T, dense_mix[None, :],
    )
    weights = (
        delta_state, decay_weight.T, beta_weight.T, query_weight, key_weight, value_weight,
        output_weight, dense_gate, dense_up, expert_gate, expert_up, expert_down, dense_down,
    )
    arrays = tuple(pltpu.with_memory_space_constraint(a, pltpu.HBM) for a in small + weights)
    steps = dense_steps(groups)
    unit_rows = batch // (2 * steps)
    starts, n_sems = semaphores(n_ep, n_tp, members, len(arrays))
    dims = (n_ep, n_tp, rows, width, heads, members, cap, len(arrays), starts)
    vmem = pl.BlockSpec(memory_space=pltpu.VMEM)
    kq_rows = -(-2 * heads // 8) * 8
    scratch = [pltpu.VMEM(a.shape, a.dtype) for a in small + weights[1:]]
    scratch += [
        pltpu.VMEM(shape, dtype)
        for shape, dtype in (
            ((n_ep, rows, depth), BF), ((n_ep, rows, depth), BF),
            ((2, pairs, rows, local), F32), ((pairs, 2, rows, local), BF),
            ((pairs, 2, rows, local), BF), ((rows, local), BF), ((rows, local), BF),
            ((2, pairs, rows, local), BF), ((2, pairs, rows, local), BF),
            ((2, pairs, rows, local), F32),
            ((2, pairs, rows, local), BF), ((2, pairs, rows, local), BF),
            ((n_ep, 8, 128), F32), ((n_ep, 8, 128), F32), ((n_ep, rows, 128), F32),
            ((rows, kq_rows, 128), F32), ((2 * heads, rows, 128), F32),
            ((heads, rows, 128), F32), ((heads, rows, 128), F32), ((rows, local), BF),
            ((n_tp, rows, chunk), BF), ((n_tp, rows, chunk), BF), ((n_tp, rows, 128), F32),
            ((n_ep, 8, 128), F32), ((n_ep, rows, 128), F32), ((rows, chunk), F32),
            ((n_ep, rows, chunk), BF), ((n_tp, groups, group_slots, chunk), BF),
            ((steps, 2, unit_rows, 2 * hidden), F32), ((steps, 2, unit_rows, 2 * hidden), BF),
            ((steps, unit_rows, 2 * hidden), BF), ((steps, lines, unit_rows, 2 * hidden), BF),
            ((2 * steps, unit_rows, hidden), BF),
            ((2, groups, lines, group_slots, chunk), BF), ((groups, lines, group_slots, chunk), BF),
            ((groups, lines, group_slots, chunk), BF), ((groups, lines, group_slots, chunk), BF),
            ((groups, 2, members // 2, rows, chunk), F32),
            ((groups, members // 2, rows, chunk), BF), ((groups, members // 2, rows, chunk), BF),
            ((n_ep, rows, chunk), BF), ((n_ep, rows, chunk), BF),
            ((groups, members * rows, group_slots), BF), ((n_ep, rows, chunk), F32),
        )
    ]
    scratch += [pltpu.SemaphoreType.DMA((n_sems,))]
    mixed_out, new_state = pl.pallas_call(
        functools.partial(kernel, dims),
        out_shape=(pltpu.VMEM((rows, chunk), BF), pltpu.VMEM(delta_state.shape, F32)),
        in_specs=[pl.BlockSpec(memory_space=pltpu.HBM)] * len(arrays),
        out_specs=(vmem, vmem),
        scratch_shapes=scratch,
        compiler_params=pltpu.CompilerParams(
            collective_id=0, has_side_effects=True, vmem_limit_bytes=44 * 1024 * 1024
        ),
    )(*arrays)
    new_state, mixed_out = pl.pallas_call(
        store_kernel,
        out_shape=(pltpu.HBM(delta_state.shape, F32), pltpu.HBM((rows, chunk), BF)),
        in_specs=[vmem] * 2,
        out_specs=(pl.BlockSpec(memory_space=pltpu.HBM),) * 2,
        scratch_shapes=[pltpu.SemaphoreType.DMA((2,))],
        compiler_params=pltpu.CompilerParams(vmem_limit_bytes=8 * 1024 * 1024),
    )(*(pltpu.with_memory_space_constraint(a, pltpu.VMEM) for a in (new_state, mixed_out)))
    return mixed_out, new_state


def solution(mesh):
    return jax.shard_map(
        per_device,
        mesh=mesh,
        in_specs=(
            P("ep", None), P("ep", "tp", None, None), P(), P("ep", "tp"), P("ep", "tp"),
            P("ep", "tp"), P(), P(), P("tp"), P(), P("tp", None), P(), P("ep", None), P("ep"),
            P("ep", None), P("ep", None, "tp"), P("ep", None, "tp"), P("ep", "tp", None),
            P("tp", "ep"), P("tp", "ep"), P("ep", "tp"), P("tp"),
        ),
        out_specs=(P("ep", "tp"), P("ep", "tp", None, None)),
        check_vma=False,
    )
```

```python
import functools
import math

import jax
import jax.numpy as jnp
from jax import lax
from jax.experimental import pallas as pl
from jax.experimental.pallas import tpu as pltpu
from jax.sharding import PartitionSpec as P

EPS = 1e-06
CROSS_AT = 6
DOTS_AT = 1
RETURNS = (0, 1, 2, 3)
LAG = 2
STORE = 1
RECALL = 4
UPDATE = 4
X_STRAIGHT = (2,)
F_STRAIGHT = (0, 2)
X_SENDS = (0, 1, 2)
X_ORDER = (2, 0, 1)
BF = jnp.bfloat16
F32 = jnp.float32
MESH = pl.DeviceIdType.MESH


def dot(left, right):
    return jnp.dot(left, right, preferred_element_type=F32)


def dot_t(left, right):
    return lax.dot_general(left, right, (((1,), (1,)), ((), ())), preferred_element_type=F32)


def silu(values):
    return values / (1.0 + jnp.exp(-values))


def far_first(position, count):
    low = 1 - lax.div(2 * position, count)
    order = []
    for k in range(count - 1):
        down = count - 1 - k
        down = down - lax.div(position - down + count, count)
        up = k + lax.div(k - position + count, count)
        order.append(low * down + (1 - low) * up)
    return order


def partners(position, count):
    if count == 4:
        low, high = lax.rem(position, 2), lax.div(position, 2)
        return [3 - position, position + 2 - 4 * high, position + 1 - 2 * low]
    return far_first(position, count)


def store_kernel(state, mixed, state_out, mixed_out, sems):
    rows = state.shape[0]
    small = pltpu.make_async_copy(mixed, mixed_out, sems.at[1])
    small.start()
    step = math.gcd(rows, STORE)
    for r in range(0, rows, step):
        block = pl.ds(r, step)
        pltpu.make_async_copy(state.at[block], state_out.at[block], sems.at[0]).start()
    pltpu.make_async_copy(state, state_out, sems.at[0]).wait()
    small.wait()


def dense_steps(groups):
    return 1 if groups % 2 else groups // 2


def semaphores(n_ep, n_tp, members, n_in):
    groups = n_ep // members
    pairs, lines = n_ep // 2, n_tp // 2
    steps = dense_steps(groups)
    sizes = {
        "load": n_in, "ns": 1, "nr": pairs + 1, "ms": 1, "mr": 1, "cs": 1, "cr": 1, "zs": 1, "zr": 1,
        "q1s": 1, "q1r": 2, "q2s": 1, "q2r": 2, "k1s": 1, "k1r": 1, "k2s": 1, "k2r": 1, "xs": 1, "xr": n_ep,
        "f1s": 1, "f1r": groups, "f2s": 1, "f2r": 1, "as": 1, "ar": 1, "ss": 1, "sr": 1,
        "d1s": 1, "d1r": steps, "d2s": 1, "d2r": steps * lines, "hs": 1, "hr": steps,
        "gs": 1, "gr": groups * n_tp, "e1s": 1, "e1r": groups * lines, "e2s": 1, "e2r": groups,
    }
    starts, total = {}, 0
    for name, size in sizes.items():
        starts[name] = total
        total += size
    return starts, total


def kernel(dims, *refs):
    n_ep, n_tp, rows, width, heads, members, cap, n_in, starts = dims
    hbm, refs = refs[:n_in], refs[n_in:]
    out, state = refs[:2]
    held = refs[2 : 11] + (state,) + refs[11 : 1 + n_in]
    refs = refs[1 + n_in :]
    (tokens, attn_gain, decay_rate, head_gain, ffn_gain, ids, group_prob, logit, mix) = held[:9]
    state, w_decay, w_beta, w_q, w_k, w_v, w_o, w_dg, w_du, w_eg, w_eu, w_ed, w_dd = held[9:]
    (
        n_send, n_recv, k_own, k_send, k_recv, k_away, k_mate, q_away, q_mate, q_own, q_send, q_recv, c_send, c_rows, c_recv, kq, recall,
        corr_ref, decay_ref, head_out, a_send, a_recv, s_recv, scale_rows, scale_ref, middle_ref,
        x_all, g_all, d_half, d_send, d_near, d_far, h_all, e_part, e_near, e_send, e_recv,
        comb, f_away, f_mate, f_send, f_recv, place_ref, dense_ref, sems,
    ) = refs
    me = lax.axis_index("ep")
    my = lax.axis_index("tp")
    chunk = width // n_tp
    depth = width // n_ep
    batch = n_ep * rows
    local = heads * 128
    groups = n_ep // members
    group_slots = members * cap
    group_tokens = members * rows
    slots = groups * group_slots
    pairs = n_ep // 2
    lines = n_tp // 2
    group_pairs = members // 2
    pair = lax.div(me, 2)
    par = lax.rem(me, 2)
    mate = me + 1 - 2 * par
    core = lax.rem(my, 2)
    line = lax.div(my, 2)
    sibling = my + 1 - 2 * core
    my_group = lax.div(pair, group_pairs)
    far_groups = partners(my_group, groups)
    x_straight = {4: X_STRAIGHT, 2: (0,)}.get(groups, ())
    f_straight = {4: F_STRAIGHT, 2: (0,)}.get(groups, ())
    x_sends = X_SENDS if groups == 4 else range(groups - 1)
    x_order = X_ORDER if groups == 4 else range(groups - 1)
    far_lines = [lax.rem(line + d, lines) for d in range(1, lines)]

    def same_core(y):
        return 2 * y + core

    def other_core(y):
        return 2 * y + 1 - core

    def twin(q):
        return 2 * q + par

    def cross(q):
        return 2 * q + 1 - par

    def pairs_in(g, own=False):
        mine = lax.rem(pair, group_pairs)
        return [
            g * group_pairs + lax.rem(mine + m, group_pairs)
            for m in range(1 if own else 0, group_pairs)
        ]

    others = [q for g in far_groups for q in pairs_in(g)] + pairs_in(my_group, True)
    ep_peers = [p for q in others for p in (cross(q), twin(q))] + [mate]
    far_tp = [p for y in far_lines for p in (same_core(y), other_core(y))]
    tp_peers = far_tp + [sibling]

    def sem(name, index=0):
        return sems.at[starts[name] + index]

    def ep_copy(src, dst, name, peer, index=0):
        return pltpu.make_async_remote_copy(
            src_ref=src, dst_ref=dst, send_sem=sem(name + "s"), recv_sem=sem(name + "r", index),
            device_id=(peer, my), device_id_type=MESH,
        )

    def tp_copy(src, dst, name, peer, index=0):
        return pltpu.make_async_remote_copy(
            src_ref=src, dst_ref=dst, send_sem=sem(name + "s"), recv_sem=sem(name + "r", index),
            device_id=(me, peer), device_id_type=MESH,
        )

    drains = []

    loads = [
        pltpu.make_async_copy(src, dst, sem("load", i))
        for i, (src, dst) in enumerate(zip(hbm, held))
    ]
    state_i, decay_i, beta_i, q_i, k_i, v_i, o_i, dg_i, du_i, eg_i, eu_i, ed_i, dd_i = range(9, 22)
    order = (decay_i, beta_i, k_i, q_i, v_i, state_i, o_i, dg_i, du_i, eg_i, eu_i, ed_i, dd_i)
    for i in range(9):
        loads[i].start()
    barrier = pltpu.get_barrier_semaphore()
    for p in ep_peers:
        pl.semaphore_signal(barrier, inc=1, device_id=(p, my), device_id_type=MESH)
    for p in tp_peers:
        pl.semaphore_signal(barrier, inc=1, device_id=(me, p), device_id_type=MESH)
    for i in order:
        loads[i].start()

    for i in range(9):
        loads[i].wait()
    x = tokens[...].astype(F32)
    mean_sq = jnp.mean(x * x, axis=-1, keepdims=True)
    normed = (x * lax.rsqrt(mean_sq + EPS) * attn_gain[...]).astype(BF)
    for p in range(n_ep):
        n_send[p] = normed[:, p * depth : (p + 1) * depth]
    pl.semaphore_wait(barrier, n_ep + n_tp - 2)
    def shelf(p):
        return lax.rem(p, 2) * pairs + lax.div(p, 2)

    def carried(q):
        return 2 * q + lax.rem(par + pair + q + core, 2)

    for q in others:
        ep_copy(n_send.at[carried(q)], n_recv.at[shelf(me)], "n", carried(q), pair).start()
    ep_copy(n_send.at[mate], n_recv.at[shelf(me)], "n", mate, pairs).start()
    n_recv[shelf(me)] = n_send[me]

    logit_exp = jnp.exp(logit[...])
    route = group_prob[...] * logit_exp / jnp.sum(logit_exp, axis=0, keepdims=True)
    names = ids[...]
    eye = lax.broadcasted_iota(jnp.int32, (rows, rows), 0) == lax.broadcasted_iota(
        jnp.int32, (rows, rows), 1
    )
    c_send[...] = jnp.zeros_like(c_send)
    for p in range(n_ep):
        flat = jnp.sum(jnp.where(names == p, route, 0.0), axis=0, keepdims=True)
        c_send[p, :, :rows] = jnp.broadcast_to(flat, (8, rows))
    for p in ep_peers:
        ep_copy(c_send.at[p], c_rows.at[me], "c", p).start()
    c_rows[me] = c_send[me]

    def column(row):
        return jnp.sum(jnp.where(eye, row[:, :rows], 0.0), axis=1, keepdims=True)

    loads[decay_i].wait()
    loads[beta_i].wait()
    decay_pre = dot_t(normed, w_decay[...])
    beta_pre = dot_t(normed, w_beta[...])
    lane = lax.broadcasted_iota(jnp.int32, decay_pre.shape, 1)
    decays, betas = [], []
    for h in range(heads):
        mine = lane == my * heads + h
        d = jnp.sum(jnp.where(mine, decay_pre, 0.0), axis=1, keepdims=True)
        b = jnp.sum(jnp.where(mine, beta_pre, 0.0), axis=1, keepdims=True)
        soft = jnp.maximum(d, 0.0) + jnp.log1p(jnp.exp(-jnp.abs(d)))
        decays.append(jnp.exp(-decay_rate[:, h : h + 1] * soft))
        betas.append(1.0 / (1.0 + jnp.exp(-b)))
    for i in (q_i, k_i, v_i):
        loads[i].wait()

    most = pl.ds(0, n_ep - 1)
    some = pl.ds(0, pairs - 1)
    for q in others:
        block = n_recv.at[shelf(carried(q))]
        ep_copy(block, block, "n", mate, q).wait_recv()
        tp_copy(block, block, "m", sibling).start()
    ep_copy(n_send.at[mate], n_recv.at[shelf(mate)], "n", mate, pairs).wait_recv()
    drains.append(ep_copy(n_send.at[pl.ds(0, pairs)], n_recv.at[pl.ds(0, pairs)], "n", mate))
    passed = tp_copy(n_recv.at[some], n_recv.at[some], "m", sibling)
    passed.wait_recv()
    drains.append(passed)

    def rows_of(parity):
        held_rows = n_recv[pl.ds(parity * pairs, pairs)].astype(F32)
        return held_rows.reshape(pairs * rows, depth).astype(BF)

    away, near = rows_of(1 - par), rows_of(par)
    k_part = dot(jnp.concatenate([away, near], axis=0), w_k[...]).reshape(2, pairs, rows, local)
    k_own[...] = k_part
    for side in range(2):
        k_send[:, side] = k_part[side].astype(BF)
    for q in others:
        ep_copy(k_send.at[q], k_recv.at[pair], "k1", twin(q)).start()
    for j, w in enumerate((w_q, w_v)):
        q_away[j] = dot(away, w[...]).reshape(pairs, rows, local).astype(BF)
        ep_copy(q_away.at[j], q_mate.at[j], "q1", mate, j).start()
    for j, w in enumerate((w_q, w_v)):
        q_own[j] = dot(near, w[...]).reshape(pairs, rows, local)
    for j in range(2):
        ep_copy(q_away.at[j], q_mate.at[j], "q1", mate, j).wait_recv()
        both = q_own[j] + q_mate[j].astype(F32)
        q_own[j] = both
        q_send[j] = both.astype(BF)
        for q in others:
            ep_copy(q_send.at[j, q], q_recv.at[j, pair], "q2", twin(q), j).start()
    drains.append(ep_copy(q_away, q_mate, "q1", mate))
    far_blocks = pl.ds(0, pairs - 1)
    sent = q_send.at[pl.ds(0, 2), far_blocks]
    drains.append(ep_copy(sent, q_recv.at[pl.ds(0, 2), far_blocks], "q2", mate))
    done_k = ep_copy(k_send.at[far_blocks], k_recv.at[far_blocks], "k1", mate)
    done_k.wait_recv()
    drains.append(done_k)
    sums = []
    for side in range(2):
        total = k_own[side, pair]
        for q in others:
            total = total + k_recv[q, side].astype(F32)
        sums.append(total)
        if side == 0:
            k_away[...] = total.astype(BF)
            cross_k = ep_copy(k_away, k_mate, "k2", mate)
            cross_k.start()
            drains.append(cross_k)

    def summed(j):
        ep_copy(
            q_send.at[j, far_blocks], q_recv.at[j, far_blocks], "q2", mate, j
        ).wait_recv()
        total = q_own[j, pair]
        for q in others:
            total = total + q_recv[j, q].astype(F32)
        return total.astype(BF).astype(F32)

    q_rows = summed(0)
    cross_k.wait_recv()
    k_rows = (sums[1] + k_mate[...].astype(F32)).astype(BF).astype(F32)
    loads[state_i].wait()

    def head_of(values, h):
        return values[:, h * 128 : (h + 1) * 128]

    def unit(values):
        return values * lax.rsqrt(jnp.sum(values * values, axis=-1, keepdims=True) + EPS)

    units = []
    for h in range(heads):
        q_unit = unit(head_of(q_rows, h)) * 128 ** (-0.5)
        k_unit = unit(head_of(k_rows, h))
        units.append((q_unit, k_unit))
        kq[:, h, :] = k_unit
        kq[:, heads + h, :] = q_unit

    beside = 2 if heads % 2 == 0 else 1

    def one_row(b, _):
        both = kq[b].astype(BF)
        for first in range(0, heads, beside):
            pieces = [state[b, first + i].astype(BF) for i in range(beside)]
            read = dot(both, jnp.concatenate(pieces, axis=1))
            for i in range(beside):
                h, lanes = first + i, slice(i * 128, (i + 1) * 128)
                recall[h, pl.ds(b, 1), :] = read[h : h + 1, lanes]
                recall[heads + h, pl.ds(b, 1), :] = read[heads + h : heads + h + 1, lanes]
        return 0

    lax.fori_loop(0, rows, one_row, 0, unroll=RECALL)
    v_rows = summed(1)
    for h in range(heads):
        q_unit, k_unit = units[h]
        decay, beta = decays[h], betas[h]
        corr = beta * (head_of(v_rows, h) - decay * recall[h])
        read = decay * recall[heads + h] + jnp.sum(q_unit * k_unit, axis=-1, keepdims=True) * corr
        read = read * lax.rsqrt(jnp.mean(read * read, axis=-1, keepdims=True) + EPS) * head_gain[...]
        head_out[:, h * 128 : (h + 1) * 128] = read.astype(BF)
        corr_ref[h] = corr
        decay_ref[h] = jnp.broadcast_to(decay, (rows, 128))

    loads[o_i].wait()
    ho = head_out[...]

    def columns_of(p):
        return pl.ds(pl.multiple_of(p * chunk, 128), chunk)

    for p in far_tp + [sibling]:
        a_send[p] = dot(ho, w_o[:, columns_of(p)]).astype(BF)
        tp_copy(a_send.at[p], a_recv.at[my], "a", p).start()
    a_recv[my] = dot(ho, w_o[:, columns_of(my)]).astype(BF)
    own = columns_of(my)

    def update_row(b, _):
        columns = kq[b].T
        for h in range(heads):
            corr = corr_ref[h, pl.ds(b, 1), :]
            decay = decay_ref[h, pl.ds(b, 1), :]
            state[b, h] = decay * state[b, h] + columns[:, h : h + 1] * corr
        return 0

    lax.fori_loop(0, rows // 2, update_row, 0, unroll=UPDATE)
    middle = tokens[:, own].astype(F32)
    most_tp = pl.ds(0, n_tp - 1)
    done_a = tp_copy(a_send.at[most_tp], a_recv.at[most_tp], "a", sibling)
    done_a.wait_recv()
    drains.append(done_a)
    for p in range(n_tp):
        middle = middle + a_recv[p].astype(F32)
    x_all[me] = (middle * ffn_gain[:, own]).astype(BF)
    x_peers = [mate] + [twin(q) for q in pairs_in(my_group, True)]
    for i in x_sends:
        x_peers += [twin(q) for q in pairs_in(far_groups[i])]
        if i in x_straight:
            x_peers += [cross(q) for q in pairs_in(far_groups[i])]
    for p in x_peers:
        ep_copy(x_all.at[me], x_all.at[me], "x", p, me).start()
    middle_ref[...] = middle
    s_recv[my] = jnp.broadcast_to(jnp.sum(middle * middle, axis=-1, keepdims=True), (rows, 128))
    for p in tp_peers:
        tp_copy(s_recv.at[my], s_recv.at[my], "s", p).start()
    lax.fori_loop(rows // 2, rows, update_row, 0, unroll=UPDATE)
    done_c = ep_copy(c_send.at[most], c_rows.at[most], "c", mate)
    done_c.wait_recv()
    drains.append(done_c)
    for p in range(n_ep):
        c_recv[p] = jnp.broadcast_to(column(c_rows[p, :1, :]), (rows, 128))
    tri = (
        lax.broadcasted_iota(jnp.int32, (group_tokens, group_tokens), 0)
        >= lax.broadcasted_iota(jnp.int32, (group_tokens, group_tokens), 1)
    ).astype(F32).astype(BF)
    slot = lax.broadcasted_iota(jnp.int32, (group_tokens, group_slots), 1).astype(F32)
    for g in range(groups):
        coef = c_recv[g * members : (g + 1) * members].reshape(group_tokens, 128)[:, :1]
        named = coef > 0.0
        flags = jnp.broadcast_to(jnp.where(named, 1.0, 0.0), (group_tokens, 128)).astype(BF)
        rank = dot(tri, flags)[:, :1] - 1.0
        place_ref[g] = jnp.where((rank == slot) & named, 1.0, 0.0).astype(BF)
    done_s = tp_copy(s_recv.at[most_tp], s_recv.at[most_tp], "s", sibling)
    done_s.wait_recv()
    drains.append(done_s)
    total = s_recv[0]
    for p in range(1, n_tp):
        total = total + s_recv[p]
    scale = lax.rsqrt(total / width + EPS)
    diagonal = lax.broadcasted_iota(jnp.int32, (rows, 128), 0) == lax.broadcasted_iota(
        jnp.int32, (rows, 128), 1
    )
    scale_rows[me] = jnp.broadcast_to(
        jnp.sum(jnp.where(diagonal, scale, 0.0), axis=0, keepdims=True), (8, 128)
    )
    for p in ep_peers:
        ep_copy(scale_rows.at[me], scale_rows.at[me], "z", p).start()

    def send_g(k, g):
        block = g_all.at[my, g]
        for p in [sibling] + [same_core(y) for y in far_lines]:
            tp_copy(block, block, "g", p, k * n_tp + my).start()

    def pass_on(k, g):
        for y in far_lines:
            p = same_core(y)
            block = g_all.at[p, g]
            tp_copy(block, block, "g", p, k * n_tp + p).wait_recv()
            tp_copy(block, block, "g", sibling, k * n_tp + p).start()

    def arrived_g(k, g, p):
        block = g_all.at[p, g]
        tp_copy(block, block, "g", p, k * n_tp + p).wait_recv()

    def forward_x(k):
        for q in pairs_in(group_from[k], k == 0):
            block = x_all.at[twin(q)]
            ep_copy(block, block, "x", twin(q), twin(q)).wait_recv()
            ep_copy(block, block, "x", mate, twin(q)).start()

    group_from = [my_group] + [far_groups[i] for i in x_order]
    hidden = w_dg.shape[1]
    if groups % 2:
        units = [(u * pairs, pairs) for u in range(2)]
    else:
        units = [(g * members, members) for g in group_from]
    steps = len(units) // 2
    unit_rows = units[0][1] * rows
    loads[dg_i].wait()
    loads[du_i].wait()

    def unit_of(ref, u):
        start, count = units[u]
        return ref.at[pl.ds(start, count)]

    def near_d(h):
        return tp_copy(d_send.at[h, 1], d_near.at[h], "d1", sibling, h)

    def far_d(h, y, source):
        return tp_copy(d_send.at[h, 0], d_far.at[h, source], "d2", same_core(y), h * lines + source)

    def dense_dots(h):
        xs = jnp.concatenate(
            [
                unit_of(x_all, 2 * h + u)[...].astype(F32).reshape(unit_rows, chunk)
                for u in range(2)
            ],
            axis=0,
        ).astype(BF)
        for j, w in enumerate((w_dg, w_du)):
            part = dot(xs, w[...]).reshape(2, unit_rows, hidden)
            d_half[h, :, :, j * hidden : (j + 1) * hidden] = part
        d_send[h, 1] = d_half[h, 1 - core].astype(BF)
        near_d(h).start()

    def dense_cross(h):
        near_d(h).wait_recv()
        pre = d_half[h, core] + d_near[h].astype(F32)
        d_half[h, 0] = pre
        d_send[h, 0] = pre.astype(BF)
        for y in far_lines:
            far_d(h, y, line).start()

    def dense_hide(h):
        pre = d_half[h, 0]
        for y in far_lines:
            far_d(h, y, y).wait_recv()
            pre = pre + d_far[h, y].astype(F32)
        first, count = units[2 * h][0] * (1 - core) + units[2 * h + 1][0] * core, units[2 * h][1]
        pre = pre * scale_ref[pl.ds(first, count)].reshape(unit_rows, 128)[:, :1]
        h_all[2 * h + core] = (silu(pre[:, :hidden]) * pre[:, hidden:]).astype(BF)
        sent_h(h).start()

    def sent_h(h):
        return tp_copy(h_all.at[2 * h + core], h_all.at[2 * h + core], "h", sibling, h)

    forward_x(0)
    relayed = [k + 1 for k, i in enumerate(x_order) if i not in x_straight]
    for k in range(groups):
        g = group_from[k]
        if k < len(relayed):
            forward_x(relayed[k])
        if steps == 2 and k == CROSS_AT:
            dense_cross(0)
        if k > 0 and k not in relayed:
            for q in pairs_in(g):
                ep_copy(x_all.at[me], x_all.at[twin(q)], "x", mate, twin(q)).wait_recv()
        for q in pairs_in(g, k == 0) + ([pair] if k == 0 else []):
            ep_copy(x_all.at[me], x_all.at[cross(q)], "x", mate, cross(q)).wait_recv()
        block = x_all[pl.ds(g * members, members)].astype(F32)
        g_all[my, g] = lax.dot_general(
            place_ref[g], block.reshape(group_tokens, chunk).astype(BF),
            (((0,), (0,)), ((), ())), preferred_element_type=F32,
        ).astype(BF)
        send_g(k, g)
        if k > 1:
            pass_on(k - 2, group_from[k - 2])
        if steps == 2 and k == DOTS_AT:
            dense_dots(0)
    drains.append(ep_copy(x_all.at[most], x_all.at[most], "x", mate))
    drains.append(tp_copy(g_all.at[most_tp], g_all.at[most_tp], "g", sibling))
    for i in (eg_i, eu_i, ed_i, dd_i):
        loads[i].wait()
    if steps == 2 and CROSS_AT == 6:
        dense_cross(0)
    for h in range(0 if steps != 2 else 1, steps):
        dense_dots(h)
    if steps == 2 and CROSS_AT == 7:
        dense_cross(0)
    if groups > 1:
        pass_on(groups - 2, group_from[groups - 2])
    if steps == 2 and CROSS_AT == 4:
        dense_cross(0)

    def expert_in(p, gate, up):
        routed = g_all[p].astype(F32).reshape(slots, chunk).astype(BF)
        return (
            gate + dot(routed, w_eg[0, columns_of(p), :]), up + dot(routed, w_eu[0, columns_of(p), :])
        )

    gate = jnp.zeros((slots, w_eg.shape[2]), F32)
    gate, up = expert_in(my, gate, gate)
    pass_on(groups - 1, group_from[groups - 1])
    for k in range(groups):
        arrived_g(k, group_from[k], sibling)
    gate, up = expert_in(sibling, gate, up)
    if steps == 2 and CROSS_AT == 5:
        dense_cross(0)
    for h in range(0 if steps != 2 else 1, steps):
        dense_cross(h)
    done_z = ep_copy(scale_rows.at[most], scale_rows.at[most], "z", mate)
    done_z.wait_recv()
    drains.append(done_z)
    for p in range(n_ep):
        scale_ref[p] = jnp.broadcast_to(column(scale_rows[p, :1, :]), (rows, 128))
    slot_scale = jnp.concatenate(
        [
            lax.dot_general(
                place_ref[g].astype(F32),
                scale_ref[g * members : (g + 1) * members].reshape(group_tokens, 128),
                (((0,), (0,)), ((), ())), precision=lax.Precision.HIGHEST,
                preferred_element_type=F32,
            )
            for g in range(groups)
        ],
        axis=0,
    )[:, :1]
    for h in range(steps - 1):
        dense_hide(h)
    for y in far_lines:
        gate, up = expert_in(same_core(y), gate, up)
    for y in far_lines:
        for k in range(groups):
            arrived_g(k, group_from[k], other_core(y))
        gate, up = expert_in(other_core(y), gate, up)
    expert_hidden = (silu(gate * slot_scale) * (up * slot_scale)).astype(BF)
    order_back = RETURNS if groups == 4 else tuple(range(groups))
    returns = [(far_groups + [my_group])[i] for i in order_back]
    own_at = order_back.index(groups - 1)
    f_direct = [k for k in range(groups) if order_back[k] in f_straight]

    def near_e(k, y):
        g = returns[k]
        return tp_copy(e_part.at[1 - core, g, y], e_near.at[g, y], "e1", sibling, k * lines + y)

    def far_e(k, y):
        g = returns[k]
        return tp_copy(e_send.at[g, y], e_recv.at[g, line], "e2", same_core(y), k)

    def expert_out(which, y):
        part = dot(expert_hidden, w_ed[0, :, columns_of(2 * y + which)])
        e_part[which, :, y] = part.reshape(groups, group_slots, chunk).astype(BF)

    for y in far_lines + [line]:
        expert_out(1 - core, y)
        for k in range(groups):
            near_e(k, y).start()
    for y in far_lines + [line]:
        expert_out(core, y)
    for k in range(groups):
        g = returns[k]
        for y in far_lines:
            near_e(k, y).wait_recv()
            e_send[g, y] = (e_part[core, g, y].astype(F32) + e_near[g, y].astype(F32)).astype(BF)
            far_e(k, y).start()
    drains.append(tp_copy(e_part.at[0], e_near, "e1", sibling))
    other_lines = pl.ds(0, lines - 1)
    sent = e_send.at[pl.ds(0, groups), other_lines]
    drains.append(tp_copy(sent, e_recv.at[pl.ds(0, groups), other_lines], "e2", sibling))
    dense_hide(steps - 1)
    for h in range(steps):
        tp_copy(h_all.at[core], h_all.at[2 * h + 1 - core], "h", sibling, h).wait_recv()
    drains.append(tp_copy(h_all.at[pl.ds(0, steps)], h_all.at[pl.ds(0, steps)], "h", sibling))
    sent = d_send.at[pl.ds(0, steps), 1]
    drains.append(tp_copy(sent, d_near, "d1", sibling))
    for y in far_lines:
        sent = d_send.at[pl.ds(0, steps), 0]
        drains.append(tp_copy(sent, d_far.at[pl.ds(0, steps), line], "d2", same_core(y)))
    dense_hidden = h_all[...].astype(F32).reshape(batch, hidden).astype(BF)
    dense = dot(dense_hidden, w_dd[...]) * (1.0 / (1.0 + jnp.exp(-mix[...])))
    for u in range(len(units)):
        part = dense[u * unit_rows : (u + 1) * unit_rows]
        unit_of(dense_ref, u)[...] = part.reshape(units[u][1], rows, chunk)

    def near_f(k):
        g = returns[k]
        return ep_copy(f_away.at[g], f_mate.at[g], "f1", mate, k)

    def far_f(k):
        g = returns[k]
        near_f(k).wait_recv()
        both = comb[g, par] + f_mate[g].astype(F32)
        comb[g, par] = both
        send_f(g, both, k == own_at)

    def send_f(g, values, own_group):
        f_send[pl.ds(g * group_pairs, group_pairs)] = values.astype(BF)
        for q in pairs_in(g, own_group):
            ep_copy(f_send.at[q], f_recv.at[pair], "f2", twin(q)).start()

    def straight_f(k, g):
        send_f(g, comb[g, par], False)
        first = pairs + f_straight.index(order_back[k]) * group_pairs
        f_send[pl.ds(first, group_pairs)] = comb[g, 1 - par].astype(BF)
        for m in range(group_pairs):
            spare = first + lax.rem(pair, group_pairs)
            q = g * group_pairs + m
            ep_copy(f_send.at[first + m], f_recv.at[spare], "f2", cross(q)).start()

    for k in range(groups):
        g = returns[k]
        block = pl.ds(g * members, members)
        near_e(k, line).wait_recv()
        result = e_part[core, g, line].astype(F32) + e_near[g, line].astype(F32)
        tp_copy(e_send.at[g, other_lines], e_recv.at[g, other_lines], "e2", sibling, k).wait_recv()
        for y in far_lines:
            result = result + e_recv[g, y].astype(F32)
        coef = c_recv[block].reshape(group_tokens, 128)[:, :1]
        mixed = coef * dot(place_ref[g], result.astype(BF))
        combined = dense_ref[block] + mixed.reshape(members, rows, chunk)
        for m in range(members):
            comb[g, m % 2, m // 2] = combined[m]
        if k in f_direct:
            straight_f(k, g)
        else:
            f_away[g] = comb[g, 1 - par].astype(BF)
            near_f(k).start()
        if k >= LAG and k - LAG not in f_direct:
            far_f(k - LAG)
    for k in range(max(0, groups - LAG), groups):
        if k not in f_direct:
            far_f(k)
    met = pl.ds(0, groups - len(f_direct))
    drains.append(ep_copy(f_away.at[met], f_mate.at[met], "f1", mate))
    spares = list(range(pairs, pairs + len(f_straight) * group_pairs))
    sent = pl.ds(0, pairs - 1 + len(spares))
    drains.append(ep_copy(f_send.at[sent], f_recv.at[sent], "f2", mate))
    final = middle_ref[...] + comb[my_group, par, lax.rem(pair, group_pairs)]
    ep_copy(f_send.at[sent], f_recv.at[sent], "f2", mate).wait_recv()
    for q in others + spares:
        final = final + f_recv[q].astype(F32)
    out[...] = final.astype(BF)
    for copy in drains:
        copy.wait_send()


def per_device(
    tokens, delta_state, attn_gain, query_weight, key_weight, value_weight, decay_weight,
    beta_weight, decay_rate, head_gain, output_weight, ffn_gain, expert_ids, group_prob,
    expert_logit, expert_gate, expert_up, expert_down, dense_gate, dense_up, dense_down, dense_mix,
):
    n_ep = lax.axis_size("ep")
    n_tp = lax.axis_size("tp")
    rows, width = tokens.shape
    heads = delta_state.shape[1]
    local = heads * 128
    topk = expert_ids.shape[1]
    cap = max(2, 2 * rows * topk // n_ep)
    members = max(2, 8 // math.gcd(cap, 8))
    if n_ep % members:
        members = n_ep
    groups = n_ep // members
    group_slots = members * cap
    chunk = width // n_tp
    depth = width // n_ep
    batch = n_ep * rows
    pairs = n_ep // 2
    lines = n_tp // 2
    hidden = dense_gate.shape[1]
    small = (
        tokens, attn_gain[None, :], decay_rate[None, :], head_gain[None, :], ffn_gain[None, :],
        expert_ids.T, group_prob[None, :], expert_logit.T, dense_mix[None, :],
    )
    weights = (
        delta_state, decay_weight.T, beta_weight.T, query_weight, key_weight, value_weight,
        output_weight, dense_gate, dense_up, expert_gate, expert_up, expert_down, dense_down,
    )
    arrays = tuple(pltpu.with_memory_space_constraint(a, pltpu.HBM) for a in small + weights)
    steps = dense_steps(groups)
    unit_rows = batch // (2 * steps)
    starts, n_sems = semaphores(n_ep, n_tp, members, len(arrays))
    dims = (n_ep, n_tp, rows, width, heads, members, cap, len(arrays), starts)
    vmem = pl.BlockSpec(memory_space=pltpu.VMEM)
    kq_rows = -(-2 * heads // 8) * 8
    scratch = [pltpu.VMEM(a.shape, a.dtype) for a in small + weights[1:]]
    scratch += [
        pltpu.VMEM(shape, dtype)
        for shape, dtype in (
            ((n_ep, rows, depth), BF), ((n_ep, rows, depth), BF),
            ((2, pairs, rows, local), F32), ((pairs, 2, rows, local), BF),
            ((pairs, 2, rows, local), BF), ((rows, local), BF), ((rows, local), BF),
            ((2, pairs, rows, local), BF), ((2, pairs, rows, local), BF),
            ((2, pairs, rows, local), F32),
            ((2, pairs, rows, local), BF), ((2, pairs, rows, local), BF),
            ((n_ep, 8, 128), F32), ((n_ep, 8, 128), F32), ((n_ep, rows, 128), F32),
            ((rows, kq_rows, 128), F32), ((2 * heads, rows, 128), F32),
            ((heads, rows, 128), F32), ((heads, rows, 128), F32), ((rows, local), BF),
            ((n_tp, rows, chunk), BF), ((n_tp, rows, chunk), BF), ((n_tp, rows, 128), F32),
            ((n_ep, 8, 128), F32), ((n_ep, rows, 128), F32), ((rows, chunk), F32),
            ((n_ep, rows, chunk), BF), ((n_tp, groups, group_slots, chunk), BF),
            ((steps, 2, unit_rows, 2 * hidden), F32), ((steps, 2, unit_rows, 2 * hidden), BF),
            ((steps, unit_rows, 2 * hidden), BF), ((steps, lines, unit_rows, 2 * hidden), BF),
            ((2 * steps, unit_rows, hidden), BF),
            ((2, groups, lines, group_slots, chunk), BF), ((groups, lines, group_slots, chunk), BF),
            ((groups, lines, group_slots, chunk), BF), ((groups, lines, group_slots, chunk), BF),
            ((groups, 2, members // 2, rows, chunk), F32),
            ((groups, members // 2, rows, chunk), BF), ((groups, members // 2, rows, chunk), BF),
            ((n_ep, rows, chunk), BF), ((n_ep, rows, chunk), BF),
            ((groups, members * rows, group_slots), BF), ((n_ep, rows, chunk), F32),
        )
    ]
    scratch += [pltpu.SemaphoreType.DMA((n_sems,))]
    mixed_out, new_state = pl.pallas_call(
        functools.partial(kernel, dims),
        out_shape=(pltpu.VMEM((rows, chunk), BF), pltpu.VMEM(delta_state.shape, F32)),
        in_specs=[pl.BlockSpec(memory_space=pltpu.HBM)] * len(arrays),
        out_specs=(vmem, vmem),
        scratch_shapes=scratch,
        compiler_params=pltpu.CompilerParams(
            collective_id=0, has_side_effects=True, vmem_limit_bytes=44 * 1024 * 1024
        ),
    )(*arrays)
    new_state, mixed_out = pl.pallas_call(
        store_kernel,
        out_shape=(pltpu.HBM(delta_state.shape, F32), pltpu.HBM((rows, chunk), BF)),
        in_specs=[vmem] * 2,
        out_specs=(pl.BlockSpec(memory_space=pltpu.HBM),) * 2,
        scratch_shapes=[pltpu.SemaphoreType.DMA((2,))],
        compiler_params=pltpu.CompilerParams(vmem_limit_bytes=8 * 1024 * 1024),
    )(*(pltpu.with_memory_space_constraint(a, pltpu.VMEM) for a in (new_state, mixed_out)))
    return mixed_out, new_state


def solution(mesh):
    return jax.shard_map(
        per_device,
        mesh=mesh,
        in_specs=(
            P("ep", None), P("ep", "tp", None, None), P(), P("ep", "tp"), P("ep", "tp"),
            P("ep", "tp"), P(), P(), P("tp"), P(), P("tp", None), P(), P("ep", None), P("ep"),
            P("ep", None), P("ep", None, "tp"), P("ep", None, "tp"), P("ep", "tp", None),
            P("tp", "ep"), P("tp", "ep"), P("ep", "tp"), P("tp"),
        ),
        out_specs=(P("ep", "tp"), P("ep", "tp", None, None)),
        check_vma=False,
    )
```

```python
import functools
import math

import jax
import jax.numpy as jnp
from jax import lax
from jax.experimental import pallas as pl
from jax.experimental.pallas import tpu as pltpu
from jax.sharding import PartitionSpec as P

EPS = 1e-06
RETURNS = (0, 1, 2, 3)
LAG = 2
STORE = 1
RECALL = 4
UPDATE = 4
X_STRAIGHT = (2,)
F_STRAIGHT = (0, 2)
X_SENDS = (0, 1, 2)
X_ORDER = (2, 0, 1)
BF = jnp.bfloat16
F32 = jnp.float32
MESH = pl.DeviceIdType.MESH


def dot(left, right):
    return jnp.dot(left, right, preferred_element_type=F32)


def dot_t(left, right):
    return lax.dot_general(left, right, (((1,), (1,)), ((), ())), preferred_element_type=F32)


def silu(values):
    return values / (1.0 + jnp.exp(-values))


def far_first(position, count):
    low = 1 - lax.div(2 * position, count)
    order = []
    for k in range(count - 1):
        down = count - 1 - k
        down = down - lax.div(position - down + count, count)
        up = k + lax.div(k - position + count, count)
        order.append(low * down + (1 - low) * up)
    return order


def partners(position, count):
    if count == 4:
        low, high = lax.rem(position, 2), lax.div(position, 2)
        return [3 - position, position + 2 - 4 * high, position + 1 - 2 * low]
    return far_first(position, count)


def store_kernel(state, mixed, state_out, mixed_out, sems):
    rows = state.shape[0]
    small = pltpu.make_async_copy(mixed, mixed_out, sems.at[1])
    small.start()
    step = math.gcd(rows, STORE)
    for r in range(0, rows, step):
        block = pl.ds(r, step)
        pltpu.make_async_copy(state.at[block], state_out.at[block], sems.at[0]).start()
    pltpu.make_async_copy(state, state_out, sems.at[0]).wait()
    small.wait()


def dense_steps(groups):
    return 1 if groups % 2 else groups // 2


def semaphores(n_ep, n_tp, members, n_in):
    groups = n_ep // members
    pairs, lines = n_ep // 2, n_tp // 2
    steps = dense_steps(groups)
    sizes = {
        "load": n_in, "ns": 1, "nr": pairs + 1, "ms": 1, "mr": 1, "cs": 1, "cr": 1, "zs": 1, "zr": 1,
        "q1s": 1, "q1r": 2, "q2s": 1, "q2r": 2, "k1s": 1, "k1r": 1, "k2s": 1, "k2r": 1, "xs": 1, "xr": n_ep,
        "f1s": 1, "f1r": groups, "f2s": 1, "f2r": 1, "as": 1, "ar": 1, "ss": 1, "sr": 1,
        "d1s": 1, "d1r": steps, "d2s": 1, "d2r": steps * lines, "hs": 1, "hr": steps,
        "gs": 1, "gr": groups * n_tp, "e1s": 1, "e1r": groups * lines, "e2s": 1, "e2r": groups,
    }
    starts, total = {}, 0
    for name, size in sizes.items():
        starts[name] = total
        total += size
    return starts, total


def kernel(dims, *refs):
    n_ep, n_tp, rows, width, heads, members, cap, n_in, starts = dims
    hbm, refs = refs[:n_in], refs[n_in:]
    out, state = refs[:2]
    held = refs[2 : 11] + (state,) + refs[11 : 1 + n_in]
    refs = refs[1 + n_in :]
    (tokens, attn_gain, decay_rate, head_gain, ffn_gain, ids, group_prob, logit, mix) = held[:9]
    state, w_decay, w_beta, w_q, w_k, w_v, w_o, w_dg, w_du, w_eg, w_eu, w_ed, w_dd = held[9:]
    (
        n_send, n_recv, k_own, k_send, k_recv, k_away, k_mate, q_away, q_mate, q_own, q_send, q_recv, c_send, c_rows, c_recv, kq, recall,
        corr_ref, decay_ref, head_out, a_send, a_recv, s_recv, scale_rows, scale_ref, middle_ref,
        x_all, g_all, d_half, d_send, d_near, d_far, h_all, e_part, e_near, e_send, e_recv,
        comb, f_away, f_mate, f_send, f_recv, place_ref, dense_ref, sems,
    ) = refs
    me = lax.axis_index("ep")
    my = lax.axis_index("tp")
    chunk = width // n_tp
    depth = width // n_ep
    batch = n_ep * rows
    local = heads * 128
    groups = n_ep // members
    group_slots = members * cap
    group_tokens = members * rows
    slots = groups * group_slots
    pairs = n_ep // 2
    lines = n_tp // 2
    group_pairs = members // 2
    pair = lax.div(me, 2)
    par = lax.rem(me, 2)
    mate = me + 1 - 2 * par
    core = lax.rem(my, 2)
    line = lax.div(my, 2)
    sibling = my + 1 - 2 * core
    my_group = lax.div(pair, group_pairs)
    far_groups = partners(my_group, groups)
    x_straight = {4: X_STRAIGHT, 2: (0,)}.get(groups, ())
    f_straight = {4: F_STRAIGHT, 2: (0,)}.get(groups, ())
    x_sends = X_SENDS if groups == 4 else range(groups - 1)
    x_order = X_ORDER if groups == 4 else range(groups - 1)
    far_lines = [lax.rem(line + d, lines) for d in range(1, lines)]

    def same_core(y):
        return 2 * y + core

    def other_core(y):
        return 2 * y + 1 - core

    def twin(q):
        return 2 * q + par

    def cross(q):
        return 2 * q + 1 - par

    def pairs_in(g, own=False):
        mine = lax.rem(pair, group_pairs)
        return [
            g * group_pairs + lax.rem(mine + m, group_pairs)
            for m in range(1 if own else 0, group_pairs)
        ]

    others = [q for g in far_groups for q in pairs_in(g)] + pairs_in(my_group, True)
    ep_peers = [p for q in others for p in (cross(q), twin(q))] + [mate]
    far_tp = [p for y in far_lines for p in (same_core(y), other_core(y))]
    tp_peers = far_tp + [sibling]

    def sem(name, index=0):
        return sems.at[starts[name] + index]

    def ep_copy(src, dst, name, peer, index=0):
        return pltpu.make_async_remote_copy(
            src_ref=src, dst_ref=dst, send_sem=sem(name + "s"), recv_sem=sem(name + "r", index),
            device_id=(peer, my), device_id_type=MESH,
        )

    def tp_copy(src, dst, name, peer, index=0):
        return pltpu.make_async_remote_copy(
            src_ref=src, dst_ref=dst, send_sem=sem(name + "s"), recv_sem=sem(name + "r", index),
            device_id=(me, peer), device_id_type=MESH,
        )

    drains = []

    loads = [
        pltpu.make_async_copy(src, dst, sem("load", i))
        for i, (src, dst) in enumerate(zip(hbm, held))
    ]
    state_i, decay_i, beta_i, q_i, k_i, v_i, o_i, dg_i, du_i, eg_i, eu_i, ed_i, dd_i = range(9, 22)
    order = (decay_i, beta_i, k_i, q_i, v_i, state_i, o_i, dg_i, du_i, eg_i, eu_i, ed_i, dd_i)
    for i in range(9):
        loads[i].start()
    barrier = pltpu.get_barrier_semaphore()
    for p in ep_peers:
        pl.semaphore_signal(barrier, inc=1, device_id=(p, my), device_id_type=MESH)
    for p in tp_peers:
        pl.semaphore_signal(barrier, inc=1, device_id=(me, p), device_id_type=MESH)
    for i in order:
        loads[i].start()

    for i in range(9):
        loads[i].wait()
    x = tokens[...].astype(F32)
    mean_sq = jnp.mean(x * x, axis=-1, keepdims=True)
    normed = (x * lax.rsqrt(mean_sq + EPS) * attn_gain[...]).astype(BF)
    for p in range(n_ep):
        n_send[p] = normed[:, p * depth : (p + 1) * depth]
    pl.semaphore_wait(barrier, n_ep + n_tp - 2)
    def shelf(p):
        return lax.rem(p, 2) * pairs + lax.div(p, 2)

    def carried(q):
        return 2 * q + lax.rem(par + pair + q + core, 2)

    for q in others:
        ep_copy(n_send.at[carried(q)], n_recv.at[shelf(me)], "n", carried(q), pair).start()
    ep_copy(n_send.at[mate], n_recv.at[shelf(me)], "n", mate, pairs).start()
    n_recv[shelf(me)] = n_send[me]

    logit_exp = jnp.exp(logit[...])
    route = group_prob[...] * logit_exp / jnp.sum(logit_exp, axis=0, keepdims=True)
    names = ids[...]
    eye = lax.broadcasted_iota(jnp.int32, (rows, rows), 0) == lax.broadcasted_iota(
        jnp.int32, (rows, rows), 1
    )
    c_send[...] = jnp.zeros_like(c_send)
    for p in range(n_ep):
        flat = jnp.sum(jnp.where(names == p, route, 0.0), axis=0, keepdims=True)
        c_send[p, :, :rows] = jnp.broadcast_to(flat, (8, rows))
    for p in ep_peers:
        ep_copy(c_send.at[p], c_rows.at[me], "c", p).start()
    c_rows[me] = c_send[me]

    def column(row):
        return jnp.sum(jnp.where(eye, row[:, :rows], 0.0), axis=1, keepdims=True)

    loads[decay_i].wait()
    loads[beta_i].wait()
    decay_pre = dot_t(normed, w_decay[...])
    beta_pre = dot_t(normed, w_beta[...])
    lane = lax.broadcasted_iota(jnp.int32, decay_pre.shape, 1)
    decays, betas = [], []
    for h in range(heads):
        mine = lane == my * heads + h
        d = jnp.sum(jnp.where(mine, decay_pre, 0.0), axis=1, keepdims=True)
        b = jnp.sum(jnp.where(mine, beta_pre, 0.0), axis=1, keepdims=True)
        soft = jnp.maximum(d, 0.0) + jnp.log1p(jnp.exp(-jnp.abs(d)))
        decays.append(jnp.exp(-decay_rate[:, h : h + 1] * soft))
        betas.append(1.0 / (1.0 + jnp.exp(-b)))
    for i in (q_i, k_i, v_i):
        loads[i].wait()

    most = pl.ds(0, n_ep - 1)
    some = pl.ds(0, pairs - 1)
    for q in others:
        block = n_recv.at[shelf(carried(q))]
        ep_copy(block, block, "n", mate, q).wait_recv()
        tp_copy(block, block, "m", sibling).start()
    ep_copy(n_send.at[mate], n_recv.at[shelf(mate)], "n", mate, pairs).wait_recv()
    drains.append(ep_copy(n_send.at[pl.ds(0, pairs)], n_recv.at[pl.ds(0, pairs)], "n", mate))
    passed = tp_copy(n_recv.at[some], n_recv.at[some], "m", sibling)
    passed.wait_recv()
    drains.append(passed)

    def rows_of(parity):
        held_rows = n_recv[pl.ds(parity * pairs, pairs)].astype(F32)
        return held_rows.reshape(pairs * rows, depth).astype(BF)

    away, near = rows_of(1 - par), rows_of(par)
    k_part = dot(jnp.concatenate([away, near], axis=0), w_k[...]).reshape(2, pairs, rows, local)
    k_own[...] = k_part
    for side in range(2):
        k_send[:, side] = k_part[side].astype(BF)
    for q in others:
        ep_copy(k_send.at[q], k_recv.at[pair], "k1", twin(q)).start()
    for j, w in enumerate((w_q, w_v)):
        q_away[j] = dot(away, w[...]).reshape(pairs, rows, local).astype(BF)
        ep_copy(q_away.at[j], q_mate.at[j], "q1", mate, j).start()
    for j, w in enumerate((w_q, w_v)):
        q_own[j] = dot(near, w[...]).reshape(pairs, rows, local)
    for j in range(2):
        ep_copy(q_away.at[j], q_mate.at[j], "q1", mate, j).wait_recv()
        both = q_own[j] + q_mate[j].astype(F32)
        q_own[j] = both
        q_send[j] = both.astype(BF)
        for q in others:
            ep_copy(q_send.at[j, q], q_recv.at[j, pair], "q2", twin(q), j).start()
    drains.append(ep_copy(q_away, q_mate, "q1", mate))
    far_blocks = pl.ds(0, pairs - 1)
    sent = q_send.at[pl.ds(0, 2), far_blocks]
    drains.append(ep_copy(sent, q_recv.at[pl.ds(0, 2), far_blocks], "q2", mate))
    done_k = ep_copy(k_send.at[far_blocks], k_recv.at[far_blocks], "k1", mate)
    done_k.wait_recv()
    drains.append(done_k)
    sums = []
    for side in range(2):
        total = k_own[side, pair]
        for q in others:
            total = total + k_recv[q, side].astype(F32)
        sums.append(total)
        if side == 0:
            k_away[...] = total.astype(BF)
            cross_k = ep_copy(k_away, k_mate, "k2", mate)
            cross_k.start()
            drains.append(cross_k)

    def summed(j):
        ep_copy(
            q_send.at[j, far_blocks], q_recv.at[j, far_blocks], "q2", mate, j
        ).wait_recv()
        total = q_own[j, pair]
        for q in others:
            total = total + q_recv[j, q].astype(F32)
        return total.astype(BF).astype(F32)

    q_rows = summed(0)
    cross_k.wait_recv()
    k_rows = (sums[1] + k_mate[...].astype(F32)).astype(BF).astype(F32)
    loads[state_i].wait()

    def head_of(values, h):
        return values[:, h * 128 : (h + 1) * 128]

    def unit(values):
        return values * lax.rsqrt(jnp.sum(values * values, axis=-1, keepdims=True) + EPS)

    units = []
    for h in range(heads):
        q_unit = unit(head_of(q_rows, h)) * 128 ** (-0.5)
        k_unit = unit(head_of(k_rows, h))
        units.append((q_unit, k_unit))
        kq[:, h, :] = k_unit
        kq[:, heads + h, :] = q_unit

    beside = 2 if heads % 2 == 0 else 1

    def one_row(b, _):
        both = kq[b].astype(BF)
        for first in range(0, heads, beside):
            pieces = [state[b, first + i].astype(BF) for i in range(beside)]
            read = dot(both, jnp.concatenate(pieces, axis=1))
            for i in range(beside):
                h, lanes = first + i, slice(i * 128, (i + 1) * 128)
                recall[h, pl.ds(b, 1), :] = read[h : h + 1, lanes]
                recall[heads + h, pl.ds(b, 1), :] = read[heads + h : heads + h + 1, lanes]
        return 0

    lax.fori_loop(0, rows, one_row, 0, unroll=RECALL)
    v_rows = summed(1)
    for h in range(heads):
        q_unit, k_unit = units[h]
        decay, beta = decays[h], betas[h]
        corr = beta * (head_of(v_rows, h) - decay * recall[h])
        read = decay * recall[heads + h] + jnp.sum(q_unit * k_unit, axis=-1, keepdims=True) * corr
        read = read * lax.rsqrt(jnp.mean(read * read, axis=-1, keepdims=True) + EPS) * head_gain[...]
        head_out[:, h * 128 : (h + 1) * 128] = read.astype(BF)
        corr_ref[h] = corr
        decay_ref[h] = jnp.broadcast_to(decay, (rows, 128))

    loads[o_i].wait()
    ho = head_out[...]

    def columns_of(p):
        return pl.ds(pl.multiple_of(p * chunk, 128), chunk)

    for p in far_tp + [sibling]:
        a_send[p] = dot(ho, w_o[:, columns_of(p)]).astype(BF)
        tp_copy(a_send.at[p], a_recv.at[my], "a", p).start()
    a_recv[my] = dot(ho, w_o[:, columns_of(my)]).astype(BF)
    own = columns_of(my)

    def update_row(b, _):
        columns = kq[b].T
        for h in range(heads):
            corr = corr_ref[h, pl.ds(b, 1), :]
            decay = decay_ref[h, pl.ds(b, 1), :]
            state[b, h] = decay * state[b, h] + columns[:, h : h + 1] * corr
        return 0

    lax.fori_loop(0, rows // 2, update_row, 0, unroll=UPDATE)
    middle = tokens[:, own].astype(F32)
    most_tp = pl.ds(0, n_tp - 1)
    done_a = tp_copy(a_send.at[most_tp], a_recv.at[most_tp], "a", sibling)
    done_a.wait_recv()
    drains.append(done_a)
    for p in range(n_tp):
        middle = middle + a_recv[p].astype(F32)
    x_all[me] = (middle * ffn_gain[:, own]).astype(BF)
    x_peers = [mate] + [twin(q) for q in pairs_in(my_group, True)]
    for i in x_sends:
        x_peers += [twin(q) for q in pairs_in(far_groups[i])]
        if i in x_straight:
            x_peers += [cross(q) for q in pairs_in(far_groups[i])]
    for p in x_peers:
        ep_copy(x_all.at[me], x_all.at[me], "x", p, me).start()
    middle_ref[...] = middle
    s_recv[my] = jnp.broadcast_to(jnp.sum(middle * middle, axis=-1, keepdims=True), (rows, 128))
    for p in tp_peers:
        tp_copy(s_recv.at[my], s_recv.at[my], "s", p).start()
    lax.fori_loop(rows // 2, rows, update_row, 0, unroll=UPDATE)
    done_c = ep_copy(c_send.at[most], c_rows.at[most], "c", mate)
    done_c.wait_recv()
    drains.append(done_c)
    for p in range(n_ep):
        c_recv[p] = jnp.broadcast_to(column(c_rows[p, :1, :]), (rows, 128))
    tri = (
        lax.broadcasted_iota(jnp.int32, (group_tokens, group_tokens), 0)
        >= lax.broadcasted_iota(jnp.int32, (group_tokens, group_tokens), 1)
    ).astype(F32).astype(BF)
    slot = lax.broadcasted_iota(jnp.int32, (group_tokens, group_slots), 1).astype(F32)
    for g in range(groups):
        coef = c_recv[g * members : (g + 1) * members].reshape(group_tokens, 128)[:, :1]
        named = coef > 0.0
        flags = jnp.broadcast_to(jnp.where(named, 1.0, 0.0), (group_tokens, 128)).astype(BF)
        rank = dot(tri, flags)[:, :1] - 1.0
        place_ref[g] = jnp.where((rank == slot) & named, 1.0, 0.0).astype(BF)
    done_s = tp_copy(s_recv.at[most_tp], s_recv.at[most_tp], "s", sibling)
    done_s.wait_recv()
    drains.append(done_s)
    total = s_recv[0]
    for p in range(1, n_tp):
        total = total + s_recv[p]
    scale = lax.rsqrt(total / width + EPS)
    diagonal = lax.broadcasted_iota(jnp.int32, (rows, 128), 0) == lax.broadcasted_iota(
        jnp.int32, (rows, 128), 1
    )
    scale_rows[me] = jnp.broadcast_to(
        jnp.sum(jnp.where(diagonal, scale, 0.0), axis=0, keepdims=True), (8, 128)
    )
    for p in ep_peers:
        ep_copy(scale_rows.at[me], scale_rows.at[me], "z", p).start()

    def send_g(k, g):
        block = g_all.at[my, g]
        for p in [sibling] + [same_core(y) for y in far_lines]:
            tp_copy(block, block, "g", p, k * n_tp + my).start()

    def pass_on(k, g):
        for y in far_lines:
            p = same_core(y)
            block = g_all.at[p, g]
            tp_copy(block, block, "g", p, k * n_tp + p).wait_recv()
            tp_copy(block, block, "g", sibling, k * n_tp + p).start()

    def arrived_g(k, g, p):
        block = g_all.at[p, g]
        tp_copy(block, block, "g", p, k * n_tp + p).wait_recv()

    def forward_x(k):
        for q in pairs_in(group_from[k], k == 0):
            block = x_all.at[twin(q)]
            ep_copy(block, block, "x", twin(q), twin(q)).wait_recv()
            ep_copy(block, block, "x", mate, twin(q)).start()

    group_from = [my_group] + [far_groups[i] for i in x_order]
    hidden = w_dg.shape[1]
    if groups % 2:
        units = [(u * pairs, pairs) for u in range(2)]
    else:
        units = [(g * members, members) for g in group_from]
    steps = len(units) // 2
    unit_rows = units[0][1] * rows
    loads[dg_i].wait()
    loads[du_i].wait()

    def unit_of(ref, u):
        start, count = units[u]
        return ref.at[pl.ds(start, count)]

    def near_d(h):
        return tp_copy(d_send.at[h, 1], d_near.at[h], "d1", sibling, h)

    def far_d(h, y, source):
        return tp_copy(d_send.at[h, 0], d_far.at[h, source], "d2", same_core(y), h * lines + source)

    def dense_dots(h):
        xs = jnp.concatenate(
            [
                unit_of(x_all, 2 * h + u)[...].astype(F32).reshape(unit_rows, chunk)
                for u in range(2)
            ],
            axis=0,
        ).astype(BF)
        for j, w in enumerate((w_dg, w_du)):
            part = dot(xs, w[...]).reshape(2, unit_rows, hidden)
            d_half[h, :, :, j * hidden : (j + 1) * hidden] = part
        d_send[h, 1] = d_half[h, 1 - core].astype(BF)
        near_d(h).start()

    def dense_cross(h):
        near_d(h).wait_recv()
        pre = d_half[h, core] + d_near[h].astype(F32)
        d_half[h, 0] = pre
        d_send[h, 0] = pre.astype(BF)
        for y in far_lines:
            far_d(h, y, line).start()

    def dense_hide(h):
        pre = d_half[h, 0]
        for y in far_lines:
            far_d(h, y, y).wait_recv()
            pre = pre + d_far[h, y].astype(F32)
        first, count = units[2 * h][0] * (1 - core) + units[2 * h + 1][0] * core, units[2 * h][1]
        pre = pre * scale_ref[pl.ds(first, count)].reshape(unit_rows, 128)[:, :1]
        h_all[2 * h + core] = (silu(pre[:, :hidden]) * pre[:, hidden:]).astype(BF)
        sent_h(h).start()

    def sent_h(h):
        return tp_copy(h_all.at[2 * h + core], h_all.at[2 * h + core], "h", sibling, h)

    forward_x(0)
    relayed = [k + 1 for k, i in enumerate(x_order) if i not in x_straight]
    for k in range(groups):
        g = group_from[k]
        if k < len(relayed):
            forward_x(relayed[k])
        if k > 0 and k not in relayed:
            for q in pairs_in(g):
                ep_copy(x_all.at[me], x_all.at[twin(q)], "x", mate, twin(q)).wait_recv()
        for q in pairs_in(g, k == 0) + ([pair] if k == 0 else []):
            ep_copy(x_all.at[me], x_all.at[cross(q)], "x", mate, cross(q)).wait_recv()
        block = x_all[pl.ds(g * members, members)].astype(F32)
        g_all[my, g] = lax.dot_general(
            place_ref[g], block.reshape(group_tokens, chunk).astype(BF),
            (((0,), (0,)), ((), ())), preferred_element_type=F32,
        ).astype(BF)
        send_g(k, g)
        if k > 1:
            pass_on(k - 2, group_from[k - 2])
        if steps == 2 and k == 1:
            dense_dots(0)
    drains.append(ep_copy(x_all.at[most], x_all.at[most], "x", mate))
    drains.append(tp_copy(g_all.at[most_tp], g_all.at[most_tp], "g", sibling))
    for i in (eg_i, eu_i, ed_i, dd_i):
        loads[i].wait()
    if steps == 2:
        dense_cross(0)
    for h in range(0 if steps != 2 else 1, steps):
        dense_dots(h)
    if groups > 1:
        pass_on(groups - 2, group_from[groups - 2])

    def expert_in(p, gate, up):
        routed = g_all[p].astype(F32).reshape(slots, chunk).astype(BF)
        return (
            gate + dot(routed, w_eg[0, columns_of(p), :]), up + dot(routed, w_eu[0, columns_of(p), :])
        )

    gate = jnp.zeros((slots, w_eg.shape[2]), F32)
    gate, up = expert_in(my, gate, gate)
    pass_on(groups - 1, group_from[groups - 1])
    for h in range(0 if steps != 2 else 1, steps):
        dense_cross(h)
    for k in range(groups):
        arrived_g(k, group_from[k], sibling)
    gate, up = expert_in(sibling, gate, up)
    done_z = ep_copy(scale_rows.at[most], scale_rows.at[most], "z", mate)
    done_z.wait_recv()
    drains.append(done_z)
    for p in range(n_ep):
        scale_ref[p] = jnp.broadcast_to(column(scale_rows[p, :1, :]), (rows, 128))
    slot_scale = jnp.concatenate(
        [
            lax.dot_general(
                place_ref[g].astype(F32),
                scale_ref[g * members : (g + 1) * members].reshape(group_tokens, 128),
                (((0,), (0,)), ((), ())), precision=lax.Precision.HIGHEST,
                preferred_element_type=F32,
            )
            for g in range(groups)
        ],
        axis=0,
    )[:, :1]
    for h in range(steps - 1):
        dense_hide(h)
    for y in far_lines:
        gate, up = expert_in(same_core(y), gate, up)
    for y in far_lines:
        for k in range(groups):
            arrived_g(k, group_from[k], other_core(y))
        gate, up = expert_in(other_core(y), gate, up)
    expert_hidden = (silu(gate * slot_scale) * (up * slot_scale)).astype(BF)
    order_back = RETURNS if groups == 4 else tuple(range(groups))
    returns = [(far_groups + [my_group])[i] for i in order_back]
    own_at = order_back.index(groups - 1)
    f_direct = [k for k in range(groups) if order_back[k] in f_straight]

    def near_e(k, y):
        g = returns[k]
        return tp_copy(e_part.at[1 - core, g, y], e_near.at[g, y], "e1", sibling, k * lines + y)

    def far_e(k, y):
        g = returns[k]
        return tp_copy(e_send.at[g, y], e_recv.at[g, line], "e2", same_core(y), k)

    def expert_out(which, y):
        part = dot(expert_hidden, w_ed[0, :, columns_of(2 * y + which)])
        e_part[which, :, y] = part.reshape(groups, group_slots, chunk).astype(BF)

    for y in far_lines + [line]:
        expert_out(1 - core, y)
        for k in range(groups):
            near_e(k, y).start()
    for y in far_lines + [line]:
        expert_out(core, y)
    for k in range(groups):
        g = returns[k]
        for y in far_lines:
            near_e(k, y).wait_recv()
            e_send[g, y] = (e_part[core, g, y].astype(F32) + e_near[g, y].astype(F32)).astype(BF)
            far_e(k, y).start()
    drains.append(tp_copy(e_part.at[0], e_near, "e1", sibling))
    other_lines = pl.ds(0, lines - 1)
    sent = e_send.at[pl.ds(0, groups), other_lines]
    drains.append(tp_copy(sent, e_recv.at[pl.ds(0, groups), other_lines], "e2", sibling))
    dense_hide(steps - 1)
    for h in range(steps):
        tp_copy(h_all.at[core], h_all.at[2 * h + 1 - core], "h", sibling, h).wait_recv()
    drains.append(tp_copy(h_all.at[pl.ds(0, steps)], h_all.at[pl.ds(0, steps)], "h", sibling))
    sent = d_send.at[pl.ds(0, steps), 1]
    drains.append(tp_copy(sent, d_near, "d1", sibling))
    for y in far_lines:
        sent = d_send.at[pl.ds(0, steps), 0]
        drains.append(tp_copy(sent, d_far.at[pl.ds(0, steps), line], "d2", same_core(y)))
    dense_hidden = h_all[...].astype(F32).reshape(batch, hidden).astype(BF)
    dense = dot(dense_hidden, w_dd[...]) * (1.0 / (1.0 + jnp.exp(-mix[...])))
    for u in range(len(units)):
        part = dense[u * unit_rows : (u + 1) * unit_rows]
        unit_of(dense_ref, u)[...] = part.reshape(units[u][1], rows, chunk)

    def near_f(k):
        g = returns[k]
        return ep_copy(f_away.at[g], f_mate.at[g], "f1", mate, k)

    def far_f(k):
        g = returns[k]
        near_f(k).wait_recv()
        both = comb[g, par] + f_mate[g].astype(F32)
        comb[g, par] = both
        send_f(g, both, k == own_at)

    def send_f(g, values, own_group):
        f_send[pl.ds(g * group_pairs, group_pairs)] = values.astype(BF)
        for q in pairs_in(g, own_group):
            ep_copy(f_send.at[q], f_recv.at[pair], "f2", twin(q)).start()

    def straight_f(k, g):
        send_f(g, comb[g, par], False)
        first = pairs + f_straight.index(order_back[k]) * group_pairs
        f_send[pl.ds(first, group_pairs)] = comb[g, 1 - par].astype(BF)
        for m in range(group_pairs):
            spare = first + lax.rem(pair, group_pairs)
            q = g * group_pairs + m
            ep_copy(f_send.at[first + m], f_recv.at[spare], "f2", cross(q)).start()

    for k in range(groups):
        g = returns[k]
        block = pl.ds(g * members, members)
        near_e(k, line).wait_recv()
        result = e_part[core, g, line].astype(F32) + e_near[g, line].astype(F32)
        tp_copy(e_send.at[g, other_lines], e_recv.at[g, other_lines], "e2", sibling, k).wait_recv()
        for y in far_lines:
            result = result + e_recv[g, y].astype(F32)
        coef = c_recv[block].reshape(group_tokens, 128)[:, :1]
        mixed = coef * dot(place_ref[g], result.astype(BF))
        combined = dense_ref[block] + mixed.reshape(members, rows, chunk)
        for m in range(members):
            comb[g, m % 2, m // 2] = combined[m]
        if k in f_direct:
            straight_f(k, g)
        else:
            f_away[g] = comb[g, 1 - par].astype(BF)
            near_f(k).start()
        if k >= LAG and k - LAG not in f_direct:
            far_f(k - LAG)
    for k in range(max(0, groups - LAG), groups):
        if k not in f_direct:
            far_f(k)
    met = pl.ds(0, groups - len(f_direct))
    drains.append(ep_copy(f_away.at[met], f_mate.at[met], "f1", mate))
    spares = list(range(pairs, pairs + len(f_straight) * group_pairs))
    sent = pl.ds(0, pairs - 1 + len(spares))
    drains.append(ep_copy(f_send.at[sent], f_recv.at[sent], "f2", mate))
    final = middle_ref[...] + comb[my_group, par, lax.rem(pair, group_pairs)]
    ep_copy(f_send.at[sent], f_recv.at[sent], "f2", mate).wait_recv()
    for q in others + spares:
        final = final + f_recv[q].astype(F32)
    out[...] = final.astype(BF)
    for copy in drains:
        copy.wait_send()


def per_device(
    tokens, delta_state, attn_gain, query_weight, key_weight, value_weight, decay_weight,
    beta_weight, decay_rate, head_gain, output_weight, ffn_gain, expert_ids, group_prob,
    expert_logit, expert_gate, expert_up, expert_down, dense_gate, dense_up, dense_down, dense_mix,
):
    n_ep = lax.axis_size("ep")
    n_tp = lax.axis_size("tp")
    rows, width = tokens.shape
    heads = delta_state.shape[1]
    local = heads * 128
    topk = expert_ids.shape[1]
    cap = max(2, 2 * rows * topk // n_ep)
    members = max(2, 8 // math.gcd(cap, 8))
    if n_ep % members:
        members = n_ep
    groups = n_ep // members
    group_slots = members * cap
    chunk = width // n_tp
    depth = width // n_ep
    batch = n_ep * rows
    pairs = n_ep // 2
    lines = n_tp // 2
    hidden = dense_gate.shape[1]
    small = (
        tokens, attn_gain[None, :], decay_rate[None, :], head_gain[None, :], ffn_gain[None, :],
        expert_ids.T, group_prob[None, :], expert_logit.T, dense_mix[None, :],
    )
    weights = (
        delta_state, decay_weight.T, beta_weight.T, query_weight, key_weight, value_weight,
        output_weight, dense_gate, dense_up, expert_gate, expert_up, expert_down, dense_down,
    )
    arrays = tuple(pltpu.with_memory_space_constraint(a, pltpu.HBM) for a in small + weights)
    steps = dense_steps(groups)
    unit_rows = batch // (2 * steps)
    starts, n_sems = semaphores(n_ep, n_tp, members, len(arrays))
    dims = (n_ep, n_tp, rows, width, heads, members, cap, len(arrays), starts)
    vmem = pl.BlockSpec(memory_space=pltpu.VMEM)
    kq_rows = -(-2 * heads // 8) * 8
    scratch = [pltpu.VMEM(a.shape, a.dtype) for a in small + weights[1:]]
    scratch += [
        pltpu.VMEM(shape, dtype)
        for shape, dtype in (
            ((n_ep, rows, depth), BF), ((n_ep, rows, depth), BF),
            ((2, pairs, rows, local), F32), ((pairs, 2, rows, local), BF),
            ((pairs, 2, rows, local), BF), ((rows, local), BF), ((rows, local), BF),
            ((2, pairs, rows, local), BF), ((2, pairs, rows, local), BF),
            ((2, pairs, rows, local), F32),
            ((2, pairs, rows, local), BF), ((2, pairs, rows, local), BF),
            ((n_ep, 8, 128), F32), ((n_ep, 8, 128), F32), ((n_ep, rows, 128), F32),
            ((rows, kq_rows, 128), F32), ((2 * heads, rows, 128), F32),
            ((heads, rows, 128), F32), ((heads, rows, 128), F32), ((rows, local), BF),
            ((n_tp, rows, chunk), BF), ((n_tp, rows, chunk), BF), ((n_tp, rows, 128), F32),
            ((n_ep, 8, 128), F32), ((n_ep, rows, 128), F32), ((rows, chunk), F32),
            ((n_ep, rows, chunk), BF), ((n_tp, groups, group_slots, chunk), BF),
            ((steps, 2, unit_rows, 2 * hidden), F32), ((steps, 2, unit_rows, 2 * hidden), BF),
            ((steps, unit_rows, 2 * hidden), BF), ((steps, lines, unit_rows, 2 * hidden), BF),
            ((2 * steps, unit_rows, hidden), BF),
            ((2, groups, lines, group_slots, chunk), BF), ((groups, lines, group_slots, chunk), BF),
            ((groups, lines, group_slots, chunk), BF), ((groups, lines, group_slots, chunk), BF),
            ((groups, 2, members // 2, rows, chunk), F32),
            ((groups, members // 2, rows, chunk), BF), ((groups, members // 2, rows, chunk), BF),
            ((n_ep, rows, chunk), BF), ((n_ep, rows, chunk), BF),
            ((groups, members * rows, group_slots), BF), ((n_ep, rows, chunk), F32),
        )
    ]
    scratch += [pltpu.SemaphoreType.DMA((n_sems,))]
    mixed_out, new_state = pl.pallas_call(
        functools.partial(kernel, dims),
        out_shape=(pltpu.VMEM((rows, chunk), BF), pltpu.VMEM(delta_state.shape, F32)),
        in_specs=[pl.BlockSpec(memory_space=pltpu.HBM)] * len(arrays),
        out_specs=(vmem, vmem),
        scratch_shapes=scratch,
        compiler_params=pltpu.CompilerParams(
            collective_id=0, has_side_effects=True, vmem_limit_bytes=44 * 1024 * 1024
        ),
    )(*arrays)
    new_state, mixed_out = pl.pallas_call(
        store_kernel,
        out_shape=(pltpu.HBM(delta_state.shape, F32), pltpu.HBM((rows, chunk), BF)),
        in_specs=[vmem] * 2,
        out_specs=(pl.BlockSpec(memory_space=pltpu.HBM),) * 2,
        scratch_shapes=[pltpu.SemaphoreType.DMA((2,))],
        compiler_params=pltpu.CompilerParams(vmem_limit_bytes=8 * 1024 * 1024),
    )(*(pltpu.with_memory_space_constraint(a, pltpu.VMEM) for a in (new_state, mixed_out)))
    return mixed_out, new_state


def solution(mesh):
    return jax.shard_map(
        per_device,
        mesh=mesh,
        in_specs=(
            P("ep", None), P("ep", "tp", None, None), P(), P("ep", "tp"), P("ep", "tp"),
            P("ep", "tp"), P(), P(), P("tp"), P(), P("tp", None), P(), P("ep", None), P("ep"),
            P("ep", None), P("ep", None, "tp"), P("ep", None, "tp"), P("ep", "tp", None),
            P("tp", "ep"), P("tp", "ep"), P("ep", "tp"), P("tp"),
        ),
        out_specs=(P("ep", "tp"), P("ep", "tp", None, None)),
        check_vma=False,
    )
```

```python
import functools
import math

import jax
import jax.numpy as jnp
from jax import lax
from jax.experimental import pallas as pl
from jax.experimental.pallas import tpu as pltpu
from jax.sharding import PartitionSpec as P

EPS = 1e-06
RETURNS = (0, 1, 2, 3)
LAG = 2
STORE = 1
RECALL = 4
UPDATE = 4
LOADED_WITH = (0,) * 9 + (1, 2, 2, 3, 3, 3, 4, 5, 5, 6, 6, 6, 6)
X_STRAIGHT = (2,)
F_STRAIGHT = (0, 2)
X_SENDS = (0, 1, 2)
X_ORDER = (2, 0, 1)
BF = jnp.bfloat16
F32 = jnp.float32
MESH = pl.DeviceIdType.MESH


def dot(left, right):
    return jnp.dot(left, right, preferred_element_type=F32)


def dot_t(left, right):
    return lax.dot_general(left, right, (((1,), (1,)), ((), ())), preferred_element_type=F32)


def silu(values):
    return values / (1.0 + jnp.exp(-values))


def far_first(position, count):
    low = 1 - lax.div(2 * position, count)
    order = []
    for k in range(count - 1):
        down = count - 1 - k
        down = down - lax.div(position - down + count, count)
        up = k + lax.div(k - position + count, count)
        order.append(low * down + (1 - low) * up)
    return order


def partners(position, count):
    if count == 4:
        low, high = lax.rem(position, 2), lax.div(position, 2)
        return [3 - position, position + 2 - 4 * high, position + 1 - 2 * low]
    return far_first(position, count)


def store_kernel(state, mixed, state_out, mixed_out, sems):
    rows = state.shape[0]
    small = pltpu.make_async_copy(mixed, mixed_out, sems.at[1])
    small.start()
    step = math.gcd(rows, STORE)
    for r in range(0, rows, step):
        block = pl.ds(r, step)
        pltpu.make_async_copy(state.at[block], state_out.at[block], sems.at[0]).start()
    pltpu.make_async_copy(state, state_out, sems.at[0]).wait()
    small.wait()


def dense_steps(groups):
    return 1 if groups % 2 else groups // 2


def semaphores(n_ep, n_tp, members, n_in):
    groups = n_ep // members
    pairs, lines = n_ep // 2, n_tp // 2
    steps = dense_steps(groups)
    sizes = {
        "load": max(LOADED_WITH) + 1, "ns": 1, "nr": pairs + 1, "ms": 1, "mr": 1, "cs": 1, "cr": 1, "zs": 1, "zr": 1,
        "q1s": 1, "q1r": 2, "q2s": 1, "q2r": 2, "k1s": 1, "k1r": 1, "k2s": 1, "k2r": 1, "xs": 1, "xr": n_ep,
        "f1s": 1, "f1r": groups, "f2s": 1, "f2r": 1, "as": 1, "ar": 1, "ss": 1, "sr": 1,
        "d1s": 1, "d1r": steps, "d2s": 1, "d2r": steps * lines, "hs": 1, "hr": steps,
        "gs": 1, "gr": groups * n_tp, "e1s": 1, "e1r": groups * lines, "e2s": 1, "e2r": groups,
    }
    starts, total = {}, 0
    for name, size in sizes.items():
        starts[name] = total
        total += size
    return starts, total


def kernel(dims, *refs):
    n_ep, n_tp, rows, width, heads, members, cap, n_in, starts = dims
    hbm, refs = refs[:n_in], refs[n_in:]
    out, state = refs[:2]
    held = refs[2 : 11] + (state,) + refs[11 : 1 + n_in]
    refs = refs[1 + n_in :]
    (tokens, attn_gain, decay_rate, head_gain, ffn_gain, ids, group_prob, logit, mix) = held[:9]
    state, w_decay, w_beta, w_q, w_k, w_v, w_o, w_dg, w_du, w_eg, w_eu, w_ed, w_dd = held[9:]
    (
        n_send, n_recv, k_own, k_send, k_recv, k_away, k_mate, q_away, q_mate, q_own, q_send, q_recv, c_send, c_rows, c_recv, kq, recall,
        corr_ref, decay_ref, head_out, a_send, a_recv, s_recv, scale_rows, scale_ref, middle_ref,
        x_all, g_all, d_half, d_send, d_near, d_far, h_all, e_part, e_near, e_send, e_recv,
        comb, f_away, f_mate, f_send, f_recv, place_ref, dense_ref, sems,
    ) = refs
    me = lax.axis_index("ep")
    my = lax.axis_index("tp")
    chunk = width // n_tp
    depth = width // n_ep
    batch = n_ep * rows
    local = heads * 128
    groups = n_ep // members
    group_slots = members * cap
    group_tokens = members * rows
    slots = groups * group_slots
    pairs = n_ep // 2
    lines = n_tp // 2
    group_pairs = members // 2
    pair = lax.div(me, 2)
    par = lax.rem(me, 2)
    mate = me + 1 - 2 * par
    core = lax.rem(my, 2)
    line = lax.div(my, 2)
    sibling = my + 1 - 2 * core
    my_group = lax.div(pair, group_pairs)
    far_groups = partners(my_group, groups)
    x_straight = {4: X_STRAIGHT, 2: (0,)}.get(groups, ())
    f_straight = {4: F_STRAIGHT, 2: (0,)}.get(groups, ())
    x_sends = X_SENDS if groups == 4 else range(groups - 1)
    x_order = X_ORDER if groups == 4 else range(groups - 1)
    far_lines = [lax.rem(line + d, lines) for d in range(1, lines)]

    def same_core(y):
        return 2 * y + core

    def other_core(y):
        return 2 * y + 1 - core

    def twin(q):
        return 2 * q + par

    def cross(q):
        return 2 * q + 1 - par

    def pairs_in(g, own=False):
        mine = lax.rem(pair, group_pairs)
        return [
            g * group_pairs + lax.rem(mine + m, group_pairs)
            for m in range(1 if own else 0, group_pairs)
        ]

    others = [q for g in far_groups for q in pairs_in(g)] + pairs_in(my_group, True)
    ep_peers = [p for q in others for p in (cross(q), twin(q))] + [mate]
    far_tp = [p for y in far_lines for p in (same_core(y), other_core(y))]
    tp_peers = far_tp + [sibling]

    def sem(name, index=0):
        return sems.at[starts[name] + index]

    def ep_copy(src, dst, name, peer, index=0):
        return pltpu.make_async_remote_copy(
            src_ref=src, dst_ref=dst, send_sem=sem(name + "s"), recv_sem=sem(name + "r", index),
            device_id=(peer, my), device_id_type=MESH,
        )

    def tp_copy(src, dst, name, peer, index=0):
        return pltpu.make_async_remote_copy(
            src_ref=src, dst_ref=dst, send_sem=sem(name + "s"), recv_sem=sem(name + "r", index),
            device_id=(me, peer), device_id_type=MESH,
        )

    drains = []

    loads = [
        pltpu.make_async_copy(src, dst, sem("load", LOADED_WITH[i]))
        for i, (src, dst) in enumerate(zip(hbm, held))
    ]
    state_i, decay_i, beta_i, q_i, k_i, v_i, o_i, dg_i, du_i, eg_i, eu_i, ed_i, dd_i = range(9, 22)
    order = (decay_i, beta_i, k_i, q_i, v_i, state_i, o_i, dg_i, du_i, eg_i, eu_i, ed_i, dd_i)
    for i in range(9):
        loads[i].start()
    barrier = pltpu.get_barrier_semaphore()
    for p in ep_peers:
        pl.semaphore_signal(barrier, inc=1, device_id=(p, my), device_id_type=MESH)
    for p in tp_peers:
        pl.semaphore_signal(barrier, inc=1, device_id=(me, p), device_id_type=MESH)
    for i in order:
        loads[i].start()

    for i in range(9):
        loads[i].wait()
    x = tokens[...].astype(F32)
    mean_sq = jnp.mean(x * x, axis=-1, keepdims=True)
    normed = (x * lax.rsqrt(mean_sq + EPS) * attn_gain[...]).astype(BF)
    for p in range(n_ep):
        n_send[p] = normed[:, p * depth : (p + 1) * depth]
    pl.semaphore_wait(barrier, n_ep + n_tp - 2)
    def shelf(p):
        return lax.rem(p, 2) * pairs + lax.div(p, 2)

    def carried(q):
        return 2 * q + lax.rem(par + pair + q + core, 2)

    for q in others:
        ep_copy(n_send.at[carried(q)], n_recv.at[shelf(me)], "n", carried(q), pair).start()
    ep_copy(n_send.at[mate], n_recv.at[shelf(me)], "n", mate, pairs).start()
    n_recv[shelf(me)] = n_send[me]

    logit_exp = jnp.exp(logit[...])
    route = group_prob[...] * logit_exp / jnp.sum(logit_exp, axis=0, keepdims=True)
    names = ids[...]
    eye = lax.broadcasted_iota(jnp.int32, (rows, rows), 0) == lax.broadcasted_iota(
        jnp.int32, (rows, rows), 1
    )
    c_send[...] = jnp.zeros_like(c_send)
    for p in range(n_ep):
        flat = jnp.sum(jnp.where(names == p, route, 0.0), axis=0, keepdims=True)
        c_send[p, :, :rows] = jnp.broadcast_to(flat, (8, rows))
    for p in ep_peers:
        ep_copy(c_send.at[p], c_rows.at[me], "c", p).start()
    c_rows[me] = c_send[me]

    def column(row):
        return jnp.sum(jnp.where(eye, row[:, :rows], 0.0), axis=1, keepdims=True)

    loads[decay_i].wait()
    loads[beta_i].wait()
    decay_pre = dot_t(normed, w_decay[...])
    beta_pre = dot_t(normed, w_beta[...])
    lane = lax.broadcasted_iota(jnp.int32, decay_pre.shape, 1)
    decays, betas = [], []
    for h in range(heads):
        mine = lane == my * heads + h
        d = jnp.sum(jnp.where(mine, decay_pre, 0.0), axis=1, keepdims=True)
        b = jnp.sum(jnp.where(mine, beta_pre, 0.0), axis=1, keepdims=True)
        soft = jnp.maximum(d, 0.0) + jnp.log1p(jnp.exp(-jnp.abs(d)))
        decays.append(jnp.exp(-decay_rate[:, h : h + 1] * soft))
        betas.append(1.0 / (1.0 + jnp.exp(-b)))
    for i in (q_i, k_i, v_i):
        loads[i].wait()

    most = pl.ds(0, n_ep - 1)
    some = pl.ds(0, pairs - 1)
    for q in others:
        block = n_recv.at[shelf(carried(q))]
        ep_copy(block, block, "n", mate, q).wait_recv()
        tp_copy(block, block, "m", sibling).start()
    ep_copy(n_send.at[mate], n_recv.at[shelf(mate)], "n", mate, pairs).wait_recv()
    drains.append(ep_copy(n_send.at[pl.ds(0, pairs)], n_recv.at[pl.ds(0, pairs)], "n", mate))
    passed = tp_copy(n_recv.at[some], n_recv.at[some], "m", sibling)
    passed.wait_recv()
    drains.append(passed)

    def rows_of(parity):
        held_rows = n_recv[pl.ds(parity * pairs, pairs)].astype(F32)
        return held_rows.reshape(pairs * rows, depth).astype(BF)

    away, near = rows_of(1 - par), rows_of(par)
    k_part = dot(jnp.concatenate([away, near], axis=0), w_k[...]).reshape(2, pairs, rows, local)
    k_own[...] = k_part
    for side in range(2):
        k_send[:, side] = k_part[side].astype(BF)
    for q in others:
        ep_copy(k_send.at[q], k_recv.at[pair], "k1", twin(q)).start()
    for j, w in enumerate((w_q, w_v)):
        q_away[j] = dot(away, w[...]).reshape(pairs, rows, local).astype(BF)
        ep_copy(q_away.at[j], q_mate.at[j], "q1", mate, j).start()
    for j, w in enumerate((w_q, w_v)):
        q_own[j] = dot(near, w[...]).reshape(pairs, rows, local)
    for j in range(2):
        ep_copy(q_away.at[j], q_mate.at[j], "q1", mate, j).wait_recv()
        both = q_own[j] + q_mate[j].astype(F32)
        q_own[j] = both
        q_send[j] = both.astype(BF)
        for q in others:
            ep_copy(q_send.at[j, q], q_recv.at[j, pair], "q2", twin(q), j).start()
    drains.append(ep_copy(q_away, q_mate, "q1", mate))
    far_blocks = pl.ds(0, pairs - 1)
    sent = q_send.at[pl.ds(0, 2), far_blocks]
    drains.append(ep_copy(sent, q_recv.at[pl.ds(0, 2), far_blocks], "q2", mate))
    done_k = ep_copy(k_send.at[far_blocks], k_recv.at[far_blocks], "k1", mate)
    done_k.wait_recv()
    drains.append(done_k)
    sums = []
    for side in range(2):
        total = k_own[side, pair]
        for q in others:
            total = total + k_recv[q, side].astype(F32)
        sums.append(total)
        if side == 0:
            k_away[...] = total.astype(BF)
            cross_k = ep_copy(k_away, k_mate, "k2", mate)
            cross_k.start()
            drains.append(cross_k)

    def summed(j):
        ep_copy(
            q_send.at[j, far_blocks], q_recv.at[j, far_blocks], "q2", mate, j
        ).wait_recv()
        total = q_own[j, pair]
        for q in others:
            total = total + q_recv[j, q].astype(F32)
        return total.astype(BF).astype(F32)

    q_rows = summed(0)
    cross_k.wait_recv()
    k_rows = (sums[1] + k_mate[...].astype(F32)).astype(BF).astype(F32)
    loads[state_i].wait()

    def head_of(values, h):
        return values[:, h * 128 : (h + 1) * 128]

    def unit(values):
        return values * lax.rsqrt(jnp.sum(values * values, axis=-1, keepdims=True) + EPS)

    units = []
    for h in range(heads):
        q_unit = unit(head_of(q_rows, h)) * 128 ** (-0.5)
        k_unit = unit(head_of(k_rows, h))
        units.append((q_unit, k_unit))
        kq[:, h, :] = k_unit
        kq[:, heads + h, :] = q_unit

    beside = 2 if heads % 2 == 0 else 1

    def one_row(b, _):
        both = kq[b].astype(BF)
        for first in range(0, heads, beside):
            pieces = [state[b, first + i].astype(BF) for i in range(beside)]
            read = dot(both, jnp.concatenate(pieces, axis=1))
            for i in range(beside):
                h, lanes = first + i, slice(i * 128, (i + 1) * 128)
                recall[h, pl.ds(b, 1), :] = read[h : h + 1, lanes]
                recall[heads + h, pl.ds(b, 1), :] = read[heads + h : heads + h + 1, lanes]
        return 0

    lax.fori_loop(0, rows, one_row, 0, unroll=RECALL)
    v_rows = summed(1)
    for h in range(heads):
        q_unit, k_unit = units[h]
        decay, beta = decays[h], betas[h]
        corr = beta * (head_of(v_rows, h) - decay * recall[h])
        read = decay * recall[heads + h] + jnp.sum(q_unit * k_unit, axis=-1, keepdims=True) * corr
        read = read * lax.rsqrt(jnp.mean(read * read, axis=-1, keepdims=True) + EPS) * head_gain[...]
        head_out[:, h * 128 : (h + 1) * 128] = read.astype(BF)
        corr_ref[h] = corr
        decay_ref[h] = jnp.broadcast_to(decay, (rows, 128))

    loads[o_i].wait()
    ho = head_out[...]

    def columns_of(p):
        return pl.ds(pl.multiple_of(p * chunk, 128), chunk)

    for p in far_tp + [sibling]:
        a_send[p] = dot(ho, w_o[:, columns_of(p)]).astype(BF)
        tp_copy(a_send.at[p], a_recv.at[my], "a", p).start()
    a_recv[my] = dot(ho, w_o[:, columns_of(my)]).astype(BF)
    own = columns_of(my)

    def update_row(b, _):
        columns = kq[b].T
        for h in range(heads):
            corr = corr_ref[h, pl.ds(b, 1), :]
            decay = decay_ref[h, pl.ds(b, 1), :]
            state[b, h] = decay * state[b, h] + columns[:, h : h + 1] * corr
        return 0

    lax.fori_loop(0, rows // 2, update_row, 0, unroll=UPDATE)
    middle = tokens[:, own].astype(F32)
    most_tp = pl.ds(0, n_tp - 1)
    done_a = tp_copy(a_send.at[most_tp], a_recv.at[most_tp], "a", sibling)
    done_a.wait_recv()
    drains.append(done_a)
    for p in range(n_tp):
        middle = middle + a_recv[p].astype(F32)
    x_all[me] = (middle * ffn_gain[:, own]).astype(BF)
    x_peers = [mate] + [twin(q) for q in pairs_in(my_group, True)]
    for i in x_sends:
        x_peers += [twin(q) for q in pairs_in(far_groups[i])]
        if i in x_straight:
            x_peers += [cross(q) for q in pairs_in(far_groups[i])]
    for p in x_peers:
        ep_copy(x_all.at[me], x_all.at[me], "x", p, me).start()
    middle_ref[...] = middle
    s_recv[my] = jnp.broadcast_to(jnp.sum(middle * middle, axis=-1, keepdims=True), (rows, 128))
    for p in tp_peers:
        tp_copy(s_recv.at[my], s_recv.at[my], "s", p).start()
    lax.fori_loop(rows // 2, rows, update_row, 0, unroll=UPDATE)
    done_c = ep_copy(c_send.at[most], c_rows.at[most], "c", mate)
    done_c.wait_recv()
    drains.append(done_c)
    for p in range(n_ep):
        c_recv[p] = jnp.broadcast_to(column(c_rows[p, :1, :]), (rows, 128))
    tri = (
        lax.broadcasted_iota(jnp.int32, (group_tokens, group_tokens), 0)
        >= lax.broadcasted_iota(jnp.int32, (group_tokens, group_tokens), 1)
    ).astype(F32).astype(BF)
    slot = lax.broadcasted_iota(jnp.int32, (group_tokens, group_slots), 1).astype(F32)
    for g in range(groups):
        coef = c_recv[g * members : (g + 1) * members].reshape(group_tokens, 128)[:, :1]
        named = coef > 0.0
        flags = jnp.broadcast_to(jnp.where(named, 1.0, 0.0), (group_tokens, 128)).astype(BF)
        rank = dot(tri, flags)[:, :1] - 1.0
        place_ref[g] = jnp.where((rank == slot) & named, 1.0, 0.0).astype(BF)
    done_s = tp_copy(s_recv.at[most_tp], s_recv.at[most_tp], "s", sibling)
    done_s.wait_recv()
    drains.append(done_s)
    total = s_recv[0]
    for p in range(1, n_tp):
        total = total + s_recv[p]
    scale = lax.rsqrt(total / width + EPS)
    diagonal = lax.broadcasted_iota(jnp.int32, (rows, 128), 0) == lax.broadcasted_iota(
        jnp.int32, (rows, 128), 1
    )
    scale_rows[me] = jnp.broadcast_to(
        jnp.sum(jnp.where(diagonal, scale, 0.0), axis=0, keepdims=True), (8, 128)
    )
    for p in ep_peers:
        ep_copy(scale_rows.at[me], scale_rows.at[me], "z", p).start()

    def send_g(k, g):
        block = g_all.at[my, g]
        for p in [sibling] + [same_core(y) for y in far_lines]:
            tp_copy(block, block, "g", p, k * n_tp + my).start()

    def pass_on(k, g):
        for y in far_lines:
            p = same_core(y)
            block = g_all.at[p, g]
            tp_copy(block, block, "g", p, k * n_tp + p).wait_recv()
            tp_copy(block, block, "g", sibling, k * n_tp + p).start()

    def arrived_g(k, g, p):
        block = g_all.at[p, g]
        tp_copy(block, block, "g", p, k * n_tp + p).wait_recv()

    def forward_x(k):
        for q in pairs_in(group_from[k], k == 0):
            block = x_all.at[twin(q)]
            ep_copy(block, block, "x", twin(q), twin(q)).wait_recv()
            ep_copy(block, block, "x", mate, twin(q)).start()

    group_from = [my_group] + [far_groups[i] for i in x_order]
    hidden = w_dg.shape[1]
    if groups % 2:
        units = [(u * pairs, pairs) for u in range(2)]
    else:
        units = [(g * members, members) for g in group_from]
    steps = len(units) // 2
    unit_rows = units[0][1] * rows
    loads[dg_i].wait()
    loads[du_i].wait()

    def unit_of(ref, u):
        start, count = units[u]
        return ref.at[pl.ds(start, count)]

    def near_d(h):
        return tp_copy(d_send.at[h, 1], d_near.at[h], "d1", sibling, h)

    def far_d(h, y, source):
        return tp_copy(d_send.at[h, 0], d_far.at[h, source], "d2", same_core(y), h * lines + source)

    def dense_dots(h):
        xs = jnp.concatenate(
            [
                unit_of(x_all, 2 * h + u)[...].astype(F32).reshape(unit_rows, chunk)
                for u in range(2)
            ],
            axis=0,
        ).astype(BF)
        for j, w in enumerate((w_dg, w_du)):
            part = dot(xs, w[...]).reshape(2, unit_rows, hidden)
            d_half[h, :, :, j * hidden : (j + 1) * hidden] = part
        d_send[h, 1] = d_half[h, 1 - core].astype(BF)
        near_d(h).start()

    def dense_cross(h):
        near_d(h).wait_recv()
        pre = d_half[h, core] + d_near[h].astype(F32)
        d_half[h, 0] = pre
        d_send[h, 0] = pre.astype(BF)
        for y in far_lines:
            far_d(h, y, line).start()

    def dense_hide(h):
        pre = d_half[h, 0]
        for y in far_lines:
            far_d(h, y, y).wait_recv()
            pre = pre + d_far[h, y].astype(F32)
        first, count = units[2 * h][0] * (1 - core) + units[2 * h + 1][0] * core, units[2 * h][1]
        pre = pre * scale_ref[pl.ds(first, count)].reshape(unit_rows, 128)[:, :1]
        h_all[2 * h + core] = (silu(pre[:, :hidden]) * pre[:, hidden:]).astype(BF)
        sent_h(h).start()

    def sent_h(h):
        return tp_copy(h_all.at[2 * h + core], h_all.at[2 * h + core], "h", sibling, h)

    forward_x(0)
    relayed = [k + 1 for k, i in enumerate(x_order) if i not in x_straight]
    for k in range(groups):
        g = group_from[k]
        if k < len(relayed):
            forward_x(relayed[k])
        if k > 0 and k not in relayed:
            for q in pairs_in(g):
                ep_copy(x_all.at[me], x_all.at[twin(q)], "x", mate, twin(q)).wait_recv()
        for q in pairs_in(g, k == 0) + ([pair] if k == 0 else []):
            ep_copy(x_all.at[me], x_all.at[cross(q)], "x", mate, cross(q)).wait_recv()
        block = x_all[pl.ds(g * members, members)].astype(F32)
        g_all[my, g] = lax.dot_general(
            place_ref[g], block.reshape(group_tokens, chunk).astype(BF),
            (((0,), (0,)), ((), ())), preferred_element_type=F32,
        ).astype(BF)
        send_g(k, g)
        if k > 1:
            pass_on(k - 2, group_from[k - 2])
        if steps == 2 and k == 1:
            dense_dots(0)
    drains.append(ep_copy(x_all.at[most], x_all.at[most], "x", mate))
    drains.append(tp_copy(g_all.at[most_tp], g_all.at[most_tp], "g", sibling))
    for i in (eg_i, eu_i, ed_i, dd_i):
        loads[i].wait()
    if steps == 2:
        dense_cross(0)
    for h in range(0 if steps != 2 else 1, steps):
        dense_dots(h)
    if groups > 1:
        pass_on(groups - 2, group_from[groups - 2])

    def expert_in(p, gate, up):
        routed = g_all[p].astype(F32).reshape(slots, chunk).astype(BF)
        return (
            gate + dot(routed, w_eg[0, columns_of(p), :]), up + dot(routed, w_eu[0, columns_of(p), :])
        )

    gate = jnp.zeros((slots, w_eg.shape[2]), F32)
    gate, up = expert_in(my, gate, gate)
    pass_on(groups - 1, group_from[groups - 1])
    for h in range(0 if steps != 2 else 1, steps):
        dense_cross(h)
    for k in range(groups):
        arrived_g(k, group_from[k], sibling)
    gate, up = expert_in(sibling, gate, up)
    done_z = ep_copy(scale_rows.at[most], scale_rows.at[most], "z", mate)
    done_z.wait_recv()
    drains.append(done_z)
    for p in range(n_ep):
        scale_ref[p] = jnp.broadcast_to(column(scale_rows[p, :1, :]), (rows, 128))
    slot_scale = jnp.concatenate(
        [
            lax.dot_general(
                place_ref[g].astype(F32),
                scale_ref[g * members : (g + 1) * members].reshape(group_tokens, 128),
                (((0,), (0,)), ((), ())), precision=lax.Precision.HIGHEST,
                preferred_element_type=F32,
            )
            for g in range(groups)
        ],
        axis=0,
    )[:, :1]
    for h in range(steps - 1):
        dense_hide(h)
    for y in far_lines:
        gate, up = expert_in(same_core(y), gate, up)
    for y in far_lines:
        for k in range(groups):
            arrived_g(k, group_from[k], other_core(y))
        gate, up = expert_in(other_core(y), gate, up)
    expert_hidden = (silu(gate * slot_scale) * (up * slot_scale)).astype(BF)
    order_back = RETURNS if groups == 4 else tuple(range(groups))
    returns = [(far_groups + [my_group])[i] for i in order_back]
    own_at = order_back.index(groups - 1)
    f_direct = [k for k in range(groups) if order_back[k] in f_straight]

    def near_e(k, y):
        g = returns[k]
        return tp_copy(e_part.at[1 - core, g, y], e_near.at[g, y], "e1", sibling, k * lines + y)

    def far_e(k, y):
        g = returns[k]
        return tp_copy(e_send.at[g, y], e_recv.at[g, line], "e2", same_core(y), k)

    def expert_out(which, y):
        part = dot(expert_hidden, w_ed[0, :, columns_of(2 * y + which)])
        e_part[which, :, y] = part.reshape(groups, group_slots, chunk).astype(BF)

    for y in far_lines + [line]:
        expert_out(1 - core, y)
        for k in range(groups):
            near_e(k, y).start()
    for y in far_lines + [line]:
        expert_out(core, y)
    for k in range(groups):
        g = returns[k]
        for y in far_lines:
            near_e(k, y).wait_recv()
            e_send[g, y] = (e_part[core, g, y].astype(F32) + e_near[g, y].astype(F32)).astype(BF)
            far_e(k, y).start()
    drains.append(tp_copy(e_part.at[0], e_near, "e1", sibling))
    other_lines = pl.ds(0, lines - 1)
    sent = e_send.at[pl.ds(0, groups), other_lines]
    drains.append(tp_copy(sent, e_recv.at[pl.ds(0, groups), other_lines], "e2", sibling))
    dense_hide(steps - 1)
    for h in range(steps):
        tp_copy(h_all.at[core], h_all.at[2 * h + 1 - core], "h", sibling, h).wait_recv()
    drains.append(tp_copy(h_all.at[pl.ds(0, steps)], h_all.at[pl.ds(0, steps)], "h", sibling))
    sent = d_send.at[pl.ds(0, steps), 1]
    drains.append(tp_copy(sent, d_near, "d1", sibling))
    for y in far_lines:
        sent = d_send.at[pl.ds(0, steps), 0]
        drains.append(tp_copy(sent, d_far.at[pl.ds(0, steps), line], "d2", same_core(y)))
    dense_hidden = h_all[...].astype(F32).reshape(batch, hidden).astype(BF)
    dense = dot(dense_hidden, w_dd[...]) * (1.0 / (1.0 + jnp.exp(-mix[...])))
    for u in range(len(units)):
        part = dense[u * unit_rows : (u + 1) * unit_rows]
        unit_of(dense_ref, u)[...] = part.reshape(units[u][1], rows, chunk)

    def near_f(k):
        g = returns[k]
        return ep_copy(f_away.at[g], f_mate.at[g], "f1", mate, k)

    def far_f(k):
        g = returns[k]
        near_f(k).wait_recv()
        both = comb[g, par] + f_mate[g].astype(F32)
        comb[g, par] = both
        send_f(g, both, k == own_at)

    def send_f(g, values, own_group):
        f_send[pl.ds(g * group_pairs, group_pairs)] = values.astype(BF)
        for q in pairs_in(g, own_group):
            ep_copy(f_send.at[q], f_recv.at[pair], "f2", twin(q)).start()

    def straight_f(k, g):
        send_f(g, comb[g, par], False)
        first = pairs + f_straight.index(order_back[k]) * group_pairs
        f_send[pl.ds(first, group_pairs)] = comb[g, 1 - par].astype(BF)
        for m in range(group_pairs):
            spare = first + lax.rem(pair, group_pairs)
            q = g * group_pairs + m
            ep_copy(f_send.at[first + m], f_recv.at[spare], "f2", cross(q)).start()

    for k in range(groups):
        g = returns[k]
        block = pl.ds(g * members, members)
        near_e(k, line).wait_recv()
        result = e_part[core, g, line].astype(F32) + e_near[g, line].astype(F32)
        tp_copy(e_send.at[g, other_lines], e_recv.at[g, other_lines], "e2", sibling, k).wait_recv()
        for y in far_lines:
            result = result + e_recv[g, y].astype(F32)
        coef = c_recv[block].reshape(group_tokens, 128)[:, :1]
        mixed = coef * dot(place_ref[g], result.astype(BF))
        combined = dense_ref[block] + mixed.reshape(members, rows, chunk)
        for m in range(members):
            comb[g, m % 2, m // 2] = combined[m]
        if k in f_direct:
            straight_f(k, g)
        else:
            f_away[g] = comb[g, 1 - par].astype(BF)
            near_f(k).start()
        if k >= LAG and k - LAG not in f_direct:
            far_f(k - LAG)
    for k in range(max(0, groups - LAG), groups):
        if k not in f_direct:
            far_f(k)
    met = pl.ds(0, groups - len(f_direct))
    drains.append(ep_copy(f_away.at[met], f_mate.at[met], "f1", mate))
    spares = list(range(pairs, pairs + len(f_straight) * group_pairs))
    sent = pl.ds(0, pairs - 1 + len(spares))
    drains.append(ep_copy(f_send.at[sent], f_recv.at[sent], "f2", mate))
    final = middle_ref[...] + comb[my_group, par, lax.rem(pair, group_pairs)]
    ep_copy(f_send.at[sent], f_recv.at[sent], "f2", mate).wait_recv()
    for q in others + spares:
        final = final + f_recv[q].astype(F32)
    out[...] = final.astype(BF)
    for copy in drains:
        copy.wait_send()


def per_device(
    tokens, delta_state, attn_gain, query_weight, key_weight, value_weight, decay_weight,
    beta_weight, decay_rate, head_gain, output_weight, ffn_gain, expert_ids, group_prob,
    expert_logit, expert_gate, expert_up, expert_down, dense_gate, dense_up, dense_down, dense_mix,
):
    n_ep = lax.axis_size("ep")
    n_tp = lax.axis_size("tp")
    rows, width = tokens.shape
    heads = delta_state.shape[1]
    local = heads * 128
    topk = expert_ids.shape[1]
    cap = max(2, 2 * rows * topk // n_ep)
    members = max(2, 8 // math.gcd(cap, 8))
    if n_ep % members:
        members = n_ep
    groups = n_ep // members
    group_slots = members * cap
    chunk = width // n_tp
    depth = width // n_ep
    batch = n_ep * rows
    pairs = n_ep // 2
    lines = n_tp // 2
    hidden = dense_gate.shape[1]
    small = (
        tokens, attn_gain[None, :], decay_rate[None, :], head_gain[None, :], ffn_gain[None, :],
        expert_ids.T, group_prob[None, :], expert_logit.T, dense_mix[None, :],
    )
    weights = (
        delta_state, decay_weight.T, beta_weight.T, query_weight, key_weight, value_weight,
        output_weight, dense_gate, dense_up, expert_gate, expert_up, expert_down, dense_down,
    )
    arrays = tuple(pltpu.with_memory_space_constraint(a, pltpu.HBM) for a in small + weights)
    steps = dense_steps(groups)
    unit_rows = batch // (2 * steps)
    starts, n_sems = semaphores(n_ep, n_tp, members, len(arrays))
    dims = (n_ep, n_tp, rows, width, heads, members, cap, len(arrays), starts)
    vmem = pl.BlockSpec(memory_space=pltpu.VMEM)
    kq_rows = -(-2 * heads // 8) * 8
    scratch = [pltpu.VMEM(a.shape, a.dtype) for a in small + weights[1:]]
    scratch += [
        pltpu.VMEM(shape, dtype)
        for shape, dtype in (
            ((n_ep, rows, depth), BF), ((n_ep, rows, depth), BF),
            ((2, pairs, rows, local), F32), ((pairs, 2, rows, local), BF),
            ((pairs, 2, rows, local), BF), ((rows, local), BF), ((rows, local), BF),
            ((2, pairs, rows, local), BF), ((2, pairs, rows, local), BF),
            ((2, pairs, rows, local), F32),
            ((2, pairs, rows, local), BF), ((2, pairs, rows, local), BF),
            ((n_ep, 8, 128), F32), ((n_ep, 8, 128), F32), ((n_ep, rows, 128), F32),
            ((rows, kq_rows, 128), F32), ((2 * heads, rows, 128), F32),
            ((heads, rows, 128), F32), ((heads, rows, 128), F32), ((rows, local), BF),
            ((n_tp, rows, chunk), BF), ((n_tp, rows, chunk), BF), ((n_tp, rows, 128), F32),
            ((n_ep, 8, 128), F32), ((n_ep, rows, 128), F32), ((rows, chunk), F32),
            ((n_ep, rows, chunk), BF), ((n_tp, groups, group_slots, chunk), BF),
            ((steps, 2, unit_rows, 2 * hidden), F32), ((steps, 2, unit_rows, 2 * hidden), BF),
            ((steps, unit_rows, 2 * hidden), BF), ((steps, lines, unit_rows, 2 * hidden), BF),
            ((2 * steps, unit_rows, hidden), BF),
            ((2, groups, lines, group_slots, chunk), BF), ((groups, lines, group_slots, chunk), BF),
            ((groups, lines, group_slots, chunk), BF), ((groups, lines, group_slots, chunk), BF),
            ((groups, 2, members // 2, rows, chunk), F32),
            ((groups, members // 2, rows, chunk), BF), ((groups, members // 2, rows, chunk), BF),
            ((n_ep, rows, chunk), BF), ((n_ep, rows, chunk), BF),
            ((groups, members * rows, group_slots), BF), ((n_ep, rows, chunk), F32),
        )
    ]
    scratch += [pltpu.SemaphoreType.DMA((n_sems,))]
    mixed_out, new_state = pl.pallas_call(
        functools.partial(kernel, dims),
        out_shape=(pltpu.VMEM((rows, chunk), BF), pltpu.VMEM(delta_state.shape, F32)),
        in_specs=[pl.BlockSpec(memory_space=pltpu.HBM)] * len(arrays),
        out_specs=(vmem, vmem),
        scratch_shapes=scratch,
        compiler_params=pltpu.CompilerParams(
            collective_id=0, has_side_effects=True, vmem_limit_bytes=44 * 1024 * 1024
        ),
    )(*arrays)
    new_state, mixed_out = pl.pallas_call(
        store_kernel,
        out_shape=(pltpu.HBM(delta_state.shape, F32), pltpu.HBM((rows, chunk), BF)),
        in_specs=[vmem] * 2,
        out_specs=(pl.BlockSpec(memory_space=pltpu.HBM),) * 2,
        scratch_shapes=[pltpu.SemaphoreType.DMA((2,))],
        compiler_params=pltpu.CompilerParams(vmem_limit_bytes=8 * 1024 * 1024),
    )(*(pltpu.with_memory_space_constraint(a, pltpu.VMEM) for a in (new_state, mixed_out)))
    return mixed_out, new_state


def solution(mesh):
    return jax.shard_map(
        per_device,
        mesh=mesh,
        in_specs=(
            P("ep", None), P("ep", "tp", None, None), P(), P("ep", "tp"), P("ep", "tp"),
            P("ep", "tp"), P(), P(), P("tp"), P(), P("tp", None), P(), P("ep", None), P("ep"),
            P("ep", None), P("ep", None, "tp"), P("ep", None, "tp"), P("ep", "tp", None),
            P("tp", "ep"), P("tp", "ep"), P("ep", "tp"), P("tp"),
        ),
        out_specs=(P("ep", "tp"), P("ep", "tp", None, None)),
        check_vma=False,
    )
```
